128 devices in a mesh: kv: 16 (over z, x), tp: 8 (over y, core).
Axes of the slice: x: 4, y: 4, z: 4, core: 2. Of those that a mesh axis runs over, the one named last changes fastest.
Arguments:
- tokens: bfloat16 [32768, 2048], P('kv'), may hold values from -6 to 6
- norm_gain: bfloat16 [2048], replicated, may hold values from 0.099609375 to 1.8984375
- query_weight: bfloat16 [2048, 1024], P(None, 'tp'), may hold values from -0.125 to 0.125
- cmp_key_weight: bfloat16 [2048, 512], P(None, 'tp'), may hold values from -0.125 to 0.125
- cmp_value_weight: bfloat16 [2048, 512], P(None, 'tp'), may hold values from -0.125 to 0.125
- sel_key_weight: bfloat16 [2048, 512], P(None, 'tp'), may hold values from -0.125 to 0.125
- sel_value_weight: bfloat16 [2048, 512], P(None, 'tp'), may hold values from -0.125 to 0.125
- branch_weight: bfloat16 [2, 2048, 16], replicated, may hold values from -0.125 to 0.125
- key_embed: bfloat16 [8, 32, 64], P('tp'), may hold values from -3 to 3
- key_inner: bfloat16 [8, 2048, 64], P('tp'), may hold values from -0.125 to 0.125
- key_outer: bfloat16 [8, 64, 64], P('tp'), may hold values from -0.75 to 0.75
- value_embed: bfloat16 [8, 32, 64], P('tp'), may hold values from -3 to 3
- value_inner: bfloat16 [8, 2048, 64], P('tp'), may hold values from -0.125 to 0.125
- value_outer: bfloat16 [8, 64, 64], P('tp'), may hold values from -0.75 to 0.75
- out_weight: bfloat16 [1024, 2048], replicated, may hold values from -0.1875 to 0.1875
- chosen: int32 [8, 256, 8], P('tp'), may hold values from 0 to 511, as said below
Outputs:
- attended: bfloat16 [32768, 2048], P(('kv', 'tp'))
The draws below stay inside these ranges and needn't reach their ends.
Inputs may be any that keep to these rules, and one draw needn't show every extreme that they name: `chosen`: each entry is the index of a block of 64 positions in the whole sequence. For every key head and query block, its 8 entries lie in 8 different aligned spans of 2048 positions (at most one from any span), and none lies inside the query block's own positions.
All inputs are finite; a program needn't handle non-finite values.
Results may differ from the reference program's by a relative error of at most 0.0075.
Values may be sent and summed in bfloat16 or wider, within the bound.
A program may use at most 128 MiB of HBM per device.

```python
import jax
import jax.numpy as jnp
from jax import lax

D = 2048
HEADS = 16
KV_HEADS = 8
HEAD_DIM = 64
CMP_BLOCK = 32
SEL_BLOCK = 64
Q_BLOCK = 128
FAR_PICKS = 8
TOK_DEV = 2048
SEQ = 32768


def draw_chosen(key, part):
    interval_limits = SEQ // TOK_DEV
    per_span = TOK_DEV // Q_BLOCK
    span_blocks = TOK_DEV // SEL_BLOCK
    own_blocks = Q_BLOCK // SEL_BLOCK
    query_blocks = SEQ // Q_BLOCK
    key_noise, key_inner, key_shift = jax.random.split(key, 3)
    diagonal_group = jnp.arange(query_blocks, dtype=jnp.int32) // per_span
    local_index = jnp.arange(query_blocks, dtype=jnp.int32) % per_span
    eligible_group = jnp.arange(interval_limits, dtype=jnp.int32)
    jitter_perturbation = jax.random.randint(key_noise, (KV_HEADS, query_blocks, interval_limits), 0, 2 ** 16)
    preference_increment = jnp.where(eligible_group[None, :] <= diagonal_group[:, None], 2 ** 24, 0)
    preference_increment = preference_increment + jnp.where(eligible_group[None, :] == diagonal_group[:, None] - 1, 2 ** 26, 0)
    preference_increment = preference_increment + jnp.where(eligible_group[None, :] == diagonal_group[:, None] - interval_limits // 2, 2 ** 26, 0)
    preference_increment = preference_increment + jnp.where(eligible_group[None, :] == 0, 2 ** 25, 0)
    group_relevance = jitter_perturbation * interval_limits + eligible_group[None, None, :] + preference_increment[None]
    _, picked = lax.top_k(group_relevance, FAR_PICKS)
    inside = jax.random.randint(key_inner, (KV_HEADS, query_blocks, FAR_PICKS), 0, span_blocks)
    offset = jax.random.randint(key_shift, (KV_HEADS, query_blocks, FAR_PICKS), 0, span_blocks - own_blocks)
    shifted = (local_index[None, :, None] * own_blocks + own_blocks + offset) % span_blocks
    within = jnp.where(picked == diagonal_group[None, :, None], shifted, inside)
    return (picked * span_blocks + within).astype(jnp.int32)


def block_scale(rng, dims, pieces, smallest, top_value):
    def one(axis_at, blocks):
        draws = jax.random.uniform(jax.random.fold_in(jax.random.fold_in(rng, 6), axis_at), (blocks,), jnp.float32, smallest / len(pieces), top_value / len(pieces))
        return jnp.repeat(jnp.exp(draws), dims[axis_at] // blocks).reshape((-1,) + (1,) * (len(dims) - axis_at - 1))

    factor_of = one(*pieces[0])
    for cut in pieces[1:]:
        factor_of = factor_of * one(*cut)
    return factor_of


def bell_draw(own_key, shape, scale, bound, cuts=(), kind=jnp.bfloat16):
    level = block_scale(own_key, shape, cuts, -0.22, 0.18) if cuts else 1.0
    result = jax.random.normal(own_key, shape, jnp.float32) * scale * level
    return jnp.minimum(jnp.maximum(result, -bound), bound).astype(kind)


def setup_inputs(seed: int = 0) -> dict:
    splits = jax.random.split(jax.random.key(seed), 17)
    return {
        "tokens": bell_draw(splits[0], (SEQ, D), 1.0, 6.0, ((0, 16),)),
        "norm_gain": jnp.clip(1.0 + 0.18 * jax.random.normal(splits[1], (D,), jnp.float32), 0.099609375, 1.8984375).astype(jnp.bfloat16),
        "query_weight": bell_draw(splits[2], (D, HEADS * HEAD_DIM), D ** -0.5, 0.125, ((1, 8),)),
        "cmp_key_weight": bell_draw(splits[3], (D, KV_HEADS * HEAD_DIM), D ** -0.5, 0.125, ((1, 8),)),
        "cmp_value_weight": bell_draw(splits[4], (D, KV_HEADS * HEAD_DIM), D ** -0.5, 0.125, ((1, 8),)),
        "sel_key_weight": bell_draw(splits[5], (D, KV_HEADS * HEAD_DIM), D ** -0.5, 0.125, ((1, 8),)),
        "sel_value_weight": bell_draw(splits[6], (D, KV_HEADS * HEAD_DIM), D ** -0.5, 0.125, ((1, 8),)),
        "branch_weight": bell_draw(splits[7], (2, D, HEADS), D ** -0.5, 0.125),
        "key_embed": bell_draw(splits[8], (KV_HEADS, CMP_BLOCK, HEAD_DIM), 0.5, 3.0, ((0, 8),)),
        "key_inner": bell_draw(splits[9], (KV_HEADS, CMP_BLOCK * HEAD_DIM, HEAD_DIM), (CMP_BLOCK * HEAD_DIM) ** -0.5, 0.125, ((0, 8),)),
        "key_outer": bell_draw(splits[10], (KV_HEADS, HEAD_DIM, HEAD_DIM), HEAD_DIM ** -0.5, 0.75, ((0, 8),)),
        "value_embed": bell_draw(splits[11], (KV_HEADS, CMP_BLOCK, HEAD_DIM), 0.5, 3.0, ((0, 8),)),
        "value_inner": bell_draw(splits[12], (KV_HEADS, CMP_BLOCK * HEAD_DIM, HEAD_DIM), (CMP_BLOCK * HEAD_DIM) ** -0.5, 0.125, ((0, 8),)),
        "value_outer": bell_draw(splits[13], (KV_HEADS, HEAD_DIM, HEAD_DIM), HEAD_DIM ** -0.5, 0.75, ((0, 8),)),
        "out_weight": bell_draw(splits[14], (HEADS * HEAD_DIM, D), (HEADS * HEAD_DIM) ** -0.5, 0.1875),
        "chosen": draw_chosen(jax.random.fold_in(splits[16], 71), 0),
    }


ROPE_BASE = 10000.0
norm_eps = 1e-06
masked_score = -1000000000.0

def rotate(values_in, positions):
    half_dim = values_in.shape[-1] // 2
    inverse = ROPE_BASE ** (-jnp.arange(half_dim, dtype=jnp.float32) / half_dim)
    rotary_phases = positions.astype(jnp.float32)[:, None] * inverse[None, :]
    cosine = jnp.cos(rotary_phases)[:, None, :]
    sine = jnp.sin(rotary_phases)[:, None, :]
    first_half = values_in[..., :half_dim]
    second_half = values_in[..., half_dim:]
    return jnp.concatenate([first_half * cosine - second_half * sine, second_half * cosine + first_half * sine], axis=-1)

def summarize(raw_rows, embed, inner, outer):
    block_count = raw_rows.shape[0] // CMP_BLOCK
    blocked = raw_rows.reshape(block_count, CMP_BLOCK, KV_HEADS, HEAD_DIM).transpose(2, 0, 1, 3).astype(jnp.float32)
    blocked = (blocked + embed.astype(jnp.float32)[:, None]).astype(jnp.bfloat16)
    blocked = blocked.reshape(KV_HEADS, block_count, CMP_BLOCK * HEAD_DIM)
    hidden = jax.nn.gelu(jnp.einsum('knc,kce->kne', blocked.astype(jnp.float32), inner.astype(jnp.float32))).astype(jnp.bfloat16)
    return jnp.einsum('kne,kef->knf', hidden.astype(jnp.float32), outer.astype(jnp.float32)).astype(jnp.bfloat16)

def reference(tokens, norm_gain, query_weight, cmp_key_weight, cmp_value_weight, sel_key_weight, sel_value_weight, branch_weight, key_embed, key_inner, key_outer, value_embed, value_inner, value_outer, out_weight, chosen):
    length = tokens.shape[0]
    group_size = HEADS // KV_HEADS
    positions = jnp.arange(length, dtype=jnp.int32)
    scale = HEAD_DIM ** (-0.5)
    expanded_mask = tokens.astype(jnp.float32)
    normed = (expanded_mask * lax.rsqrt(lax.optimization_barrier(jnp.mean(expanded_mask * expanded_mask, axis=-1, keepdims=True)) + norm_eps) * norm_gain.astype(jnp.float32)).astype(jnp.bfloat16)

    def project(weight_in):
        return jnp.dot(normed, weight_in, preferred_element_type=jnp.float32)
    query = project(query_weight).reshape(length, HEADS, HEAD_DIM)
    q_plain = query.astype(jnp.bfloat16)
    q_turn = rotate(query, positions).astype(jnp.bfloat16)
    cmp_key = project(cmp_key_weight).astype(jnp.bfloat16).reshape(length, KV_HEADS, HEAD_DIM)
    cmp_value = project(cmp_value_weight).astype(jnp.bfloat16).reshape(length, KV_HEADS, HEAD_DIM)
    sel_key = rotate(project(sel_key_weight).reshape(length, KV_HEADS, HEAD_DIM), positions).astype(jnp.bfloat16)
    selected_value = project(sel_value_weight).astype(jnp.bfloat16).reshape(length, KV_HEADS, HEAD_DIM)
    gate_cmp = jax.nn.sigmoid(project(branch_weight[0]))
    gate_sel = jax.nn.sigmoid(project(branch_weight[1]))
    summary_key = summarize(cmp_key, key_embed, key_inner, key_outer)
    summary_value = summarize(cmp_value, value_embed, value_inner, value_outer)
    summary_count = summary_key.shape[1]
    block_end = (jnp.arange(summary_count, dtype=jnp.int32) + 1) * CMP_BLOCK - 1

    def compress_head(packed_rows):
        head_query, head_keys, head_values = packed_rows
        scores = jnp.einsum('tgd,cd->tgc', head_query.astype(jnp.float32), head_keys.astype(jnp.float32)) * scale
        allowed_keys = (block_end[None, :] <= positions[:, None])[:, None, :]
        probs = jax.nn.softmax(jnp.where(allowed_keys, scores, masked_score), axis=-1) * allowed_keys.astype(jnp.float32)
        return jnp.einsum('tgc,cd->tgd', probs.astype(jnp.bfloat16).astype(jnp.float32), head_values.astype(jnp.float32))
    q_group = q_plain.reshape(length, KV_HEADS, group_size, HEAD_DIM).transpose(1, 0, 2, 3)
    out_cmp = lax.map(compress_head, (q_group, summary_key, summary_value))
    out_cmp = out_cmp.transpose(1, 0, 2, 3).reshape(length, HEADS, HEAD_DIM)
    query_blocks = length // Q_BLOCK
    block_pos = jnp.arange(query_blocks, dtype=jnp.int32)[:, None] * Q_BLOCK + jnp.arange(Q_BLOCK, dtype=jnp.int32)[None, :]

    def select_head(packed_rows):
        head_query, head_keys, head_values, head_picks = packed_rows
        far_keys = head_keys.reshape(-1, SEL_BLOCK, HEAD_DIM)[head_picks].reshape(query_blocks, FAR_PICKS * SEL_BLOCK, HEAD_DIM)
        far_values = head_values.reshape(-1, SEL_BLOCK, HEAD_DIM)[head_picks].reshape(query_blocks, FAR_PICKS * SEL_BLOCK, HEAD_DIM)
        all_keys = jnp.concatenate([head_keys.reshape(query_blocks, Q_BLOCK, HEAD_DIM), far_keys], axis=1)
        all_values = jnp.concatenate([head_values.reshape(query_blocks, Q_BLOCK, HEAD_DIM), far_values], axis=1)
        far_pos = (head_picks[:, :, None] * SEL_BLOCK + jnp.arange(SEL_BLOCK, dtype=jnp.int32)[None, None, :]).reshape(query_blocks, -1)
        key_pos = jnp.concatenate([block_pos, far_pos], axis=1)
        allowed_keys = key_pos[:, None, None, :] <= block_pos[:, :, None, None]
        scores = jnp.einsum('nqgd,nmd->nqgm', head_query.astype(jnp.float32), all_keys.astype(jnp.float32)) * scale
        probs = jax.nn.softmax(jnp.where(allowed_keys, scores, masked_score), axis=-1)
        return jnp.einsum('nqgm,nmd->nqgd', probs.astype(jnp.bfloat16).astype(jnp.float32), all_values.astype(jnp.float32))
    q_sel = q_turn.reshape(query_blocks, Q_BLOCK, KV_HEADS, group_size, HEAD_DIM).transpose(2, 0, 1, 3, 4)
    out_sel = lax.map(select_head, (q_sel, sel_key.transpose(1, 0, 2), selected_value.transpose(1, 0, 2), chosen.astype(jnp.int32)))
    out_sel = out_sel.transpose(1, 2, 0, 3, 4).reshape(length, HEADS, HEAD_DIM)
    mixed = (gate_cmp[..., None] * out_cmp + gate_sel[..., None] * out_sel).reshape(length, HEADS * HEAD_DIM).astype(jnp.bfloat16)
    return jnp.dot(mixed, out_weight, preferred_element_type=jnp.float32).astype(jnp.bfloat16)
```

```python
import math

import jax
import jax.numpy as jnp
import numpy as np
from jax import lax
from jax.experimental import pallas as pl
from jax.experimental.pallas import tpu as pltpu
from jax.sharding import PartitionSpec as P

HEAD_DIM = 64
CMP_BLOCK = 32
SEL_BLOCK = 64
Q_BLOCK = 128
FAR_PICKS = 8
ROPE_BASE = 10000.0
NORM_EPS = 1e-06
MESH = pl.DeviceIdType.MESH
NT = (((1,), (1,)), ((), ()))
NEG = -1e30
ROWS = 512


def rope_tables(seq):
    half = HEAD_DIM // 2
    inverse = ROPE_BASE ** (-np.arange(half, dtype=np.float64) / half)
    lane = np.arange(128) % half
    low = np.arange(64, dtype=np.float64)[:, None] * inverse[lane][None, :]
    high = np.arange(seq // 64, dtype=np.float64)[:, None] * 64.0 * inverse[lane][None, :]
    return tuple(np.asarray(f(a), np.float32) for a in (low, high) for f in (np.cos, np.sin))


def gelu(x):
    return 0.5 * x * (1.0 + jnp.tanh(math.sqrt(2.0 / math.pi) * (x + 0.044715 * (x * x * x))))


def project_kernel(
    x_ref, gain_ref, qw_ref, ck_ref, cv_ref, sk_ref, sv_ref, bw_ref, ke_ref, ki_ref, ko_ref, ve_ref, vi_ref, vo_ref,
    cl_ref, sl_ref, ch_ref, sh_ref,
    qp_ref, qt_ref, kv_ref, gate_ref, sum_ref,
    w_ref, bi_ref, xk_ref, xv_ref,
):
    step = pl.program_id(0)
    me = lax.axis_index("kv")
    tp = lax.axis_index("tp")

    @pl.when(step == 0)
    def _():
        gain = gain_ref[...].astype(jnp.float32)
        w_ref[0:128, :] = (qw_ref[...].astype(jnp.float32).T * gain).astype(jnp.bfloat16)
        for at, ref in ((128, sk_ref), (192, sv_ref), (256, ck_ref), (320, cv_ref)):
            w_ref[at : at + 64, :] = (ref[...].astype(jnp.float32) * gain).astype(jnp.bfloat16)
        r = lax.broadcasted_iota(jnp.int32, (128, 32), 0)
        c = lax.broadcasted_iota(jnp.int32, (128, 32), 1)
        want = jnp.where(r < 2, tp * 2 + r, 16 + tp * 2 + (r - 2))
        pick = jnp.where((r < 4) & (c == want), 1.0, 0.0).astype(jnp.bfloat16)
        gates = jnp.dot(pick, bw_ref[...].reshape(32, -1), preferred_element_type=jnp.float32)
        w_ref[384:512, :] = (gates * gain).astype(jnp.bfloat16)

    x = x_ref[...]
    xf = x.astype(jnp.float32)
    scale = lax.rsqrt(jnp.sum(xf * xf, axis=1, keepdims=True) * (1.0 / x.shape[1]) + NORM_EPS)
    y = lax.dot_general(x, w_ref[...], NT, preferred_element_type=jnp.float32) * scale

    lane = lax.broadcasted_iota(jnp.int32, (1, 128), 1)
    front = lane < 64
    flip = lane % 64 < 32
    sign = jnp.where(flip, -1.0, 1.0)
    cos, sin = [], []
    low_c, low_s = cl_ref[...], sl_ref[...]
    for g in range(ROWS // 64):
        at = me * 32 + step * (ROWS // 64) + g
        hc, hs = ch_ref[pl.ds(at, 1), :], sh_ref[pl.ds(at, 1), :]
        cos.append(low_c * hc - low_s * hs)
        sin.append(low_c * (hs * sign) + low_s * (hc * sign))
    cos = jnp.concatenate(cos, axis=0)
    sin = jnp.concatenate(sin, axis=0)

    def turn(v, c, s):
        swapped = jnp.where(flip, pltpu.roll(v, 96, 1), pltpu.roll(v, 32, 1))
        return v * c + swapped * s

    def by_head(v):
        v = v * (HEAD_DIM**-0.5)
        first = jnp.where(front, v, 0.0)
        second = jnp.where(front, pltpu.roll(v, 64, 1), 0.0)
        return jnp.stack([first, second]).astype(jnp.bfloat16)

    q = y[:, 0:128]
    qp_ref[...] = by_head(q)
    qt_ref[...] = by_head(turn(q, cos, sin))
    kv_ref[...] = turn(y[:, 128:256], jnp.where(front, cos, 1.0), jnp.where(front, sin, 0.0)).astype(jnp.bfloat16)
    gate_ref[...] = 1.0 / (1.0 + jnp.exp(-y[:, 384:512]))
    embed = jnp.concatenate([ke_ref[0], ve_ref[0]], axis=1).astype(jnp.float32)
    embed = jnp.concatenate([embed] * (ROWS // CMP_BLOCK), axis=0)
    raw = y[:, 256:384].astype(jnp.bfloat16).astype(jnp.float32)
    bi_ref[pl.ds(pl.multiple_of(step * ROWS, ROWS), ROWS), :] = raw + embed

    @pl.when(step == pl.num_programs(0) - 1)
    def _():
        n = bi_ref.shape[0] // CMP_BLOCK
        for t in range(0, CMP_BLOCK, 2):
            a = bi_ref[pl.ds(t, n, stride=CMP_BLOCK), :]
            b = bi_ref[pl.ds(t + 1, n, stride=CMP_BLOCK), :]
            xk_ref[:, t * 64 : t * 64 + 128] = jnp.where(front, a, pltpu.roll(b, 64, 1)).astype(jnp.bfloat16)
            xv_ref[:, t * 64 : t * 64 + 128] = jnp.where(front, pltpu.roll(a, 64, 1), b).astype(jnp.bfloat16)
        out = []
        for x_in, inner, outer in ((xk_ref, ki_ref, ko_ref), (xv_ref, vi_ref, vo_ref)):
            hidden = lax.dot_general(x_in[...], inner[0], NT, preferred_element_type=jnp.float32)
            hidden = gelu(hidden).astype(jnp.bfloat16)
            out.append(jnp.dot(hidden, outer[0], preferred_element_type=jnp.float32))
        sum_ref[...] = jnp.concatenate(out, axis=1).astype(jnp.bfloat16)


def project(tokens, gain, qw, ck, cv, sk, sv, bw, ke, ki, ko, ve, vi, vo, seq):
    rows, width = tokens.shape
    tables = rope_tables(seq)
    steps = rows // ROWS

    def full(a):
        return pl.BlockSpec(a.shape, lambda i, n=a.ndim: (0,) * n, pipeline_mode=pl.Buffered(1))

    rest = (gain, qw, ck, cv, sk, sv, bw, ke, ki, ko, ve, vi, vo, *tables)
    bf, f32 = jnp.bfloat16, jnp.float32
    return pl.pallas_call(
        project_kernel,
        grid=(steps,),
        in_specs=[pl.BlockSpec((ROWS, width), lambda i: (i, 0))] + [full(a) for a in rest],
        out_specs=[
            pl.BlockSpec((2, ROWS, 128), lambda i: (0, i, 0)),
            pl.BlockSpec((2, ROWS, 128), lambda i: (0, i, 0)),
            pl.BlockSpec((ROWS, 128), lambda i: (i, 0)),
            pl.BlockSpec((ROWS, 128), lambda i: (i, 0)),
            pl.BlockSpec((rows // CMP_BLOCK, 128), lambda i: (0, 0)),
        ],
        out_shape=[
            jax.ShapeDtypeStruct((2, rows, 128), bf),
            jax.ShapeDtypeStruct((2, rows, 128), bf),
            jax.ShapeDtypeStruct((rows, 128), bf),
            jax.ShapeDtypeStruct((rows, 128), f32),
            jax.ShapeDtypeStruct((rows // CMP_BLOCK, 128), bf),
        ],
        scratch_shapes=[
            pltpu.VMEM((512, width), bf),
            pltpu.VMEM((rows, 128), f32),
            pltpu.VMEM((rows // CMP_BLOCK, CMP_BLOCK * 64), bf),
            pltpu.VMEM((rows // CMP_BLOCK, CMP_BLOCK * 64), bf),
        ],
        compiler_params=pltpu.CompilerParams(dimension_semantics=("arbitrary",), vmem_limit_bytes=26 << 20),
        name="project",
    )(tokens, *rest)


def rel(dz, dx):
    return (dz % 4) * 4 + dx % 4


def transfer_plan():
    plan = [("x+", rel(0, 0), 0, 2, rel(0, -1)), ("x-", rel(0, 0), 0, 2, rel(0, 1))]
    plan += [("z+", rel(0, 0), 2, 2, rel(-1, 0)), ("z-", rel(0, 0), 2, 2, rel(1, 0))]
    plan += [("z+", rel(0, 0), 0, 2, rel(-1, 0)), ("z-", rel(0, 0), 0, 2, rel(1, 0))]
    plan += [("x+", rel(0, 0), 2, 2, rel(0, -1)), ("x-", rel(0, 0), 2, 2, rel(0, 1))]
    plan += [("x+", rel(0, -1), 0, 1, rel(0, 2)), ("x-", rel(0, 1), 1, 1, rel(0, 2))]
    plan += [("z+", rel(-1, 0), 2, 1, rel(2, 0)), ("z-", rel(1, 0), 3, 1, rel(2, 0))]
    for d in (-1, 1):
        plan += [("z+", rel(0, d), 0, 2, rel(-1, d)), ("z-", rel(0, d), 0, 2, rel(1, d))]
        plan += [("x+", rel(d, 0), 2, 2, rel(d, -1)), ("x-", rel(d, 0), 2, 2, rel(d, 1))]
    plan += [("z+", rel(-1, 0), 0, 1, rel(2, 0)), ("z-", rel(1, 0), 1, 1, rel(2, 0))]
    plan += [("x+", rel(0, -1), 2, 1, rel(0, 2)), ("x-", rel(0, 1), 3, 1, rel(0, 2))]
    plan += [("z+", rel(0, 2), 0, 2, rel(-1, 2)), ("z-", rel(0, 2), 0, 2, rel(1, 2))]
    plan += [("x+", rel(2, 0), 2, 2, rel(2, -1)), ("x-", rel(2, 0), 2, 2, rel(2, 1))]
    for d in (-1, 1):
        plan += [("z+", rel(-1, d), 0, 1, rel(2, d)), ("z-", rel(1, d), 1, 1, rel(2, d))]
        plan += [("x+", rel(d, -1), 2, 1, rel(d, 2)), ("x-", rel(d, 1), 3, 1, rel(d, 2))]
    plan += [("z+", rel(-1, 2), 0, 1, rel(2, 2)), ("z-", rel(1, 2), 1, 1, rel(2, 2))]
    plan += [("x+", rel(2, -1), 2, 1, rel(2, 2)), ("x-", rel(2, 1), 3, 1, rel(2, 2))]
    return plan


PLAN = transfer_plan()


def attend_kernel(
    chosen_ref, kv_ref, qp_ref, qt_ref, gate_ref, sum_ref,
    out_ref,
    span_ref, sums_ref, mix_ref, send_ref, local_sem, span_send, span_recv, sum_send, sum_recv, tp_send, tp_recv,
):
    me = lax.axis_index("kv")
    tp = lax.axis_index("tp")
    mz, mx = me // 4, me % 4
    step_to = {
        "x+": (mz * 4 + (mx + 1) % 4, tp),
        "x-": (mz * 4 + (mx + 3) % 4, tp),
        "z+": (((mz + 1) % 4) * 4 + mx, tp),
        "z-": (((mz + 3) % 4) * 4 + mx, tp),
    }
    own = pltpu.make_async_copy(kv_ref, span_ref.at[0], local_sem)
    own.start()
    barrier = pltpu.get_barrier_semaphore()
    for k in range(1, 16):
        pl.semaphore_signal(barrier, inc=1, device_id=((me + k) % 16, tp), device_id_type=MESH)
    for k in range(1, 8):
        pl.semaphore_signal(barrier, inc=1, device_id=(me, (tp + k) % 8), device_id_type=MESH)
    pl.semaphore_wait(barrier, 22)

    def sum_copy(k):
        return pltpu.make_async_remote_copy(
            src_ref=sum_ref, dst_ref=sums_ref.at[me], send_sem=sum_send.at[k - 1], recv_sem=sum_recv.at[k - 1],
            device_id=((me + k) % 16, tp), device_id_type=MESH,
        )

    for k in range(1, 16):
        sum_copy(k).start()
    sums_ref[me] = sum_ref[...]

    def span_copy(i):
        way, source, first, n, target = PLAN[i]
        return pltpu.make_async_remote_copy(
            src_ref=span_ref.at[source, pl.ds(first * 8, n * 8)],
            dst_ref=span_ref.at[target, pl.ds(first * 8, n * 8)],
            send_sem=span_send.at[i], recv_sem=span_recv.at[i],
            device_id=step_to[way], device_id_type=MESH,
        )

    brings = {}
    for i, (_, _, first, n, target) in enumerate(PLAN):
        for quarter in range(first, first + n):
            brings[target, quarter] = i
    arrived = set()

    def start(i):
        _, source, first, n, _ = PLAN[i]
        if source:
            for quarter in range(first, first + n):
                need = brings[source, quarter]
                if need not in arrived:
                    span_copy(need).wait_recv()
                    arrived.add(need)
        span_copy(i).start()

    own.wait()
    for i in range(8):
        start(i)
    for k in range(1, 16):
        sum_copy(k).wait_recv()

    lane = lax.broadcasted_iota(jnp.int32, (1, 128), 1)
    front = lane < 64
    base = me * 2048

    def join(first, second):
        return jnp.where(front, pltpu.roll(first, 64, 1), second)

    @pl.loop(0, 8)
    def _(t):
        at = pl.multiple_of(t * 256, 256)
        rows = base + at + lax.broadcasted_iota(jnp.int32, (256, 1), 0)
        limit = (rows + 1) // CMP_BLOCK
        column = lax.broadcasted_iota(jnp.int32, (256, 1024), 1)
        sums = sums_ref[...].reshape(1024, 128)
        out = []
        for h in range(2):
            s = lax.dot_general(qp_ref[h, pl.ds(at, 256), :], sums, NT, preferred_element_type=jnp.float32)
            s = jnp.where(column < limit, s, NEG)
            top = jnp.maximum(jnp.max(s, axis=1, keepdims=True), -1e20)
            p = jnp.exp(s - top)
            total = jnp.maximum(jnp.sum(p, axis=1, keepdims=True), 0.5)
            o = jnp.dot(p.astype(jnp.bfloat16), sums, preferred_element_type=jnp.float32)
            out.append(o * (gate_ref[pl.ds(at, 256), h : h + 1] / total))
        mix_ref[pl.ds(at, 256), :] = join(*out)

    for i in range(8, len(PLAN)):
        start(i)
    for i in range(len(PLAN)):
        if i not in arrived:
            span_copy(i).wait_recv()

    triangle = lax.broadcasted_iota(jnp.int32, (128, 128), 1) <= lax.broadcasted_iota(jnp.int32, (128, 128), 0)
    ty, core = tp // 2, tp % 2

    def target_of(i):
        pair = i // 2
        dy = jnp.where(pair == 0, 2, jnp.where(pair == 1, 1, jnp.where(pair == 2, 3, 0)))
        flip = jnp.where(pair == 3, 1 - i % 2, i % 2)
        return ((ty + dy) % 4) * 2 + (core + flip) % 2

    def tp_copy(i, to):
        return pltpu.make_async_remote_copy(
            src_ref=send_ref.at[i], dst_ref=out_ref.at[:, pl.ds(pl.multiple_of(tp * 128, 128), 128)],
            send_sem=tp_send.at[i], recv_sem=tp_recv.at[i], device_id=(me, to), device_id_type=MESH,
        )

    @pl.loop(0, 8)
    def _(i):
        to = target_of(i)
        for half in range(2):
            j = to * 2 + half
            at = pl.multiple_of(j * 128, 128)
            parts, bias = [span_ref[0, 2 * j], span_ref[0, 2 * j + 1]], []
            for c in range(FAR_PICKS):
                block = chosen_ref[0, c, me * 16 + j]
                span, inside = block // 32, block % 32
                slot = ((span // 4 + 4 - mz) % 4) * 4 + (span % 4 + 4 - mx) % 4
                parts.append(span_ref[slot, inside])
                bias.append(jnp.where(block * 64 < base + at, 0.0, NEG))
            keys = jnp.concatenate(parts, axis=0)
            q = jnp.concatenate([qt_ref[0, pl.ds(at, 128), :], qt_ref[1, pl.ds(at, 128), :]], axis=0)
            s = lax.dot_general(q, keys, NT, preferred_element_type=jnp.float32)
            mine = jnp.where(jnp.concatenate([triangle, triangle], axis=0), s[:, :128], NEG)
            far = [
                s[:, 128 + 128 * c : 256 + 128 * c] + jnp.where(front, bias[2 * c], bias[2 * c + 1])
                for c in range(FAR_PICKS // 2)
            ]
            s = jnp.concatenate([mine, *far], axis=1)
            p = jnp.exp(s - jnp.max(s, axis=1, keepdims=True))
            total = jnp.sum(p, axis=1, keepdims=True)
            o = jnp.dot(p.astype(jnp.bfloat16), keys, preferred_element_type=jnp.float32)
            gates = gate_ref[pl.ds(at, 128), :]
            first = o[:128] * (gates[:, 2:3] / total[:128])
            second = o[128:] * (gates[:, 3:4] / total[128:])
            mixed = (mix_ref[pl.ds(at, 128), :] + join(first, second)).astype(jnp.bfloat16)
            send_ref[i, half * 128 : half * 128 + 128, :] = mixed

            @pl.when(i == 7)
            def _():
                out_ref[half * 128 : half * 128 + 128, pl.ds(pl.multiple_of(tp * 128, 128), 128)] = mixed

        @pl.when(i < 7)
        def _():
            tp_copy(i, to).start()

    for i in range(7):
        tp_copy(i, target_of(i)).wait_recv()
    for i in range(7):
        tp_copy(i, target_of(i)).wait_send()
    for k in range(1, 16):
        sum_copy(k).wait_send()
    for i in range(len(PLAN)):
        span_copy(i).wait_send()


def attend(chosen, kv, qp, qt, gates, summary):
    vmem = pl.BlockSpec(memory_space=pltpu.VMEM)
    return pl.pallas_call(
        attend_kernel,
        in_specs=[pl.BlockSpec(memory_space=pltpu.SMEM), pl.BlockSpec(memory_space=pl.ANY), vmem, vmem, vmem, vmem],
        out_specs=vmem,
        out_shape=jax.ShapeDtypeStruct((256, 1024), jnp.bfloat16),
        scratch_shapes=[
            pltpu.VMEM((16, 32, 64, 128), jnp.bfloat16),
            pltpu.VMEM((16, 64, 128), jnp.bfloat16),
            pltpu.VMEM((2048, 128), jnp.float32),
            pltpu.VMEM((8, 256, 128), jnp.bfloat16),
            pltpu.SemaphoreType.DMA,
            pltpu.SemaphoreType.DMA((len(PLAN),)),
            pltpu.SemaphoreType.DMA((len(PLAN),)),
            pltpu.SemaphoreType.DMA((15,)),
            pltpu.SemaphoreType.DMA((15,)),
            pltpu.SemaphoreType.DMA((7,)),
            pltpu.SemaphoreType.DMA((7,)),
        ],
        compiler_params=pltpu.CompilerParams(collective_id=0, has_side_effects=True, vmem_limit_bytes=30 << 20),
        name="attend",
    )(chosen, kv.reshape(32, 64, 128), qp, qt, gates, summary)


def per_device(
    tokens, norm_gain, query_weight, cmp_key_weight, cmp_value_weight, sel_key_weight, sel_value_weight,
    branch_weight, key_embed, key_inner, key_outer, value_embed, value_inner, value_outer, out_weight, chosen,
):
    seq = tokens.shape[0] * lax.axis_size("kv")
    qp, qt, kv, gates, summary = project(
        tokens, norm_gain.reshape(1, -1), query_weight,
        cmp_key_weight.T, cmp_value_weight.T, sel_key_weight.T, sel_value_weight.T,
        branch_weight.transpose(0, 2, 1),
        key_embed, key_inner.transpose(0, 2, 1), key_outer,
        value_embed, value_inner.transpose(0, 2, 1), value_outer, seq,
    )
    rows = attend(chosen.transpose(0, 2, 1), kv, qp, qt, gates, summary)
    return jnp.dot(rows, out_weight, preferred_element_type=jnp.float32).astype(jnp.bfloat16)


def solution(mesh):
    placed = (
        P("kv", None), P(), P(None, "tp"), P(None, "tp"), P(None, "tp"), P(None, "tp"), P(None, "tp"), P(),
        P("tp", None, None), P("tp", None, None), P("tp", None, None), P("tp", None, None), P("tp", None, None),
        P("tp", None, None), P(), P("tp", None, None),
    )
    return jax.shard_map(
        per_device, mesh=mesh, in_specs=placed, out_specs=P(("kv", "tp"), None), check_vma=False
    )
```

```python
import math

import jax
import jax.numpy as jnp
import numpy as np
from jax import lax
from jax.experimental import pallas as pl
from jax.experimental.pallas import tpu as pltpu
from jax.sharding import PartitionSpec as P

HEAD_DIM = 64
CMP_BLOCK = 32
SEL_BLOCK = 64
Q_BLOCK = 128
FAR_PICKS = 8
ROPE_BASE = 10000.0
NORM_EPS = 1e-06
MESH = pl.DeviceIdType.MESH
NT = (((1,), (1,)), ((), ()))
NEG = -1e30
ROWS = 512


def rope_tables(seq):
    half = HEAD_DIM // 2
    inverse = ROPE_BASE ** (-np.arange(half, dtype=np.float64) / half)
    lane = np.arange(128) % half
    low = np.arange(64, dtype=np.float64)[:, None] * inverse[lane][None, :]
    high = np.arange(seq // 64, dtype=np.float64)[:, None] * 64.0 * inverse[lane][None, :]
    return tuple(np.asarray(f(a), np.float32) for a in (low, high) for f in (np.cos, np.sin))


def gelu(x):
    return 0.5 * x * (1.0 + jnp.tanh(math.sqrt(2.0 / math.pi) * (x + 0.044715 * (x * x * x))))


def rel(dz, dx):
    return (dz % 4) * 4 + dx % 4


def transfer_plan():
    plan = []
    for q in (0, 2):
        plan += [("x+", rel(0, 0), q, 2, rel(0, -1)), ("x-", rel(0, 0), q, 2, rel(0, 1))]
        plan += [("z+", rel(0, 0), q, 2, rel(-1, 0)), ("z-", rel(0, 0), q, 2, rel(1, 0))]
    plan += [("x+", rel(0, -1), 0, 1, rel(0, 2)), ("x-", rel(0, 1), 1, 1, rel(0, 2))]
    plan += [("z+", rel(-1, 0), 2, 1, rel(2, 0)), ("z-", rel(1, 0), 3, 1, rel(2, 0))]
    for d in (-1, 1):
        plan += [("z+", rel(0, d), 0, 2, rel(-1, d)), ("z-", rel(0, d), 0, 2, rel(1, d))]
        plan += [("x+", rel(d, 0), 2, 2, rel(d, -1)), ("x-", rel(d, 0), 2, 2, rel(d, 1))]
    plan += [("z+", rel(-1, 0), 0, 1, rel(2, 0)), ("z-", rel(1, 0), 1, 1, rel(2, 0))]
    plan += [("x+", rel(0, -1), 2, 1, rel(0, 2)), ("x-", rel(0, 1), 3, 1, rel(0, 2))]
    plan += [("z+", rel(0, 2), 0, 2, rel(-1, 2)), ("z-", rel(0, 2), 0, 2, rel(1, 2))]
    plan += [("x+", rel(2, 0), 2, 2, rel(2, -1)), ("x-", rel(2, 0), 2, 2, rel(2, 1))]
    for d in (-1, 1):
        plan += [("z+", rel(-1, d), 0, 1, rel(2, d)), ("z-", rel(1, d), 1, 1, rel(2, d))]
        plan += [("x+", rel(d, -1), 2, 1, rel(d, 2)), ("x-", rel(d, 1), 3, 1, rel(d, 2))]
    plan += [("z+", rel(-1, 2), 0, 1, rel(2, 2)), ("z-", rel(1, 2), 1, 1, rel(2, 2))]
    plan += [("x+", rel(2, -1), 2, 1, rel(2, 2)), ("x-", rel(2, 1), 3, 1, rel(2, 2))]
    return plan


PLAN = transfer_plan()


def layer_kernel(
    chosen_ref, x_hbm, gain_hbm, qw_hbm, ck_hbm, cv_hbm, sk_hbm, sv_hbm, bw_hbm,
    ke_hbm, ki_hbm, ko_hbm, ve_hbm, vi_hbm, vo_hbm, cl_hbm, sl_hbm, ch_hbm, sh_hbm,
    out_ref,
    x_ref, gain_ref, qw_ref, ck_ref, cv_ref, sk_ref, sv_ref, bw_ref,
    ke_ref, ki_ref, ko_ref, ve_ref, vi_ref, vo_ref, cl_ref, sl_ref, ch_ref, sh_ref,
    w_ref, scale_ref, bi_ref, xk_ref, xv_ref, qp_ref, qt_ref, gate_ref, sum_ref,
    span_ref, sums_ref, mix_ref, send_ref,
    in_sem, x_sem, span_send, span_recv, sum_send, sum_recv, tp_send, tp_recv,
):
    me = lax.axis_index("kv")
    tp = lax.axis_index("tp")
    mz, mx = me // 4, me % 4
    width = x_ref.shape[-1]
    steps = x_ref.shape[0]

    small = [
        (gain_hbm, gain_ref), (sk_hbm, sk_ref), (sv_hbm, sv_ref), (ck_hbm, ck_ref), (cv_hbm, cv_ref),
        (cl_hbm, cl_ref), (sl_hbm, sl_ref), (ch_hbm.at[pl.ds(me * 32, 32)], ch_ref),
        (sh_hbm.at[pl.ds(me * 32, 32)], sh_ref), (ke_hbm, ke_ref), (ve_hbm, ve_ref),
        (ki_hbm, ki_ref), (ko_hbm, ko_ref), (vi_hbm, vi_ref), (vo_hbm, vo_ref), (qw_hbm, qw_ref), (bw_hbm, bw_ref),
    ]
    small = [pltpu.make_async_copy(a, b, in_sem.at[i]) for i, (a, b) in enumerate(small)]
    rows_in = [pltpu.make_async_copy(x_hbm.at[pl.ds(i * ROWS, ROWS)], x_ref.at[i], x_sem.at[i]) for i in range(steps)]
    for copy in small[:9]:
        copy.start()
    for copy in rows_in:
        copy.start()
    for copy in small[9:]:
        copy.start()

    barrier = pltpu.get_barrier_semaphore()
    for k in range(1, 16):
        pl.semaphore_signal(barrier, inc=1, device_id=((me + k) % 16, tp), device_id_type=MESH)
    for k in range(1, 8):
        pl.semaphore_signal(barrier, inc=1, device_id=(me, (tp + k) % 8), device_id_type=MESH)

    lane = lax.broadcasted_iota(jnp.int32, (1, 128), 1)
    front = lane < 64
    flip = lane % 64 < 32
    sign = jnp.where(flip, -1.0, 1.0)

    def angles(step):
        cos, sin = [], []
        low_c, low_s = cl_ref[...], sl_ref[...]
        for g in range(ROWS // 64):
            hc = ch_ref[pl.ds(step * (ROWS // 64) + g, 1), :]
            hs = sh_ref[pl.ds(step * (ROWS // 64) + g, 1), :]
            cos.append(low_c * hc - low_s * hs)
            sin.append(low_c * (hs * sign) + low_s * (hc * sign))
        return jnp.concatenate(cos, axis=0), jnp.concatenate(sin, axis=0)

    def turn(v, c, s):
        swapped = jnp.where(flip, pltpu.roll(v, 96, 1), pltpu.roll(v, 32, 1))
        return v * c + swapped * s

    for copy in small[:9]:
        copy.wait()
    gain = gain_ref[...].astype(jnp.float32).reshape(1, width)
    for at, ref in ((0, sk_ref), (64, sv_ref), (128, ck_ref), (192, cv_ref)):
        w_ref[at : at + 64, :] = (ref[...].astype(jnp.float32) * gain).astype(jnp.bfloat16)
    for copy in small[9:11]:
        copy.wait()
    embed = jnp.concatenate([ke_ref[0], ve_ref[0]], axis=1).astype(jnp.float32)
    embed = jnp.concatenate([embed] * (ROWS // CMP_BLOCK), axis=0)
    for copy in rows_in:
        copy.wait()

    @pl.loop(0, steps)
    def _(step):
        x = x_ref[step]
        xf = x.astype(jnp.float32)
        scale = lax.rsqrt(jnp.sum(xf * xf, axis=1, keepdims=True) * (1.0 / width) + NORM_EPS)
        scale_ref[step] = scale
        y = lax.dot_general(x, w_ref[...], NT, preferred_element_type=jnp.float32) * scale
        cos, sin = angles(step)
        kv = turn(y[:, 0:128], jnp.where(front, cos, 1.0), jnp.where(front, sin, 0.0)).astype(jnp.bfloat16)
        span_ref[0, pl.ds(step * (ROWS // 64), ROWS // 64)] = kv.reshape(ROWS // 64, 64, 128)
        raw = y[:, 128:256].astype(jnp.bfloat16).astype(jnp.float32)
        bi_ref[pl.ds(pl.multiple_of(step * ROWS, ROWS), ROWS), :] = raw + embed

    pl.semaphore_wait(barrier, 22)

    step_to = {
        "x+": (mz * 4 + (mx + 1) % 4, tp),
        "x-": (mz * 4 + (mx + 3) % 4, tp),
        "z+": (((mz + 1) % 4) * 4 + mx, tp),
        "z-": (((mz + 3) % 4) * 4 + mx, tp),
    }

    def sum_copy(k):
        return pltpu.make_async_remote_copy(
            src_ref=sum_ref, dst_ref=sums_ref.at[me], send_sem=sum_send.at[k - 1], recv_sem=sum_recv.at[k - 1],
            device_id=((me + k) % 16, tp), device_id_type=MESH,
        )

    def span_copy(i):
        way, source, first, n, target = PLAN[i]
        return pltpu.make_async_remote_copy(
            src_ref=span_ref.at[source, pl.ds(first * 8, n * 8)],
            dst_ref=span_ref.at[target, pl.ds(first * 8, n * 8)],
            send_sem=span_send.at[i], recv_sem=span_recv.at[i],
            device_id=step_to[way], device_id_type=MESH,
        )

    brings = {}
    for i, (_, _, first, n, target) in enumerate(PLAN):
        for quarter in range(first, first + n):
            brings[target, quarter] = i
    arrived = set()

    def start(i):
        _, source, first, n, _ = PLAN[i]
        if source:
            for quarter in range(first, first + n):
                need = brings[source, quarter]
                if need not in arrived:
                    span_copy(need).wait_recv()
                    arrived.add(need)
        span_copy(i).start()

    for i in range(4):
        start(i)

    for copy in small[11:]:
        copy.wait()
    count = bi_ref.shape[0] // CMP_BLOCK
    for t in range(0, CMP_BLOCK, 2):
        a = bi_ref[pl.ds(t, count, stride=CMP_BLOCK), :]
        b = bi_ref[pl.ds(t + 1, count, stride=CMP_BLOCK), :]
        xk_ref[:, t * 64 : t * 64 + 128] = jnp.where(front, a, pltpu.roll(b, 64, 1)).astype(jnp.bfloat16)
        xv_ref[:, t * 64 : t * 64 + 128] = jnp.where(front, pltpu.roll(a, 64, 1), b).astype(jnp.bfloat16)
    summary = []
    for x_in, inner, outer in ((xk_ref, ki_ref, ko_ref), (xv_ref, vi_ref, vo_ref)):
        hidden = lax.dot_general(x_in[...], inner[0], NT, preferred_element_type=jnp.float32)
        hidden = gelu(hidden).astype(jnp.bfloat16)
        summary.append(jnp.dot(hidden, outer[0], preferred_element_type=jnp.float32))
    summary = jnp.concatenate(summary, axis=1).astype(jnp.bfloat16)
    sum_ref[...] = summary
    sums_ref[me] = summary
    for i in range(4, 8):
        start(i)

    w_ref[0:128, :] = (qw_ref[...].astype(jnp.float32).T * gain).astype(jnp.bfloat16)
    r = lax.broadcasted_iota(jnp.int32, (128, 32), 0)
    c = lax.broadcasted_iota(jnp.int32, (128, 32), 1)
    want = jnp.where(r < 2, tp * 2 + r, 16 + tp * 2 + (r - 2))
    pick = jnp.where((r < 4) & (c == want), 1.0, 0.0).astype(jnp.bfloat16)
    gates = jnp.dot(pick, bw_ref[...].reshape(32, width), preferred_element_type=jnp.float32)
    w_ref[128:256, :] = (gates * gain).astype(jnp.bfloat16)
    for k in range(1, 16):
        sum_copy(k).start()

    def by_head(v):
        v = v * (HEAD_DIM**-0.5)
        first = jnp.where(front, v, 0.0)
        second = jnp.where(front, pltpu.roll(v, 64, 1), 0.0)
        return jnp.stack([first, second]).astype(jnp.bfloat16)

    @pl.loop(0, steps)
    def _(step):
        y = lax.dot_general(x_ref[step], w_ref[...], NT, preferred_element_type=jnp.float32) * scale_ref[step]
        at = pl.ds(pl.multiple_of(step * ROWS, ROWS), ROWS)
        q = y[:, 0:128]
        qp_ref[:, at, :] = by_head(q)
        qt_ref[:, at, :] = by_head(turn(q, *angles(step)))
        gate_ref[at, :] = 1.0 / (1.0 + jnp.exp(-y[:, 128:256]))

    for i in range(8, 20):
        start(i)
    for k in range(1, 16):
        sum_copy(k).wait_recv()

    base = me * 2048

    def join(first, second):
        return jnp.where(front, pltpu.roll(first, 64, 1), second)

    @pl.loop(0, 8)
    def _(t):
        at = pl.multiple_of(t * 256, 256)
        rows = base + at + lax.broadcasted_iota(jnp.int32, (256, 1), 0)
        limit = (rows + 1) // CMP_BLOCK
        column = lax.broadcasted_iota(jnp.int32, (256, 1024), 1)
        sums = sums_ref[...].reshape(1024, 128)
        out = []
        for h in range(2):
            s = lax.dot_general(qp_ref[h, pl.ds(at, 256), :], sums, NT, preferred_element_type=jnp.float32)
            s = jnp.where(column < limit, s, NEG)
            top = jnp.maximum(jnp.max(s, axis=1, keepdims=True), -1e20)
            p = jnp.exp(s - top)
            total = jnp.maximum(jnp.sum(p, axis=1, keepdims=True), 0.5)
            o = jnp.dot(p.astype(jnp.bfloat16), sums, preferred_element_type=jnp.float32)
            out.append(o * (gate_ref[pl.ds(at, 256), h : h + 1] / total))
        mix_ref[pl.ds(at, 256), :] = join(*out)

    for i in range(20, len(PLAN)):
        start(i)

    for i in range(len(PLAN)):
        if i not in arrived:
            span_copy(i).wait_recv()

    triangle = lax.broadcasted_iota(jnp.int32, (128, 128), 1) <= lax.broadcasted_iota(jnp.int32, (128, 128), 0)
    ty, core = tp // 2, tp % 2

    def target_of(i):
        pair = i // 2
        dy = jnp.where(pair == 0, 2, jnp.where(pair == 1, 1, jnp.where(pair == 2, 3, 0)))
        flip = jnp.where(pair == 3, 1 - i % 2, i % 2)
        return ((ty + dy) % 4) * 2 + (core + flip) % 2

    def tp_copy(i, to):
        return pltpu.make_async_remote_copy(
            src_ref=send_ref.at[i], dst_ref=out_ref.at[:, pl.ds(pl.multiple_of(tp * 128, 128), 128)],
            send_sem=tp_send.at[i], recv_sem=tp_recv.at[i], device_id=(me, to), device_id_type=MESH,
        )

    @pl.loop(0, 8)
    def _(i):
        to = target_of(i)
        for half in range(2):
            j = to * 2 + half
            at = pl.multiple_of(j * 128, 128)
            parts, bias = [span_ref[0, 2 * j], span_ref[0, 2 * j + 1]], []
            for c in range(FAR_PICKS):
                block = chosen_ref[0, c, me * 16 + j]
                span, inside = block // 32, block % 32
                slot = ((span // 4 + 4 - mz) % 4) * 4 + (span % 4 + 4 - mx) % 4
                parts.append(span_ref[slot, inside])
                bias.append(jnp.where(block * 64 < base + at, 0.0, NEG))
            keys = jnp.concatenate(parts, axis=0)
            q = jnp.concatenate([qt_ref[0, pl.ds(at, 128), :], qt_ref[1, pl.ds(at, 128), :]], axis=0)
            s = lax.dot_general(q, keys, NT, preferred_element_type=jnp.float32)
            mine = jnp.where(jnp.concatenate([triangle, triangle], axis=0), s[:, :128], NEG)
            far = [
                s[:, 128 + 128 * c : 256 + 128 * c] + jnp.where(front, bias[2 * c], bias[2 * c + 1])
                for c in range(FAR_PICKS // 2)
            ]
            s = jnp.concatenate([mine, *far], axis=1)
            p = jnp.exp(s - jnp.max(s, axis=1, keepdims=True))
            total = jnp.sum(p, axis=1, keepdims=True)
            o = jnp.dot(p.astype(jnp.bfloat16), keys, preferred_element_type=jnp.float32)
            gates = gate_ref[pl.ds(at, 128), :]
            first = o[:128] * (gates[:, 2:3] / total[:128])
            second = o[128:] * (gates[:, 3:4] / total[128:])
            mixed = (mix_ref[pl.ds(at, 128), :] + join(first, second)).astype(jnp.bfloat16)
            send_ref[i, half * 128 : half * 128 + 128, :] = mixed

            @pl.when(i == 7)
            def _():
                out_ref[half * 128 : half * 128 + 128, pl.ds(pl.multiple_of(tp * 128, 128), 128)] = mixed

        @pl.when(i < 7)
        def _():
            tp_copy(i, to).start()

    for i in range(7):
        tp_copy(i, target_of(i)).wait_recv()
    for i in range(7):
        tp_copy(i, target_of(i)).wait_send()
    for k in range(1, 16):
        sum_copy(k).wait_send()
    for i in range(len(PLAN)):
        span_copy(i).wait_send()


def layer(chosen, tokens, rest, seq):
    rows, width = tokens.shape
    args = (tokens, *rest, *rope_tables(seq))
    bf, f32 = jnp.bfloat16, jnp.float32
    spans = seq // rows
    held = [pltpu.VMEM((rows // ROWS, ROWS, width), bf)]
    held += [pltpu.VMEM(a.shape, a.dtype) for a in args[1:-2]]
    held += [pltpu.VMEM((rows // 64, 128), f32)] * 2
    dma = pltpu.SemaphoreType.DMA
    return pl.pallas_call(
        layer_kernel,
        in_specs=[pl.BlockSpec(memory_space=pltpu.SMEM)] + [pl.BlockSpec(memory_space=pltpu.HBM)] * len(args),
        out_specs=pl.BlockSpec(memory_space=pltpu.VMEM),
        out_shape=jax.ShapeDtypeStruct((rows // 8, 1024), bf),
        scratch_shapes=held + [
            pltpu.VMEM((256, width), bf),
            pltpu.VMEM((rows // ROWS, ROWS, 1), f32),
            pltpu.VMEM((rows, 128), f32),
            pltpu.VMEM((rows // CMP_BLOCK, CMP_BLOCK * 64), bf),
            pltpu.VMEM((rows // CMP_BLOCK, CMP_BLOCK * 64), bf),
            pltpu.VMEM((2, rows, 128), bf),
            pltpu.VMEM((2, rows, 128), bf),
            pltpu.VMEM((rows, 128), f32),
            pltpu.VMEM((rows // CMP_BLOCK, 128), bf),
            pltpu.VMEM((spans, rows // 64, 64, 128), bf),
            pltpu.VMEM((spans, rows // CMP_BLOCK, 128), bf),
            pltpu.VMEM((rows, 128), f32),
            pltpu.VMEM((8, rows // 8, 128), bf),
            dma((17,)), dma((rows // ROWS,)), dma((len(PLAN),)), dma((len(PLAN),)),
            dma((15,)), dma((15,)), dma((7,)), dma((7,)),
        ],
        compiler_params=pltpu.CompilerParams(collective_id=0, has_side_effects=True, vmem_limit_bytes=67043328),
        name="layer",
    )(chosen, *args)


def per_device(
    tokens, norm_gain, query_weight, cmp_key_weight, cmp_value_weight, sel_key_weight, sel_value_weight,
    branch_weight, key_embed, key_inner, key_outer, value_embed, value_inner, value_outer, out_weight, chosen,
):
    seq = tokens.shape[0] * lax.axis_size("kv")
    rest = (
        norm_gain, query_weight,
        cmp_key_weight.T, cmp_value_weight.T, sel_key_weight.T, sel_value_weight.T,
        branch_weight.transpose(0, 2, 1),
        key_embed, key_inner.transpose(0, 2, 1), key_outer,
        value_embed, value_inner.transpose(0, 2, 1), value_outer,
    )
    rows = layer(chosen.transpose(0, 2, 1), tokens, rest, seq)
    return jnp.dot(rows, out_weight, preferred_element_type=jnp.float32).astype(jnp.bfloat16)


def solution(mesh):
    placed = (
        P("kv", None), P(), P(None, "tp"), P(None, "tp"), P(None, "tp"), P(None, "tp"), P(None, "tp"), P(),
        P("tp", None, None), P("tp", None, None), P("tp", None, None), P("tp", None, None), P("tp", None, None),
        P("tp", None, None), P(), P("tp", None, None),
    )
    return jax.shard_map(
        per_device, mesh=mesh, in_specs=placed, out_specs=P(("kv", "tp"), None), check_vma=False
    )
```

```python
import math

import jax
import jax.numpy as jnp
import numpy as np
from jax import lax
from jax.experimental import pallas as pl
from jax.experimental.pallas import tpu as pltpu
from jax.sharding import PartitionSpec as P

HEAD_DIM = 64
CMP_BLOCK = 32
SEL_BLOCK = 64
Q_BLOCK = 128
FAR_PICKS = 8
ROPE_BASE = 10000.0
NORM_EPS = 1e-06
MESH = pl.DeviceIdType.MESH
NT = (((1,), (1,)), ((), ()))
NEG = -1e30
ROWS = 512


def rope_tables(seq):
    half = HEAD_DIM // 2
    inverse = ROPE_BASE ** (-np.arange(half, dtype=np.float64) / half)
    lane = np.arange(128) % half
    low = np.arange(64, dtype=np.float64)[:, None] * inverse[lane][None, :]
    high = np.arange(seq // 64, dtype=np.float64)[:, None] * 64.0 * inverse[lane][None, :]
    return tuple(np.asarray(f(a), np.float32) for a in (low, high) for f in (np.cos, np.sin))


def gelu(x):
    return 0.5 * x * (1.0 + jnp.tanh(math.sqrt(2.0 / math.pi) * (x + 0.044715 * (x * x * x))))


WAYS = {0: ("x", "z"), 1: ("z", "x")}
ORDER = (0, 1, 3, 2)
VIA_PLUS = 24


def copy_plan():
    plan = {}
    for kind, (first, second) in WAYS.items():
        plan[kind, "own+"] = (first + "+", "ring", 0, 32, "ring", 96)
        plan[kind, "own-"] = (first + "-", "ring", 0, 32, "ring", 32)
        plan[kind, "far+"] = (first + "+", "ring", 96, 16, "ring", 64)
        plan[kind, "far-"] = (first + "-", "ring", 48, 16, "ring", 80)
        for name, at, n, half in (("early", 0, 16, 8), ("late", 16, 48, VIA_PLUS)):
            plan[kind, name + "+"] = (second + "+", "pack", at, n, "slot", 128 + at)
            plan[kind, name + "-"] = (second + "-", "pack", 128 + at, n, "slot", at)
            plan[kind, name + "2+"] = (second + "+", "pack", 64 + at, half, "pass", at)
            plan[kind, name + "2-"] = (second + "-", "pack", 64 + at + half, n - half, "pass", at + half)
            plan[kind, name + "3+"] = (second + "+", "pass", at, half, "slot", 64 + at)
            plan[kind, name + "3-"] = (second + "-", "pass", at + half, n - half, "slot", 64 + at + half)
    return plan


PLAN = copy_plan()
NAMES = list(PLAN)


def layer_kernel(
    chosen_hbm, x_hbm, gain_hbm, qw_hbm, ck_hbm, cv_hbm, sk_hbm, sv_hbm, bw_hbm,
    ke_hbm, ki_hbm, ko_hbm, ve_hbm, vi_hbm, vo_hbm, cl_hbm, sl_hbm, ch_hbm, sh_hbm,
    out_ref,
    x_ref, gain_ref, qw_ref, ck_ref, cv_ref, sk_ref, sv_ref, bw_ref,
    ke_ref, ki_ref, ko_ref, ve_ref, vi_ref, vo_ref, cl_ref, sl_ref, ch_ref, sh_ref,
    w_ref, scale_ref, bi_ref, xk_ref, xv_ref, qp_ref, qt_ref, gate_ref, sum_ref,
    own_ref, ring_ref, pack_ref, pass_ref, slot_ref, chosen_ref, table_ref, find_ref,
    sums_ref, mix_ref, send_ref,
    in_sem, x_sem, find_sem, span_send, span_recv, sum_send, sum_recv, tp_send, tp_recv,
):
    me = lax.axis_index("kv")
    tp = lax.axis_index("tp")
    mz, mx = me // 4, me % 4
    width = x_ref.shape[-1]
    steps = x_ref.shape[0]

    small = [
        (gain_hbm, gain_ref), (sk_hbm, sk_ref), (sv_hbm, sv_ref), (ck_hbm, ck_ref), (cv_hbm, cv_ref),
        (cl_hbm, cl_ref), (sl_hbm, sl_ref), (ch_hbm.at[pl.ds(me * 32, 32)], ch_ref),
        (sh_hbm.at[pl.ds(me * 32, 32)], sh_ref), (ke_hbm, ke_ref), (ve_hbm, ve_ref),
        (ki_hbm, ki_ref), (ko_hbm, ko_ref), (vi_hbm, vi_ref), (vo_hbm, vo_ref), (qw_hbm, qw_ref), (bw_hbm, bw_ref),
        (chosen_hbm, chosen_ref),
    ]
    small = [pltpu.make_async_copy(a, b, in_sem.at[i]) for i, (a, b) in enumerate(small)]
    rows_in = [pltpu.make_async_copy(x_hbm.at[pl.ds(i * ROWS, ROWS)], x_ref.at[i], x_sem.at[i]) for i in range(steps)]
    small[17].start()
    for copy in small[:9]:
        copy.start()
    for copy in rows_in:
        copy.start()
    for copy in small[9:17]:
        copy.start()

    barrier = pltpu.get_barrier_semaphore()
    for k in range(1, 16):
        pl.semaphore_signal(barrier, inc=1, device_id=((me + k) % 16, tp), device_id_type=MESH)
    for k in range(1, 8):
        pl.semaphore_signal(barrier, inc=1, device_id=(me, (tp + k) % 8), device_id_type=MESH)

    lane = lax.broadcasted_iota(jnp.int32, (1, 128), 1)
    front = lane < 64
    flip = lane % 64 < 32
    sign = jnp.where(flip, -1.0, 1.0)

    small[17].wait()
    block = chosen_ref[0]
    query = lax.broadcasted_iota(jnp.int32, block.shape, 1)
    for s in range(16):
        table_ref[s : s + 1, :] = jnp.sum(jnp.where(block // 32 == s, block % 32, 0), axis=0, keepdims=True)
    usable = block * SEL_BLOCK < query * Q_BLOCK
    rz = jnp.where(usable, (block // 128 + 4 - mz) % 4, 0)
    rx = jnp.where(usable, (block // 32 % 4 + 4 - mx) % 4, 0)
    inside = jnp.where(usable, block % 32, 0)
    for row, r_first, r_second in ((16, rx, rz), (32, rz, rx)):
        place = jnp.where(r_first < 2, r_first, 5 - r_first)
        table_ref[row : row + 8, :] = r_first * 32 + inside
        table_ref[row + 8 : row + 16, :] = jnp.where(r_second == 0, -1, r_second * 64 - 64 + place * 16 + query % 16)
    table_ref[48:56, :] = jnp.where(usable, 1, 0)
    find = pltpu.make_async_copy(table_ref, find_ref, find_sem)
    find.start()

    def angles(step):
        cos, sin = [], []
        low_c, low_s = cl_ref[...], sl_ref[...]
        for g in range(ROWS // 64):
            hc = ch_ref[pl.ds(step * (ROWS // 64) + g, 1), :]
            hs = sh_ref[pl.ds(step * (ROWS // 64) + g, 1), :]
            cos.append(low_c * hc - low_s * hs)
            sin.append(low_c * (hs * sign) + low_s * (hc * sign))
        return jnp.concatenate(cos, axis=0), jnp.concatenate(sin, axis=0)

    def turn(v, c, s):
        swapped = jnp.where(flip, pltpu.roll(v, 96, 1), pltpu.roll(v, 32, 1))
        return v * c + swapped * s

    for copy in small[:9]:
        copy.wait()
    gain = gain_ref[...].astype(jnp.float32).reshape(1, width)
    for at, ref in ((0, sk_ref), (64, sv_ref), (128, ck_ref), (192, cv_ref)):
        w_ref[at : at + 64, :] = (ref[...].astype(jnp.float32) * gain).astype(jnp.bfloat16)
    for copy in small[9:11]:
        copy.wait()
    embed = jnp.concatenate([ke_ref[0], ve_ref[0]], axis=1).astype(jnp.float32)
    embed = jnp.concatenate([embed] * (ROWS // CMP_BLOCK), axis=0)
    for copy in rows_in:
        copy.wait()

    @pl.loop(0, steps)
    def _(step):
        x = x_ref[step]
        xf = x.astype(jnp.float32)
        scale = lax.rsqrt(jnp.sum(xf * xf, axis=1, keepdims=True) * (1.0 / width) + NORM_EPS)
        scale_ref[step] = scale
        y = lax.dot_general(x, w_ref[...], NT, preferred_element_type=jnp.float32) * scale
        cos, sin = angles(step)
        kv = turn(y[:, 0:128], jnp.where(front, cos, 1.0), jnp.where(front, sin, 0.0)).astype(jnp.bfloat16)
        kv = kv.reshape(ROWS // 64, 2, 32, 128)
        for kind in range(2):
            own_ref[kind, pl.ds(step * (ROWS // 64), ROWS // 64)] = kv[:, kind]
            ring_ref[kind, pl.ds(step * (ROWS // 64), ROWS // 64)] = kv[:, kind]
        raw = y[:, 128:256].astype(jnp.bfloat16).astype(jnp.float32)
        bi_ref[pl.ds(pl.multiple_of(step * ROWS, ROWS), ROWS), :] = raw + embed

    pl.semaphore_wait(barrier, 22)

    step_to = {
        "x+": (mz * 4 + (mx + 1) % 4, tp),
        "x-": (mz * 4 + (mx + 3) % 4, tp),
        "z+": (((mz + 1) % 4) * 4 + mx, tp),
        "z-": (((mz + 3) % 4) * 4 + mx, tp),
    }

    def sum_copy(k):
        return pltpu.make_async_remote_copy(
            src_ref=sum_ref, dst_ref=sums_ref.at[me], send_sem=sum_send.at[k - 1], recv_sem=sum_recv.at[k - 1],
            device_id=((me + k) % 16, tp), device_id_type=MESH,
        )

    refs = {"ring": ring_ref, "pack": pack_ref, "pass": pass_ref, "slot": slot_ref}

    def span_copy(*name):
        way, source, at, n, target, to = PLAN[name]
        i = NAMES.index(name)
        return pltpu.make_async_remote_copy(
            src_ref=refs[source].at[name[0], pl.ds(at, n)], dst_ref=refs[target].at[name[0], pl.ds(to, n)],
            send_sem=span_send.at[i], recv_sem=span_recv.at[i], device_id=step_to[way], device_id_type=MESH,
        )

    def start(*names):
        for name in names:
            for kind in range(2):
                span_copy(kind, name).start()

    def arrive(*names):
        for name in names:
            for kind in range(2):
                span_copy(kind, name).wait_recv()

    def pack(targets, places, source):
        @pl.loop(0, 16, unroll=2)
        def _(j):
            for kind in range(2):
                for e in targets:
                    d = e + 1
                    to = ((mz + d) % 4) * 4 + mx if kind == 0 else mz * 4 + (mx + d) % 4
                    for place in places:
                        r = ORDER[place]
                        span = mz * 4 + (mx + r) % 4 if kind == 0 else ((mz + r) % 4) * 4 + mx
                        wanted = find_ref[span, to * 16 + j]
                        pack_ref[kind, e * 64 + place * 16 + j] = source[kind, r * 32 + wanted]

    start("own+", "own-")
    find.wait()
    pack((0, 1, 2), (0,), own_ref)
    start("early+", "early-")

    for copy in small[11:17]:
        copy.wait()
    count = bi_ref.shape[0] // CMP_BLOCK
    for t in range(0, CMP_BLOCK, 2):
        a = bi_ref[pl.ds(t, count, stride=CMP_BLOCK), :]
        b = bi_ref[pl.ds(t + 1, count, stride=CMP_BLOCK), :]
        xk_ref[:, t * 64 : t * 64 + 128] = jnp.where(front, a, pltpu.roll(b, 64, 1)).astype(jnp.bfloat16)
        xv_ref[:, t * 64 : t * 64 + 128] = jnp.where(front, pltpu.roll(a, 64, 1), b).astype(jnp.bfloat16)
    summary = []
    for x_in, inner, outer in ((xk_ref, ki_ref, ko_ref), (xv_ref, vi_ref, vo_ref)):
        hidden = lax.dot_general(x_in[...], inner[0], NT, preferred_element_type=jnp.float32)
        hidden = gelu(hidden).astype(jnp.bfloat16)
        summary.append(jnp.dot(hidden, outer[0], preferred_element_type=jnp.float32))
    summary = jnp.concatenate(summary, axis=1).astype(jnp.bfloat16)
    sum_ref[...] = summary
    sums_ref[me] = summary

    w_ref[0:128, :] = (qw_ref[...].astype(jnp.float32).T * gain).astype(jnp.bfloat16)
    r = lax.broadcasted_iota(jnp.int32, (128, 32), 0)
    c = lax.broadcasted_iota(jnp.int32, (128, 32), 1)
    want = jnp.where(r < 2, tp * 2 + r, 16 + tp * 2 + (r - 2))
    pick = jnp.where((r < 4) & (c == want), 1.0, 0.0).astype(jnp.bfloat16)
    gates = jnp.dot(pick, bw_ref[...].reshape(32, width), preferred_element_type=jnp.float32)
    w_ref[128:256, :] = (gates * gain).astype(jnp.bfloat16)
    for k in range(1, 16):
        sum_copy(k).start()

    arrive("own+", "own-")
    start("far+", "far-", "early2+", "early2-")

    def by_head(v):
        v = v * (HEAD_DIM**-0.5)
        first = jnp.where(front, v, 0.0)
        second = jnp.where(front, pltpu.roll(v, 64, 1), 0.0)
        return jnp.stack([first, second]).astype(jnp.bfloat16)

    @pl.loop(0, steps)
    def _(step):
        y = lax.dot_general(x_ref[step], w_ref[...], NT, preferred_element_type=jnp.float32) * scale_ref[step]
        at = pl.ds(pl.multiple_of(step * ROWS, ROWS), ROWS)
        q = y[:, 0:128]
        qp_ref[:, at, :] = by_head(q)
        qt_ref[:, at, :] = by_head(turn(q, *angles(step)))
        gate_ref[at, :] = 1.0 / (1.0 + jnp.exp(-y[:, 128:256]))

    arrive("far+", "far-")
    pack((1,), (1, 2, 3), ring_ref)
    start("late2+", "late2-")
    arrive("early2+", "early2-")
    start("early3+", "early3-")
    pack((0,), (1, 2, 3), ring_ref)
    start("late+")
    pack((2,), (1, 2, 3), ring_ref)
    start("late-")
    for k in range(1, 16):
        sum_copy(k).wait_recv()

    base = me * 2048

    def join(first, second):
        return jnp.where(front, pltpu.roll(first, 64, 1), second)

    def compressed(t):
        at = pl.multiple_of(t * 256, 256)
        rows = base + at + lax.broadcasted_iota(jnp.int32, (256, 1), 0)
        limit = (rows + 1) // CMP_BLOCK
        column = lax.broadcasted_iota(jnp.int32, (256, 1024), 1)
        sums = sums_ref[...].reshape(1024, 128)
        out = []
        for h in range(2):
            s = lax.dot_general(qp_ref[h, pl.ds(at, 256), :], sums, NT, preferred_element_type=jnp.float32)
            s = jnp.where(column < limit, s, NEG)
            top = jnp.maximum(jnp.max(s, axis=1, keepdims=True), -1e20)
            p = jnp.exp(s - top)
            total = jnp.maximum(jnp.sum(p, axis=1, keepdims=True), 0.5)
            o = jnp.dot(p.astype(jnp.bfloat16), sums, preferred_element_type=jnp.float32)
            out.append(o * (gate_ref[pl.ds(at, 256), h : h + 1] / total))
        mix_ref[pl.ds(at, 256), :] = join(*out)

    pl.loop(0, 4)(compressed)
    arrive("late2+", "late2-")
    start("late3+", "late3-")
    pl.loop(4, 8)(compressed)
    arrive("early+", "early-", "early3+", "early3-", "late+", "late-", "late3+", "late3-")

    triangle = lax.broadcasted_iota(jnp.int32, (128, 128), 1) <= lax.broadcasted_iota(jnp.int32, (128, 128), 0)
    ty, core = tp // 2, tp % 2

    def target_of(i):
        pair = i // 2
        dy = jnp.where(pair == 0, 2, jnp.where(pair == 1, 1, jnp.where(pair == 2, 3, 0)))
        flip = jnp.where(pair == 3, 1 - i % 2, i % 2)
        return ((ty + dy) % 4) * 2 + (core + flip) % 2

    def tp_copy(i, to):
        return pltpu.make_async_remote_copy(
            src_ref=send_ref.at[i], dst_ref=out_ref.at[:, pl.ds(pl.multiple_of(tp * 128, 128), 128)],
            send_sem=tp_send.at[i], recv_sem=tp_recv.at[i], device_id=(me, to), device_id_type=MESH,
        )

    @pl.loop(0, 8)
    def _(i):
        to = target_of(i)
        for half in range(2):
            j = to * 2 + half
            at = pl.multiple_of(j * 128, 128)
            parts = [own_ref[kind, 2 * j + b] for b in range(2) for kind in range(2)]
            bias = []
            for c in range(FAR_PICKS):
                for kind in range(2):
                    near = find_ref[16 + 16 * kind + c, me * 16 + j]
                    far = find_ref[24 + 16 * kind + c, me * 16 + j]
                    parts.append(
                        jnp.where(far < 0, ring_ref[kind, near], slot_ref[kind, jnp.maximum(far, 0)])
                    )
                bias.append(jnp.where(find_ref[48 + c, me * 16 + j] > 0, 0.0, NEG))
            keys = jnp.concatenate(parts, axis=0)
            q = jnp.concatenate([qt_ref[0, pl.ds(at, 128), :], qt_ref[1, pl.ds(at, 128), :]], axis=0)
            s = lax.dot_general(q, keys, NT, preferred_element_type=jnp.float32)
            mine = jnp.where(jnp.concatenate([triangle, triangle], axis=0), s[:, :128], NEG)
            far = [
                s[:, 128 + 128 * c : 256 + 128 * c] + jnp.where(front, bias[2 * c], bias[2 * c + 1])
                for c in range(FAR_PICKS // 2)
            ]
            s = jnp.concatenate([mine, *far], axis=1)
            p = jnp.exp(s - jnp.max(s, axis=1, keepdims=True))
            total = jnp.sum(p, axis=1, keepdims=True)
            o = jnp.dot(p.astype(jnp.bfloat16), keys, preferred_element_type=jnp.float32)
            gates = gate_ref[pl.ds(at, 128), :]
            first = o[:128] * (gates[:, 2:3] / total[:128])
            second = o[128:] * (gates[:, 3:4] / total[128:])
            mixed = (mix_ref[pl.ds(at, 128), :] + join(first, second)).astype(jnp.bfloat16)
            send_ref[i, half * 128 : half * 128 + 128, :] = mixed

            @pl.when(i == 7)
            def _():
                out_ref[half * 128 : half * 128 + 128, pl.ds(pl.multiple_of(tp * 128, 128), 128)] = mixed

        @pl.when(i < 7)
        def _():
            tp_copy(i, to).start()

    for i in range(7):
        tp_copy(i, target_of(i)).wait_recv()
    for i in range(7):
        tp_copy(i, target_of(i)).wait_send()
    for k in range(1, 16):
        sum_copy(k).wait_send()
    for name in NAMES:
        span_copy(*name).wait_send()


def layer(chosen, tokens, rest, seq):
    rows, width = tokens.shape
    args = (tokens, *rest, *rope_tables(seq))
    bf, f32 = jnp.bfloat16, jnp.float32
    spans = seq // rows
    held = [pltpu.VMEM((rows // ROWS, ROWS, width), bf)]
    held += [pltpu.VMEM(a.shape, a.dtype) for a in args[1:-2]]
    held += [pltpu.VMEM((rows // 64, 128), f32)] * 2
    entry = (32, 128)
    dma = pltpu.SemaphoreType.DMA
    return pl.pallas_call(
        layer_kernel,
        in_specs=[pl.BlockSpec(memory_space=pltpu.HBM)] * (len(args) + 1),
        out_specs=pl.BlockSpec(memory_space=pltpu.VMEM),
        out_shape=jax.ShapeDtypeStruct((rows // 8, 1024), bf),
        scratch_shapes=held + [
            pltpu.VMEM((256, width), bf),
            pltpu.VMEM((rows // ROWS, ROWS, 1), f32),
            pltpu.VMEM((rows, 128), f32),
            pltpu.VMEM((rows // CMP_BLOCK, CMP_BLOCK * 64), bf),
            pltpu.VMEM((rows // CMP_BLOCK, CMP_BLOCK * 64), bf),
            pltpu.VMEM((2, rows, 128), bf),
            pltpu.VMEM((2, rows, 128), bf),
            pltpu.VMEM((rows, 128), f32),
            pltpu.VMEM((rows // CMP_BLOCK, 128), bf),
            pltpu.VMEM((2, 32, *entry), bf),
            pltpu.VMEM((2, 128, *entry), bf),
            pltpu.VMEM((2, 192, *entry), bf),
            pltpu.VMEM((2, 64, *entry), bf),
            pltpu.VMEM((2, 192, *entry), bf),
            pltpu.VMEM(chosen.shape, jnp.int32),
            pltpu.VMEM((56, chosen.shape[-1]), jnp.int32),
            pltpu.SMEM((56, chosen.shape[-1]), jnp.int32),
            pltpu.VMEM((spans, rows // CMP_BLOCK, 128), bf),
            pltpu.VMEM((rows, 128), f32),
            pltpu.VMEM((8, rows // 8, 128), bf),
            dma((18,)), dma((rows // ROWS,)), dma, dma((len(PLAN),)), dma((len(PLAN),)),
            dma((15,)), dma((15,)), dma((7,)), dma((7,)),
        ],
        compiler_params=pltpu.CompilerParams(collective_id=0, has_side_effects=True, vmem_limit_bytes=67043328),
        name="layer",
    )(chosen, *args)


def per_device(
    tokens, norm_gain, query_weight, cmp_key_weight, cmp_value_weight, sel_key_weight, sel_value_weight,
    branch_weight, key_embed, key_inner, key_outer, value_embed, value_inner, value_outer, out_weight, chosen,
):
    seq = tokens.shape[0] * lax.axis_size("kv")
    rest = (
        norm_gain, query_weight,
        cmp_key_weight.T, cmp_value_weight.T, sel_key_weight.T, sel_value_weight.T,
        branch_weight.transpose(0, 2, 1),
        key_embed, key_inner.transpose(0, 2, 1), key_outer,
        value_embed, value_inner.transpose(0, 2, 1), value_outer,
    )
    rows = layer(chosen.transpose(0, 2, 1), tokens, rest, seq)
    return jnp.dot(rows, out_weight, preferred_element_type=jnp.float32).astype(jnp.bfloat16)


def solution(mesh):
    placed = (
        P("kv", None), P(), P(None, "tp"), P(None, "tp"), P(None, "tp"), P(None, "tp"), P(None, "tp"), P(),
        P("tp", None, None), P("tp", None, None), P("tp", None, None), P("tp", None, None), P("tp", None, None),
        P("tp", None, None), P(), P("tp", None, None),
    )
    return jax.shard_map(
        per_device, mesh=mesh, in_specs=placed, out_specs=P(("kv", "tp"), None), check_vma=False
    )
```

```python
import math

import jax
import jax.numpy as jnp
import numpy as np
from jax import lax
from jax.experimental import pallas as pl
from jax.experimental.pallas import tpu as pltpu
from jax.sharding import PartitionSpec as P

HEAD_DIM = 64
CMP_BLOCK = 32
SEL_BLOCK = 64
Q_BLOCK = 128
FAR_PICKS = 8
ROPE_BASE = 10000.0
NORM_EPS = 1e-06
MESH = pl.DeviceIdType.MESH
NT = (((1,), (1,)), ((), ()))
NEG = -1e30
ROWS = 512


def rope_tables(seq):
    half = HEAD_DIM // 2
    inverse = ROPE_BASE ** (-np.arange(half, dtype=np.float64) / half)
    lane = np.arange(128) % half
    low = np.arange(64, dtype=np.float64)[:, None] * inverse[lane][None, :]
    high = np.arange(seq // 64, dtype=np.float64)[:, None] * 64.0 * inverse[lane][None, :]
    return tuple(np.asarray(f(a), np.float32) for a in (low, high) for f in (np.cos, np.sin))


def gelu(x):
    return 0.5 * x * (1.0 + jnp.tanh(math.sqrt(2.0 / math.pi) * (x + 0.044715 * (x * x * x))))


WAYS = {0: ("x", "z"), 1: ("z", "x")}
ORDER = (0, 1, 3, 2)
VIA_PLUS = 24


def copy_plan():
    plan = {}
    for kind, (first, second) in WAYS.items():
        for part in (0, 1):
            plan[kind, f"own{part}+"] = (first + "+", "ring", 16 * part, 16, "ring", 96 + 16 * part)
            plan[kind, f"own{part}-"] = (first + "-", "ring", 16 * part, 16, "ring", 32 + 16 * part)
        plan[kind, "far+"] = (first + "+", "ring", 96, 16, "ring", 64)
        plan[kind, "far-"] = (first + "-", "ring", 48, 16, "ring", 80)
        for name, at, n, half in (("early", 0, 16, 8), ("late", 16, 48, VIA_PLUS)):
            plan[kind, name + "+"] = (second + "+", "pack", at, n, "all", 256 + at)
            plan[kind, name + "-"] = (second + "-", "pack", 128 + at, n, "all", 128 + at)
            plan[kind, name + "2+"] = (second + "+", "pack", 64 + at, half, "pass", at)
            plan[kind, name + "2-"] = (second + "-", "pack", 64 + at + half, n - half, "pass", at + half)
            plan[kind, name + "3+"] = (second + "+", "pass", at, half, "all", 192 + at)
            plan[kind, name + "3-"] = (second + "-", "pass", at + half, n - half, "all", 192 + at + half)
    return plan


PLAN = copy_plan()
NAMES = list(PLAN)


def layer_kernel(
    chosen_hbm, x_hbm, gain_hbm, qw_hbm, ck_hbm, cv_hbm, sk_hbm, sv_hbm, bw_hbm,
    ke_hbm, ki_hbm, ko_hbm, ve_hbm, vi_hbm, vo_hbm, cl_hbm, sl_hbm, ch_hbm, sh_hbm, weight_hbm,
    out_ref,
    x_ref, gain_ref, qw_ref, ck_ref, cv_ref, sk_ref, sv_ref, bw_ref,
    ke_ref, ki_ref, ko_ref, ve_ref, vi_ref, vo_ref, cl_ref, sl_ref, ch_ref, sh_ref,
    w_ref, scale_ref, bi_ref, xk_ref, xv_ref, qp_ref, qt_ref, gate_ref, sum_ref,
    own_ref, ring_ref, pack_ref, pass_ref, all_ref, chosen_ref, table_ref, find_ref,
    sums_ref, mix_ref, send_ref, rows_ref, hop_ref, weight_ref, total_ref,
    in_sem, x_sem, find_sem, weight_sem, span_send, span_recv, sum_send, sum_recv, tp_send, tp_recv,
):
    me = lax.axis_index("kv")
    tp = lax.axis_index("tp")
    mz, mx = me // 4, me % 4
    width = x_ref.shape[-1]
    steps = x_ref.shape[0]

    small = [
        (gain_hbm, gain_ref), (sk_hbm, sk_ref), (sv_hbm, sv_ref), (ck_hbm, ck_ref), (cv_hbm, cv_ref),
        (cl_hbm, cl_ref), (sl_hbm, sl_ref), (ch_hbm.at[pl.ds(me * 32, 32)], ch_ref),
        (sh_hbm.at[pl.ds(me * 32, 32)], sh_ref), (ke_hbm, ke_ref), (ve_hbm, ve_ref),
        (ki_hbm, ki_ref), (ko_hbm, ko_ref), (vi_hbm, vi_ref), (vo_hbm, vo_ref), (qw_hbm, qw_ref), (bw_hbm, bw_ref),
        (chosen_hbm, chosen_ref),
    ]
    small = [pltpu.make_async_copy(a, b, in_sem.at[i]) for i, (a, b) in enumerate(small)]
    rows_in = [pltpu.make_async_copy(x_hbm.at[pl.ds(i * ROWS, ROWS)], x_ref.at[i], x_sem.at[i]) for i in range(steps)]
    small[17].start()
    for copy in small[:9]:
        copy.start()
    for copy in rows_in:
        copy.start()
    for copy in small[9:17]:
        copy.start()

    weight = pltpu.make_async_copy(weight_hbm, weight_ref, weight_sem)
    weight.start()

    barrier = pltpu.get_barrier_semaphore()
    for k in range(1, 16):
        pl.semaphore_signal(barrier, inc=1, device_id=((me + k) % 16, tp), device_id_type=MESH)
    for k in range(1, 8):
        pl.semaphore_signal(barrier, inc=1, device_id=(me, (tp + k) % 8), device_id_type=MESH)

    lane = lax.broadcasted_iota(jnp.int32, (1, 128), 1)
    front = lane < 64
    flip = lane % 64 < 32
    sign = jnp.where(flip, -1.0, 1.0)

    small[17].wait()
    block = chosen_ref[0]
    query = lax.broadcasted_iota(jnp.int32, block.shape, 1)
    for s in range(16):
        table_ref[s : s + 1, :] = jnp.sum(jnp.where(block // 32 == s, block % 32, 0), axis=0, keepdims=True)
    usable = block * SEL_BLOCK < query * Q_BLOCK
    rz = (block // 128 + 4 - mz) % 4
    rx = (block // 32 % 4 + 4 - mx) % 4
    for row, r_first, r_second in ((16, rx, rz), (24, rz, rx)):
        place = jnp.where(r_first < 2, r_first, 5 - r_first)
        at = jnp.where(r_second == 0, r_first * 32 + block % 32, 64 + r_second * 64 + place * 16 + query % 16)
        table_ref[row : row + 8, :] = jnp.where(usable, at, -1)
    find = pltpu.make_async_copy(table_ref, find_ref, find_sem)
    find.start()

    def angles(step):
        cos, sin = [], []
        low_c, low_s = cl_ref[...], sl_ref[...]
        for g in range(ROWS // 64):
            hc = ch_ref[pl.ds(step * (ROWS // 64) + g, 1), :]
            hs = sh_ref[pl.ds(step * (ROWS // 64) + g, 1), :]
            cos.append(low_c * hc - low_s * hs)
            sin.append(low_c * (hs * sign) + low_s * (hc * sign))
        return jnp.concatenate(cos, axis=0), jnp.concatenate(sin, axis=0)

    def turn(v, c, s):
        swapped = jnp.where(flip, pltpu.roll(v, 96, 1), pltpu.roll(v, 32, 1))
        return v * c + swapped * s

    for copy in small[:9]:
        copy.wait()
    gain = gain_ref[...].astype(jnp.float32).reshape(1, width)
    for at, ref in ((0, sk_ref), (64, sv_ref), (128, ck_ref), (192, cv_ref)):
        w_ref[at : at + 64, :] = (ref[...].astype(jnp.float32) * gain).astype(jnp.bfloat16)
    for copy in small[9:11]:
        copy.wait()
    embed = jnp.concatenate([ke_ref[0], ve_ref[0]], axis=1).astype(jnp.float32)
    embed = jnp.concatenate([embed] * (ROWS // CMP_BLOCK), axis=0)

    def keys_and_values(step):
        pltpu.make_async_copy(
            x_hbm.at[pl.ds(pl.multiple_of(step * ROWS, ROWS), ROWS)], x_ref.at[step], x_sem.at[step]
        ).wait()
        x = x_ref[step]
        xf = x.astype(jnp.float32)
        scale = lax.rsqrt(jnp.sum(xf * xf, axis=1, keepdims=True) * (1.0 / width) + NORM_EPS)
        scale_ref[step] = scale
        y = lax.dot_general(x, w_ref[...], NT, preferred_element_type=jnp.float32) * scale
        cos, sin = angles(step)
        kv = turn(y[:, 0:128], jnp.where(front, cos, 1.0), jnp.where(front, sin, 0.0)).astype(jnp.bfloat16)
        kv = kv.reshape(ROWS // 64, 2, 32, 128)
        for kind in range(2):
            own_ref[kind, pl.ds(step * (ROWS // 64), ROWS // 64)] = kv[:, kind]
            ring_ref[kind, pl.ds(step * (ROWS // 64), ROWS // 64)] = kv[:, kind]
        raw = y[:, 128:256].astype(jnp.bfloat16).astype(jnp.float32)
        bi_ref[pl.ds(pl.multiple_of(step * ROWS, ROWS), ROWS), :] = raw + embed

    step_to = {
        "x+": (mz * 4 + (mx + 1) % 4, tp),
        "x-": (mz * 4 + (mx + 3) % 4, tp),
        "z+": (((mz + 1) % 4) * 4 + mx, tp),
        "z-": (((mz + 3) % 4) * 4 + mx, tp),
    }

    def sum_copy(k):
        return pltpu.make_async_remote_copy(
            src_ref=sum_ref, dst_ref=sums_ref.at[me], send_sem=sum_send.at[k - 1], recv_sem=sum_recv.at[k - 1],
            device_id=((me + k) % 16, tp), device_id_type=MESH,
        )

    refs = {"ring": ring_ref, "pack": pack_ref, "pass": pass_ref, "all": all_ref}

    def span_copy(*name):
        way, source, at, n, target, to = PLAN[name]
        i = NAMES.index(name)
        return pltpu.make_async_remote_copy(
            src_ref=refs[source].at[name[0], pl.ds(at, n)], dst_ref=refs[target].at[name[0], pl.ds(to, n)],
            send_sem=span_send.at[i], recv_sem=span_recv.at[i], device_id=step_to[way], device_id_type=MESH,
        )

    def start(*names):
        for name in names:
            for kind in range(2):
                span_copy(kind, name).start()

    def arrive(*names):
        for name in names:
            for kind in range(2):
                span_copy(kind, name).wait_recv()

    def pack(targets, places, source):
        @pl.loop(0, 16, unroll=2)
        def _(j):
            for kind in range(2):
                for e in targets:
                    d = e + 1
                    to = ((mz + d) % 4) * 4 + mx if kind == 0 else mz * 4 + (mx + d) % 4
                    for place in places:
                        r = ORDER[place]
                        span = mz * 4 + (mx + r) % 4 if kind == 0 else ((mz + r) % 4) * 4 + mx
                        wanted = find_ref[span, to * 16 + j]
                        pack_ref[kind, e * 64 + place * 16 + j] = source[kind, r * 32 + wanted]

    pl.loop(0, steps // 2)(keys_and_values)
    pl.semaphore_wait(barrier, 22)
    start("own0+", "own0-")
    pl.loop(steps // 2, steps)(keys_and_values)
    start("own1+", "own1-")
    find.wait()
    pack((0, 1, 2), (0,), own_ref)
    start("early+", "early-")

    for copy in small[11:17]:
        copy.wait()
    count = bi_ref.shape[0] // CMP_BLOCK
    for t in range(0, CMP_BLOCK, 2):
        a = bi_ref[pl.ds(t, count, stride=CMP_BLOCK), :]
        b = bi_ref[pl.ds(t + 1, count, stride=CMP_BLOCK), :]
        xk_ref[:, t * 64 : t * 64 + 128] = jnp.where(front, a, pltpu.roll(b, 64, 1)).astype(jnp.bfloat16)
        xv_ref[:, t * 64 : t * 64 + 128] = jnp.where(front, pltpu.roll(a, 64, 1), b).astype(jnp.bfloat16)
    summary = []
    for x_in, inner, outer in ((xk_ref, ki_ref, ko_ref), (xv_ref, vi_ref, vo_ref)):
        hidden = lax.dot_general(x_in[...], inner[0], NT, preferred_element_type=jnp.float32)
        hidden = gelu(hidden).astype(jnp.bfloat16)
        summary.append(jnp.dot(hidden, outer[0], preferred_element_type=jnp.float32))
    summary = jnp.concatenate(summary, axis=1).astype(jnp.bfloat16)
    sum_ref[...] = summary
    sums_ref[me] = summary

    w_ref[0:128, :] = (qw_ref[...].astype(jnp.float32).T * gain).astype(jnp.bfloat16)
    r = lax.broadcasted_iota(jnp.int32, (128, 32), 0)
    c = lax.broadcasted_iota(jnp.int32, (128, 32), 1)
    want = jnp.where(r < 2, tp * 2 + r, 16 + tp * 2 + (r - 2))
    pick = jnp.where((r < 4) & (c == want), 1.0, 0.0).astype(jnp.bfloat16)
    gates = jnp.dot(pick, bw_ref[...].reshape(32, width), preferred_element_type=jnp.float32)
    w_ref[128:256, :] = (gates * gain).astype(jnp.bfloat16)
    for k in range(1, 16):
        sum_copy(k).start()

    arrive("own0+", "own0-", "own1+", "own1-")
    start("far+", "far-", "early2+", "early2-")

    def by_head(v):
        v = v * (HEAD_DIM**-0.5)
        first = jnp.where(front, v, 0.0)
        second = jnp.where(front, pltpu.roll(v, 64, 1), 0.0)
        return jnp.stack([first, second]).astype(jnp.bfloat16)

    @pl.loop(0, steps)
    def _(step):
        y = lax.dot_general(x_ref[step], w_ref[...], NT, preferred_element_type=jnp.float32) * scale_ref[step]
        at = pl.ds(pl.multiple_of(step * ROWS, ROWS), ROWS)
        q = y[:, 0:128]
        qp_ref[:, at, :] = by_head(q)
        qt_ref[:, at, :] = by_head(turn(q, *angles(step)))
        gate_ref[at, :] = 1.0 / (1.0 + jnp.exp(-y[:, 128:256]))

    arrive("far+", "far-")
    pack((1,), (1, 2, 3), ring_ref)
    start("late2+", "late2-")
    arrive("early2+", "early2-")
    start("early3+", "early3-")
    pack((0,), (1, 2, 3), ring_ref)
    start("late+")
    pack((2,), (1, 2, 3), ring_ref)
    start("late-")
    for kind in range(2):
        all_ref[kind, 0:128] = ring_ref[kind]
    for k in range(1, 16):
        sum_copy(k).wait_recv()

    base = me * 2048

    def join(first, second):
        return jnp.where(front, pltpu.roll(first, 64, 1), second)

    def compressed(t):
        at = pl.multiple_of(t * 256, 256)
        rows = base + at + lax.broadcasted_iota(jnp.int32, (256, 1), 0)
        limit = (rows + 1) // CMP_BLOCK
        column = lax.broadcasted_iota(jnp.int32, (256, 1024), 1)
        sums = sums_ref[...].reshape(1024, 128)
        out = []
        for h in range(2):
            s = lax.dot_general(qp_ref[h, pl.ds(at, 256), :], sums, NT, preferred_element_type=jnp.float32)
            s = jnp.where(column < limit, s, NEG)
            top = jnp.maximum(jnp.max(s, axis=1, keepdims=True), -1e20)
            p = jnp.exp(s - top)
            total = jnp.maximum(jnp.sum(p, axis=1, keepdims=True), 0.5)
            o = jnp.dot(p.astype(jnp.bfloat16), sums, preferred_element_type=jnp.float32)
            out.append(o * (gate_ref[pl.ds(at, 256), h : h + 1] / total))
        mix_ref[pl.ds(at, 256), :] = join(*out)

    pl.loop(0, 4)(compressed)
    arrive("late2+", "late2-")
    start("late3+", "late3-")
    pl.loop(4, 8)(compressed)
    arrive("early+", "early-", "early3+", "early3-", "late+", "late-", "late3+", "late3-")

    triangle = lax.broadcasted_iota(jnp.int32, (128, 128), 1) <= lax.broadcasted_iota(jnp.int32, (128, 128), 0)
    ty, core = tp // 2, tp % 2

    def target_of(i):
        pair = i // 2
        dy = jnp.where(pair == 0, 2, jnp.where(pair == 1, 1, jnp.where(pair == 2, 3, 0)))
        flip = jnp.where(pair == 3, 1 - i % 2, i % 2)
        return ((ty + dy) % 4) * 2 + (core + flip) % 2

    def lanes_of(t):
        return pl.ds(pl.multiple_of(t * 128, 128), 128)

    def tp_copy(i, to):
        return pltpu.make_async_remote_copy(
            src_ref=send_ref.at[i], dst_ref=rows_ref.at[:, lanes_of(tp)],
            send_sem=tp_send.at[i], recv_sem=tp_recv.at[i], device_id=(me, to), device_id_type=MESH,
        )

    def direct_copy(i):
        return pltpu.make_async_remote_copy(
            src_ref=send_ref.at[i, pl.ds(0, 128)], dst_ref=rows_ref.at[pl.ds(0, 128), lanes_of(tp)],
            send_sem=tp_send.at[i], recv_sem=tp_recv.at[i], device_id=(me, target_of(i)), device_id_type=MESH,
        )

    def hop_copy(i):
        return pltpu.make_async_remote_copy(
            src_ref=send_ref.at[i, pl.ds(128, 128)], dst_ref=hop_ref.at[i],
            send_sem=tp_send.at[7 + i], recv_sem=tp_recv.at[7 + i],
            device_id=(me, (ty + 3) % 4 * 2 + core), device_id_type=MESH,
        )

    def relay_copy(i):
        return pltpu.make_async_remote_copy(
            src_ref=hop_ref.at[i], dst_ref=rows_ref.at[pl.ds(128, 128), lanes_of((ty + 1) % 4 * 2 + core)],
            send_sem=tp_send.at[9 + i], recv_sem=tp_recv.at[9 + i],
            device_id=(me, (ty + 3) % 4 * 2 + (core + i) % 2), device_id_type=MESH,
        )

    @pl.loop(0, 8)
    def _(i):
        to = target_of(i)
        for half in range(2):
            j = to * 2 + half
            at = pl.multiple_of(j * 128, 128)
            parts = [own_ref[kind, 2 * j + b] for b in range(2) for kind in range(2)]
            bias = []
            for c in range(FAR_PICKS):
                places = [find_ref[16 + 8 * kind + c, me * 16 + j] for kind in range(2)]
                parts += [all_ref[kind, jnp.maximum(places[kind], 0)] for kind in range(2)]
                bias.append(jnp.where(places[0] < 0, NEG, 0.0))
            keys = jnp.concatenate(parts, axis=0)
            q = jnp.concatenate([qt_ref[0, pl.ds(at, 128), :], qt_ref[1, pl.ds(at, 128), :]], axis=0)
            s = lax.dot_general(q, keys, NT, preferred_element_type=jnp.float32)
            mine = jnp.where(jnp.concatenate([triangle, triangle], axis=0), s[:, :128], NEG)
            far = [
                s[:, 128 + 128 * c : 256 + 128 * c] + jnp.where(front, bias[2 * c], bias[2 * c + 1])
                for c in range(FAR_PICKS // 2)
            ]
            s = jnp.concatenate([mine, *far], axis=1)
            p = jnp.exp(s - jnp.max(s, axis=1, keepdims=True))
            total = jnp.sum(p, axis=1, keepdims=True)
            o = jnp.dot(p.astype(jnp.bfloat16), keys, preferred_element_type=jnp.float32)
            gates = gate_ref[pl.ds(at, 128), :]
            first = o[:128] * (gates[:, 2:3] / total[:128])
            second = o[128:] * (gates[:, 3:4] / total[128:])
            mixed = (mix_ref[pl.ds(at, 128), :] + join(first, second)).astype(jnp.bfloat16)
            send_ref[i, half * 128 : half * 128 + 128, :] = mixed

            @pl.when(i == 7)
            def _():
                rows_ref[half * 128 : half * 128 + 128, lanes_of(tp)] = mixed

        for two in range(2):

            @pl.when(i == two)
            def _():
                direct_copy(two).start()
                hop_copy(two).start()

        @pl.when((i > 1) & (i < 7))
        def _():
            tp_copy(i, to).start()

        @pl.when(i == 4)
        def _():
            for two in range(2):
                hop_copy(two).wait_recv()
                relay_copy(two).start()

    weight.wait()
    for pair, away in ((1, 1), (2, 3), (3, 0), (0, 2)):
        if pair == 0:
            for i in range(2):
                direct_copy(i).wait_recv()
                relay_copy(i).wait_recv()
        else:
            for i in range(2 * pair, min(2 * pair + 2, 7)):
                tp_copy(i, target_of(i)).wait_recv()
        at = pl.ds(pl.multiple_of((ty + 4 - away) % 4 * 256, 256), 256)
        part = jnp.dot(rows_ref[:, at], weight_ref[at, :], preferred_element_type=jnp.float32)
        if pair == 1:
            total_ref[...] = part
        elif pair:
            total_ref[...] += part
        else:
            out_ref[...] = (total_ref[...] + part).astype(out_ref.dtype)

    for i in range(2):
        direct_copy(i).wait_send()
        hop_copy(i).wait_send()
        relay_copy(i).wait_send()
    for i in range(2, 7):
        tp_copy(i, target_of(i)).wait_send()
    for k in range(1, 16):
        sum_copy(k).wait_send()
    for name in NAMES:
        span_copy(*name).wait_send()


def layer(chosen, tokens, rest, out_weight, seq):
    rows, width = tokens.shape
    args = (tokens, *rest, *rope_tables(seq))
    bf, f32 = jnp.bfloat16, jnp.float32
    spans = seq // rows
    held = [pltpu.VMEM((rows // ROWS, ROWS, width), bf)]
    held += [pltpu.VMEM(a.shape, a.dtype) for a in args[1:-2]]
    held += [pltpu.VMEM((rows // 64, 128), f32)] * 2
    entry = (32, 128)
    dma = pltpu.SemaphoreType.DMA
    return pl.pallas_call(
        layer_kernel,
        in_specs=[pl.BlockSpec(memory_space=pltpu.HBM)] * (len(args) + 2),
        out_specs=pl.BlockSpec(memory_space=pltpu.VMEM),
        out_shape=jax.ShapeDtypeStruct((rows // 8, width), bf),
        scratch_shapes=held + [
            pltpu.VMEM((256, width), bf),
            pltpu.VMEM((rows // ROWS, ROWS, 1), f32),
            pltpu.VMEM((rows, 128), f32),
            pltpu.VMEM((rows // CMP_BLOCK, CMP_BLOCK * 64), bf),
            pltpu.VMEM((rows // CMP_BLOCK, CMP_BLOCK * 64), bf),
            pltpu.VMEM((2, rows, 128), bf),
            pltpu.VMEM((2, rows, 128), bf),
            pltpu.VMEM((rows, 128), f32),
            pltpu.VMEM((rows // CMP_BLOCK, 128), bf),
            pltpu.VMEM((2, 32, *entry), bf),
            pltpu.VMEM((2, 128, *entry), bf),
            pltpu.VMEM((2, 192, *entry), bf),
            pltpu.VMEM((2, 64, *entry), bf),
            pltpu.VMEM((2, 320, *entry), bf),
            pltpu.VMEM(chosen.shape, jnp.int32),
            pltpu.VMEM((32, chosen.shape[-1]), jnp.int32),
            pltpu.SMEM((32, chosen.shape[-1]), jnp.int32),
            pltpu.VMEM((spans, rows // CMP_BLOCK, 128), bf),
            pltpu.VMEM((rows, 128), f32),
            pltpu.VMEM((8, rows // 8, 128), bf),
            pltpu.VMEM((rows // 8, 1024), bf),
            pltpu.VMEM((2, 128, 128), bf),
            pltpu.VMEM(out_weight.shape, bf),
            pltpu.VMEM((rows // 8, width), f32),
            dma((18,)), dma((rows // ROWS,)), dma, dma, dma((len(PLAN),)), dma((len(PLAN),)),
            dma((15,)), dma((15,)), dma((11,)), dma((11,)),
        ],
        compiler_params=pltpu.CompilerParams(collective_id=0, has_side_effects=True, vmem_limit_bytes=67043328),
        name="layer",
    )(chosen, *args, out_weight)


def per_device(
    tokens, norm_gain, query_weight, cmp_key_weight, cmp_value_weight, sel_key_weight, sel_value_weight,
    branch_weight, key_embed, key_inner, key_outer, value_embed, value_inner, value_outer, out_weight, chosen,
):
    seq = tokens.shape[0] * lax.axis_size("kv")
    rest = (
        norm_gain, query_weight,
        cmp_key_weight.T, cmp_value_weight.T, sel_key_weight.T, sel_value_weight.T,
        branch_weight.transpose(0, 2, 1),
        key_embed, key_inner.transpose(0, 2, 1), key_outer,
        value_embed, value_inner.transpose(0, 2, 1), value_outer,
    )
    return layer(chosen.transpose(0, 2, 1), tokens, rest, out_weight, seq)


def solution(mesh):
    placed = (
        P("kv", None), P(), P(None, "tp"), P(None, "tp"), P(None, "tp"), P(None, "tp"), P(None, "tp"), P(),
        P("tp", None, None), P("tp", None, None), P("tp", None, None), P("tp", None, None), P("tp", None, None),
        P("tp", None, None), P(), P("tp", None, None),
    )
    return jax.shard_map(
        per_device, mesh=mesh, in_specs=placed, out_specs=P(("kv", "tp"), None), check_vma=False
    )
```

```python
import math

import jax
import jax.numpy as jnp
import numpy as np
from jax import lax
from jax.experimental import pallas as pl
from jax.experimental.pallas import tpu as pltpu
from jax.sharding import PartitionSpec as P

HEAD_DIM = 64
CMP_BLOCK = 32
SEL_BLOCK = 64
Q_BLOCK = 128
FAR_PICKS = 8
ROPE_BASE = 10000.0
NORM_EPS = 1e-06
MESH = pl.DeviceIdType.MESH
NT = (((1,), (1,)), ((), ()))
NEG = -1e30
ROWS = 512


def rope_tables(seq):
    half = HEAD_DIM // 2
    inverse = ROPE_BASE ** (-np.arange(half, dtype=np.float64) / half)
    lane = np.arange(128) % half
    low = np.arange(64, dtype=np.float64)[:, None] * inverse[lane][None, :]
    high = np.arange(seq // 64, dtype=np.float64)[:, None] * 64.0 * inverse[lane][None, :]
    return tuple(np.asarray(f(a), np.float32) for a in (low, high) for f in (np.cos, np.sin))


def gelu(x):
    return 0.5 * x * (1.0 + jnp.tanh(math.sqrt(2.0 / math.pi) * (x + 0.044715 * (x * x * x))))


WAYS = {0: ("x", "z"), 1: ("z", "x")}
ORDER = (0, 1, 3, 2)
VIA_PLUS = 24


def copy_plan():
    plan = {}
    for kind, (first, second) in WAYS.items():
        for part in (0, 1):
            plan[kind, f"own{part}+"] = (first + "+", "ring", 16 * part, 16, "ring", 96 + 16 * part)
            plan[kind, f"own{part}-"] = (first + "-", "ring", 16 * part, 16, "ring", 32 + 16 * part)
        plan[kind, "far+"] = (first + "+", "ring", 96, 16, "ring", 64)
        plan[kind, "far-"] = (first + "-", "ring", 48, 16, "ring", 80)
        for name, at, n, half in (("early", 0, 16, 8), ("late", 16, 48, VIA_PLUS)):
            plan[kind, name + "+"] = (second + "+", "pack", at, n, "all", 256 + at)
            plan[kind, name + "-"] = (second + "-", "pack", 128 + at, n, "all", 128 + at)
            plan[kind, name + "2+"] = (second + "+", "pack", 64 + at, half, "pass", at)
            plan[kind, name + "2-"] = (second + "-", "pack", 64 + at + half, n - half, "pass", at + half)
            plan[kind, name + "3+"] = (second + "+", "pass", at, half, "all", 192 + at)
            plan[kind, name + "3-"] = (second + "-", "pass", at + half, n - half, "all", 192 + at + half)
    return plan


PLAN = copy_plan()
NAMES = list(PLAN)


def layer_kernel(
    chosen_hbm, x_hbm, gain_hbm, qw_hbm, ck_hbm, cv_hbm, sk_hbm, sv_hbm, bw_hbm,
    ke_hbm, ki_hbm, ko_hbm, ve_hbm, vi_hbm, vo_hbm, cl_hbm, sl_hbm, ch_hbm, sh_hbm, weight_hbm,
    out_ref,
    x_ref, gain_ref, qw_ref, ck_ref, cv_ref, sk_ref, sv_ref, bw_ref,
    ke_ref, ki_ref, ko_ref, ve_ref, vi_ref, vo_ref, cl_ref, sl_ref, ch_ref, sh_ref,
    w_ref, scale_ref, bi_ref, xk_ref, xv_ref, qp_ref, qt_ref, gate_ref, sum_ref,
    own_ref, ring_ref, pack_ref, pass_ref, all_ref, chosen_ref, table_ref, find_ref,
    sums_ref, mix_ref, send_ref, rows_ref, hop_ref, weight_ref, total_ref,
    in_sem, x_sem, find_sem, weight_sem, span_send, span_recv, sum_send, sum_recv, tp_send, tp_recv,
):
    me = lax.axis_index("kv")
    tp = lax.axis_index("tp")
    mz, mx = me // 4, me % 4
    width = x_ref.shape[-1]
    steps = x_ref.shape[0]

    small = [
        (gain_hbm, gain_ref), (sk_hbm, sk_ref), (sv_hbm, sv_ref), (ck_hbm, ck_ref), (cv_hbm, cv_ref),
        (cl_hbm, cl_ref), (sl_hbm, sl_ref), (ch_hbm.at[pl.ds(me * 32, 32)], ch_ref),
        (sh_hbm.at[pl.ds(me * 32, 32)], sh_ref), (ke_hbm, ke_ref), (ve_hbm, ve_ref),
        (ki_hbm, ki_ref), (ko_hbm, ko_ref), (vi_hbm, vi_ref), (vo_hbm, vo_ref), (qw_hbm, qw_ref), (bw_hbm, bw_ref),
        (chosen_hbm, chosen_ref),
    ]
    small = [pltpu.make_async_copy(a, b, in_sem.at[i]) for i, (a, b) in enumerate(small)]
    rows_in = [pltpu.make_async_copy(x_hbm.at[pl.ds(i * ROWS, ROWS)], x_ref.at[i], x_sem.at[i]) for i in range(steps)]
    small[17].start()
    for copy in small[:9]:
        copy.start()
    for copy in rows_in:
        copy.start()
    for copy in small[9:17]:
        copy.start()

    weight = pltpu.make_async_copy(weight_hbm, weight_ref, weight_sem)
    weight.start()

    barrier = pltpu.get_barrier_semaphore()
    for k in range(1, 16):
        pl.semaphore_signal(barrier, inc=1, device_id=((me + k) % 16, tp), device_id_type=MESH)
    for k in range(1, 8):
        pl.semaphore_signal(barrier, inc=1, device_id=(me, (tp + k) % 8), device_id_type=MESH)

    lane = lax.broadcasted_iota(jnp.int32, (1, 128), 1)
    front = lane < 64
    flip = lane % 64 < 32
    sign = jnp.where(flip, -1.0, 1.0)

    small[17].wait()
    block = chosen_ref[0]
    query = lax.broadcasted_iota(jnp.int32, block.shape, 1)
    for s in range(16):
        table_ref[s : s + 1, :] = jnp.sum(jnp.where(block // 32 == s, block % 32, 0), axis=0, keepdims=True)
    usable = block * SEL_BLOCK < query * Q_BLOCK
    rz = (block // 128 + 4 - mz) % 4
    rx = (block // 32 % 4 + 4 - mx) % 4
    for row, r_first, r_second in ((16, rx, rz), (24, rz, rx)):
        place = jnp.where(r_first < 2, r_first, 5 - r_first)
        at = jnp.where(r_second == 0, r_first * 32 + block % 32, 64 + r_second * 64 + place * 16 + query % 16)
        table_ref[row : row + 8, :] = jnp.where(usable, at, -1)
    find = pltpu.make_async_copy(table_ref, find_ref, find_sem)
    find.start()

    def angles(step):
        cos, sin = [], []
        low_c, low_s = cl_ref[...], sl_ref[...]
        for g in range(ROWS // 64):
            hc = ch_ref[pl.ds(step * (ROWS // 64) + g, 1), :]
            hs = sh_ref[pl.ds(step * (ROWS // 64) + g, 1), :]
            cos.append(low_c * hc - low_s * hs)
            sin.append(low_c * (hs * sign) + low_s * (hc * sign))
        return jnp.concatenate(cos, axis=0), jnp.concatenate(sin, axis=0)

    def turn(v, c, s):
        swapped = jnp.where(flip, pltpu.roll(v, 96, 1), pltpu.roll(v, 32, 1))
        return v * c + swapped * s

    for copy in small[:9]:
        copy.wait()
    gain = gain_ref[...].astype(jnp.float32).reshape(1, width)
    for at, ref in ((0, sk_ref), (64, sv_ref), (128, ck_ref), (192, cv_ref)):
        w_ref[at : at + 64, :] = (ref[...].astype(jnp.float32) * gain).astype(jnp.bfloat16)
    for copy in small[9:11]:
        copy.wait()
    embed = jnp.concatenate([ke_ref[0], ve_ref[0]], axis=1).astype(jnp.float32)
    embed = jnp.concatenate([embed] * (ROWS // CMP_BLOCK), axis=0)

    def keys_and_values(step):
        pltpu.make_async_copy(
            x_hbm.at[pl.ds(pl.multiple_of(step * ROWS, ROWS), ROWS)], x_ref.at[step], x_sem.at[step]
        ).wait()
        x = x_ref[step]
        xf = x.astype(jnp.float32)
        scale = lax.rsqrt(jnp.sum(xf * xf, axis=1, keepdims=True) * (1.0 / width) + NORM_EPS)
        scale_ref[step] = scale
        y = lax.dot_general(x, w_ref[...], NT, preferred_element_type=jnp.float32) * scale
        cos, sin = angles(step)
        kv = turn(y[:, 0:128], jnp.where(front, cos, 1.0), jnp.where(front, sin, 0.0)).astype(jnp.bfloat16)
        kv = kv.reshape(ROWS // 64, 2, 32, 128)
        for kind in range(2):
            own_ref[kind, pl.ds(step * (ROWS // 64), ROWS // 64)] = kv[:, kind]
            ring_ref[kind, pl.ds(step * (ROWS // 64), ROWS // 64)] = kv[:, kind]
        raw = y[:, 128:256].astype(jnp.bfloat16).astype(jnp.float32)
        bi_ref[pl.ds(pl.multiple_of(step * ROWS, ROWS), ROWS), :] = raw + embed

    step_to = {
        "x+": (mz * 4 + (mx + 1) % 4, tp),
        "x-": (mz * 4 + (mx + 3) % 4, tp),
        "z+": (((mz + 1) % 4) * 4 + mx, tp),
        "z-": (((mz + 3) % 4) * 4 + mx, tp),
    }

    def sum_copy(k):
        return pltpu.make_async_remote_copy(
            src_ref=sum_ref, dst_ref=sums_ref.at[me], send_sem=sum_send.at[k - 1], recv_sem=sum_recv.at[k - 1],
            device_id=((me + k) % 16, tp), device_id_type=MESH,
        )

    refs = {"ring": ring_ref, "pack": pack_ref, "pass": pass_ref, "all": all_ref}

    def span_copy(*name):
        way, source, at, n, target, to = PLAN[name]
        i = NAMES.index(name)
        return pltpu.make_async_remote_copy(
            src_ref=refs[source].at[name[0], pl.ds(at, n)], dst_ref=refs[target].at[name[0], pl.ds(to, n)],
            send_sem=span_send.at[i], recv_sem=span_recv.at[i], device_id=step_to[way], device_id_type=MESH,
        )

    def start(*names):
        for name in names:
            for kind in range(2):
                span_copy(kind, name).start()

    def arrive(*names):
        for name in names:
            for kind in range(2):
                span_copy(kind, name).wait_recv()

    def pack(targets, places, source):
        @pl.loop(0, 16, unroll=2)
        def _(j):
            for kind in range(2):
                for e in targets:
                    d = e + 1
                    to = ((mz + d) % 4) * 4 + mx if kind == 0 else mz * 4 + (mx + d) % 4
                    for place in places:
                        r = ORDER[place]
                        span = mz * 4 + (mx + r) % 4 if kind == 0 else ((mz + r) % 4) * 4 + mx
                        wanted = find_ref[span, to * 16 + j]
                        pack_ref[kind, e * 64 + place * 16 + j] = source[kind, r * 32 + wanted]

    pl.loop(0, steps // 2)(keys_and_values)
    pl.semaphore_wait(barrier, 22)
    start("own0+", "own0-")
    pl.loop(steps // 2, steps)(keys_and_values)
    start("own1+", "own1-")
    find.wait()
    pack((0, 1, 2), (0,), own_ref)
    start("early+", "early-")

    for copy in small[11:17]:
        copy.wait()
    count = bi_ref.shape[0] // CMP_BLOCK
    for t in range(0, CMP_BLOCK, 2):
        a = bi_ref[pl.ds(t, count, stride=CMP_BLOCK), :]
        b = bi_ref[pl.ds(t + 1, count, stride=CMP_BLOCK), :]
        xk_ref[:, t * 64 : t * 64 + 128] = jnp.where(front, a, pltpu.roll(b, 64, 1)).astype(jnp.bfloat16)
        xv_ref[:, t * 64 : t * 64 + 128] = jnp.where(front, pltpu.roll(a, 64, 1), b).astype(jnp.bfloat16)
    summary = []
    for x_in, inner, outer in ((xk_ref, ki_ref, ko_ref), (xv_ref, vi_ref, vo_ref)):
        hidden = lax.dot_general(x_in[...], inner[0], NT, preferred_element_type=jnp.float32)
        hidden = gelu(hidden).astype(jnp.bfloat16)
        summary.append(jnp.dot(hidden, outer[0], preferred_element_type=jnp.float32))
    summary = jnp.concatenate(summary, axis=1).astype(jnp.bfloat16)
    sum_ref[...] = summary
    sums_ref[me] = summary

    w_ref[0:128, :] = (qw_ref[...].astype(jnp.float32).T * gain).astype(jnp.bfloat16)
    r = lax.broadcasted_iota(jnp.int32, (128, 32), 0)
    c = lax.broadcasted_iota(jnp.int32, (128, 32), 1)
    want = jnp.where(r < 2, tp * 2 + r, 16 + tp * 2 + (r - 2))
    pick = jnp.where((r < 4) & (c == want), 1.0, 0.0).astype(jnp.bfloat16)
    gates = jnp.dot(pick, bw_ref[...].reshape(32, width), preferred_element_type=jnp.float32)
    w_ref[128:256, :] = (gates * gain).astype(jnp.bfloat16)

    arrive("own0+", "own0-", "own1+", "own1-")
    start("far+", "far-", "early2+", "early2-")
    for k in range(1, 16):
        sum_copy(k).start()

    def by_head(v):
        v = v * (HEAD_DIM**-0.5 * math.log2(math.e))
        first = jnp.where(front, v, 0.0)
        second = jnp.where(front, pltpu.roll(v, 64, 1), 0.0)
        return jnp.stack([first, second]).astype(jnp.bfloat16)

    @pl.loop(0, steps)
    def _(step):
        y = lax.dot_general(x_ref[step], w_ref[...], NT, preferred_element_type=jnp.float32) * scale_ref[step]
        at = pl.ds(pl.multiple_of(step * ROWS, ROWS), ROWS)
        q = y[:, 0:128]
        qp_ref[:, at, :] = by_head(q)
        qt_ref[:, at, :] = by_head(turn(q, *angles(step)))
        gates = 1.0 / (1.0 + jnp.exp(-y[:, 128:256]))
        for branch in range(2):
            gate_ref[branch, at, :] = jnp.where(
                front, gates[:, 2 * branch : 2 * branch + 1], gates[:, 2 * branch + 1 : 2 * branch + 2]
            )

    arrive("far+", "far-")
    pack((1,), (1, 2, 3), ring_ref)
    start("late2+", "late2-")
    arrive("early2+", "early2-")
    start("early3+", "early3-")
    pack((0,), (1, 2, 3), ring_ref)
    start("late+")
    pack((2,), (1, 2, 3), ring_ref)
    start("late-")
    for kind in range(2):
        all_ref[kind, 0:128] = ring_ref[kind]
    for k in range(1, 16):
        sum_copy(k).wait_recv()

    base = me * 2048

    def with_totals(keys):
        return jnp.where(front, jnp.ones((), jnp.bfloat16), keys)

    def join(first, second):
        value = jnp.where(front, pltpu.roll(first, 64, 1), second)
        total = jnp.where(front, first, pltpu.roll(second, 64, 1))
        return value / jnp.maximum(total, 0.5)

    def compressed(t):
        at = pl.multiple_of(t * 256, 256)
        rows = base + at + lax.broadcasted_iota(jnp.int32, (256, 1), 0)
        limit = (rows + 1) // CMP_BLOCK
        column = lax.broadcasted_iota(jnp.int32, (256, 1024), 1)
        sums = sums_ref[...].reshape(1024, 128)
        out = []
        for h in range(2):
            s = lax.dot_general(qp_ref[h, pl.ds(at, 256), :], sums, NT, preferred_element_type=jnp.float32)
            s = jnp.where(column < limit, s, NEG)
            p = jnp.exp2(s - jnp.maximum(jnp.max(s, axis=1, keepdims=True), -1e20)).astype(jnp.bfloat16)
            out.append(jnp.dot(p, with_totals(sums), preferred_element_type=jnp.float32))
        mix_ref[pl.ds(at, 256), :] = join(*out) * gate_ref[0, pl.ds(at, 256), :]

    pl.loop(0, 4)(compressed)
    arrive("late2+", "late2-")
    start("late3+", "late3-")
    pl.loop(4, 8)(compressed)
    arrive("early+", "early-", "early3+", "early3-", "late+", "late-", "late3+", "late3-")

    triangle = lax.broadcasted_iota(jnp.int32, (128, 128), 1) <= lax.broadcasted_iota(jnp.int32, (128, 128), 0)
    ty, core = tp // 2, tp % 2

    def target_of(i):
        pair = i // 2
        dy = jnp.where(pair == 0, 2, jnp.where(pair == 1, 1, jnp.where(pair == 2, 3, 0)))
        flip = jnp.where(pair == 3, 1 - i % 2, i % 2)
        return ((ty + dy) % 4) * 2 + (core + flip) % 2

    def lanes_of(t):
        return pl.ds(pl.multiple_of(t * 128, 128), 128)

    def tp_copy(i, to):
        return pltpu.make_async_remote_copy(
            src_ref=send_ref.at[i], dst_ref=rows_ref.at[:, lanes_of(tp)],
            send_sem=tp_send.at[i], recv_sem=tp_recv.at[i], device_id=(me, to), device_id_type=MESH,
        )

    def direct_copy(i):
        return pltpu.make_async_remote_copy(
            src_ref=send_ref.at[i, pl.ds(0, 128)], dst_ref=rows_ref.at[pl.ds(0, 128), lanes_of(tp)],
            send_sem=tp_send.at[i], recv_sem=tp_recv.at[i], device_id=(me, target_of(i)), device_id_type=MESH,
        )

    def hop_copy(i):
        return pltpu.make_async_remote_copy(
            src_ref=send_ref.at[i, pl.ds(128, 128)], dst_ref=hop_ref.at[i],
            send_sem=tp_send.at[7 + i], recv_sem=tp_recv.at[7 + i],
            device_id=(me, (ty + 3) % 4 * 2 + core), device_id_type=MESH,
        )

    def relay_copy(i):
        return pltpu.make_async_remote_copy(
            src_ref=hop_ref.at[i], dst_ref=rows_ref.at[pl.ds(128, 128), lanes_of((ty + 1) % 4 * 2 + core)],
            send_sem=tp_send.at[9 + i], recv_sem=tp_recv.at[9 + i],
            device_id=(me, (ty + 3) % 4 * 2 + (core + i) % 2), device_id_type=MESH,
        )

    @pl.loop(0, 8)
    def _(i):
        to = target_of(i)
        at = pl.multiple_of(to * 256, 256)
        keys, score = [], []
        for half in range(2):
            j = to * 2 + half
            parts = [own_ref[kind, 2 * j + b] for b in range(2) for kind in range(2)]
            bias = []
            for c in range(FAR_PICKS):
                places = [find_ref[16 + 8 * kind + c, me * 16 + j] for kind in range(2)]
                parts += [all_ref[kind, jnp.maximum(places[kind], 0)] for kind in range(2)]
                bias.append(jnp.where(places[0] < 0, NEG, 0.0))
            keys.append(jnp.concatenate(parts, axis=0))
            q = jnp.concatenate([qt_ref[h, pl.ds(at + half * 128, 128), :] for h in range(2)], axis=0)
            s = lax.dot_general(q, keys[half], NT, preferred_element_type=jnp.float32)
            mine = jnp.where(jnp.concatenate([triangle, triangle], axis=0), s[:, :128], NEG)
            far = [
                s[:, 128 + 128 * c : 256 + 128 * c] + jnp.where(front, bias[2 * c], bias[2 * c + 1])
                for c in range(FAR_PICKS // 2)
            ]
            score.append(jnp.concatenate([mine, *far], axis=1))
        weights = [jnp.exp2(s - jnp.max(s, axis=1, keepdims=True)).astype(jnp.bfloat16) for s in score]
        out = [
            jnp.dot(w, with_totals(k), preferred_element_type=jnp.float32) for w, k in zip(weights, keys)
        ]
        mixed = [join(o[:128], o[128:]) for o in out]
        mixed = jnp.concatenate(mixed, axis=0) * gate_ref[1, pl.ds(at, 256), :] + mix_ref[pl.ds(at, 256), :]
        mixed = mixed.astype(jnp.bfloat16)
        send_ref[i] = mixed

        @pl.when(i == 7)
        def _():
            rows_ref[:, lanes_of(tp)] = mixed

        for two in range(2):

            @pl.when(i == two)
            def _():
                direct_copy(two).start()
                hop_copy(two).start()

        @pl.when((i > 1) & (i < 7))
        def _():
            tp_copy(i, to).start()

        @pl.when(i == 4)
        def _():
            for two in range(2):
                hop_copy(two).wait_recv()
                relay_copy(two).start()

    weight.wait()
    for pair, away in ((1, 1), (2, 3), (3, 0), (0, 2)):
        if pair == 0:
            for i in range(2):
                direct_copy(i).wait_recv()
                relay_copy(i).wait_recv()
        else:
            for i in range(2 * pair, min(2 * pair + 2, 7)):
                tp_copy(i, target_of(i)).wait_recv()
        at = pl.ds(pl.multiple_of((ty + 4 - away) % 4 * 256, 256), 256)
        part = jnp.dot(rows_ref[:, at], weight_ref[at, :], preferred_element_type=jnp.float32)
        if pair == 1:
            total_ref[...] = part
        elif pair:
            total_ref[...] += part
        else:
            out_ref[...] = (total_ref[...] + part).astype(out_ref.dtype)

    for i in range(2):
        direct_copy(i).wait_send()
        hop_copy(i).wait_send()
        relay_copy(i).wait_send()
    for i in range(2, 7):
        tp_copy(i, target_of(i)).wait_send()
    for k in range(1, 16):
        sum_copy(k).wait_send()
    for name in NAMES:
        span_copy(*name).wait_send()


def layer(chosen, tokens, rest, out_weight, seq):
    rows, width = tokens.shape
    args = (tokens, *rest, *rope_tables(seq))
    bf, f32 = jnp.bfloat16, jnp.float32
    spans = seq // rows
    held = [pltpu.VMEM((rows // ROWS, ROWS, width), bf)]
    held += [pltpu.VMEM(a.shape, a.dtype) for a in args[1:-2]]
    held += [pltpu.VMEM((rows // 64, 128), f32)] * 2
    entry = (32, 128)
    dma = pltpu.SemaphoreType.DMA
    return pl.pallas_call(
        layer_kernel,
        in_specs=[pl.BlockSpec(memory_space=pltpu.HBM)] * (len(args) + 2),
        out_specs=pl.BlockSpec(memory_space=pltpu.VMEM),
        out_shape=jax.ShapeDtypeStruct((rows // 8, width), bf),
        scratch_shapes=held + [
            pltpu.VMEM((256, width), bf),
            pltpu.VMEM((rows // ROWS, ROWS, 1), f32),
            pltpu.VMEM((rows, 128), f32),
            pltpu.VMEM((rows // CMP_BLOCK, CMP_BLOCK * 64), bf),
            pltpu.VMEM((rows // CMP_BLOCK, CMP_BLOCK * 64), bf),
            pltpu.VMEM((2, rows, 128), bf),
            pltpu.VMEM((2, rows, 128), bf),
            pltpu.VMEM((2, rows, 128), f32),
            pltpu.VMEM((rows // CMP_BLOCK, 128), bf),
            pltpu.VMEM((2, 32, *entry), bf),
            pltpu.VMEM((2, 128, *entry), bf),
            pltpu.VMEM((2, 192, *entry), bf),
            pltpu.VMEM((2, 64, *entry), bf),
            pltpu.VMEM((2, 320, *entry), bf),
            pltpu.VMEM(chosen.shape, jnp.int32),
            pltpu.VMEM((32, chosen.shape[-1]), jnp.int32),
            pltpu.SMEM((32, chosen.shape[-1]), jnp.int32),
            pltpu.VMEM((spans, rows // CMP_BLOCK, 128), bf),
            pltpu.VMEM((rows, 128), f32),
            pltpu.VMEM((8, rows // 8, 128), bf),
            pltpu.VMEM((rows // 8, 1024), bf),
            pltpu.VMEM((2, 128, 128), bf),
            pltpu.VMEM(out_weight.shape, bf),
            pltpu.VMEM((rows // 8, width), f32),
            dma((18,)), dma((rows // ROWS,)), dma, dma, dma((len(PLAN),)), dma((len(PLAN),)),
            dma((15,)), dma((15,)), dma((11,)), dma((11,)),
        ],
        compiler_params=pltpu.CompilerParams(collective_id=0, has_side_effects=True, vmem_limit_bytes=67043328),
        name="layer",
    )(chosen, *args, out_weight)


def per_device(
    tokens, norm_gain, query_weight, cmp_key_weight, cmp_value_weight, sel_key_weight, sel_value_weight,
    branch_weight, key_embed, key_inner, key_outer, value_embed, value_inner, value_outer, out_weight, chosen,
):
    seq = tokens.shape[0] * lax.axis_size("kv")
    rest = (
        norm_gain, query_weight,
        cmp_key_weight.T, cmp_value_weight.T, sel_key_weight.T, sel_value_weight.T,
        branch_weight.transpose(0, 2, 1),
        key_embed, key_inner.transpose(0, 2, 1), key_outer,
        value_embed, value_inner.transpose(0, 2, 1), value_outer,
    )
    return layer(chosen.transpose(0, 2, 1), tokens, rest, out_weight, seq)


def solution(mesh):
    placed = (
        P("kv", None), P(), P(None, "tp"), P(None, "tp"), P(None, "tp"), P(None, "tp"), P(None, "tp"), P(),
        P("tp", None, None), P("tp", None, None), P("tp", None, None), P("tp", None, None), P("tp", None, None),
        P("tp", None, None), P(), P("tp", None, None),
    )
    return jax.shard_map(
        per_device, mesh=mesh, in_specs=placed, out_specs=P(("kv", "tp"), None), check_vma=False
    )
```

```python
import math

import jax
import jax.numpy as jnp
import numpy as np
from jax import lax
from jax.experimental import pallas as pl
from jax.experimental.pallas import tpu as pltpu
from jax.sharding import PartitionSpec as P

HEAD_DIM = 64
CMP_BLOCK = 32
SEL_BLOCK = 64
Q_BLOCK = 128
FAR_PICKS = 8
ROPE_BASE = 10000.0
NORM_EPS = 1e-06
MESH = pl.DeviceIdType.MESH
NT = (((1,), (1,)), ((), ()))
NEG = -1e30
ROWS = 512


def rope_tables(seq):
    half = HEAD_DIM // 2
    inverse = ROPE_BASE ** (-np.arange(half, dtype=np.float64) / half)
    lane = np.arange(128) % half
    low = np.arange(64, dtype=np.float64)[:, None] * inverse[lane][None, :]
    high = np.arange(seq // 64, dtype=np.float64)[:, None] * 64.0 * inverse[lane][None, :]
    return tuple(np.asarray(f(a), np.float32) for a in (low, high) for f in (np.cos, np.sin))


def gelu(x):
    return 0.5 * x * (1.0 + jnp.tanh(math.sqrt(2.0 / math.pi) * (x + 0.044715 * (x * x * x))))


WAYS = {0: ("x", "z"), 1: ("z", "x")}
ORDER = (0, 1, 3, 2)


def copy_plan():
    plan = {}
    for kind, (first, second) in WAYS.items():
        for part in (0, 1):
            plan[kind, f"own{part}+"] = (first + "+", "ring", 16 * part, 16, "ring", 96 + 16 * part)
            plan[kind, f"own{part}-"] = (first + "-", "ring", 16 * part, 16, "ring", 32 + 16 * part)
        plan[kind, "far+"] = (first + "+", "ring", 96, 16, "ring", 64)
        plan[kind, "far-"] = (first + "-", "ring", 48, 16, "ring", 80)
        for batch, to in enumerate(("even", "odd")):
            out, hop = 96 * batch, 32 * batch
            for name, at, n in ((f"early{batch}", 0, 8), (f"late{batch}", 8, 24)):
                half = n // 2
                plan[kind, name + "+"] = (second + "+", "pack", out + at, n, to, 192 + at)
                plan[kind, name + "-"] = (second + "-", "pack", out + 64 + at, n, to, 128 + at)
                plan[kind, name + "2+"] = (second + "+", "pack", out + 32 + at, half, "pass", hop + at)
                plan[kind, name + "2-"] = (second + "-", "pack", out + 32 + at + half, half, "pass", hop + at + half)
                plan[kind, name + "3+"] = (second + "+", "pass", hop + at, half, to, 160 + at)
                plan[kind, name + "3-"] = (second + "-", "pass", hop + at + half, half, to, 160 + at + half)
    return plan


PLAN = copy_plan()
NAMES = list(PLAN)


def layer_kernel(
    chosen_hbm, x_hbm, gain_hbm, qw_hbm, ck_hbm, cv_hbm, sk_hbm, sv_hbm, bw_hbm,
    ke_hbm, ki_hbm, ko_hbm, ve_hbm, vi_hbm, vo_hbm, cl_hbm, sl_hbm, ch_hbm, sh_hbm, weight_hbm,
    out_ref,
    x_ref, gain_ref, qw_ref, ck_ref, cv_ref, sk_ref, sv_ref, bw_ref,
    ke_ref, ki_ref, ko_ref, ve_ref, vi_ref, vo_ref, cl_ref, sl_ref, ch_ref, sh_ref,
    w_ref, scale_ref, bi_ref, xk_ref, xv_ref, qp_ref, qt_ref, gate_ref, sum_ref,
    own_ref, ring_ref, pack_ref, pass_ref, even_ref, odd_ref, chosen_ref, table_ref, find_ref,
    sums_ref, mix_ref, send_ref, rows_ref, hop_ref, weight_ref, total_ref,
    in_sem, x_sem, find_sem, weight_sem, span_send, span_recv, sum_send, sum_recv, tp_send, tp_recv,
):
    me = lax.axis_index("kv")
    tp = lax.axis_index("tp")
    mz, mx = me // 4, me % 4
    width = x_ref.shape[-1]
    steps = x_ref.shape[0]

    small = [
        (gain_hbm, gain_ref), (sk_hbm, sk_ref), (sv_hbm, sv_ref), (ck_hbm, ck_ref), (cv_hbm, cv_ref),
        (cl_hbm, cl_ref), (sl_hbm, sl_ref), (ch_hbm.at[pl.ds(me * 32, 32)], ch_ref),
        (sh_hbm.at[pl.ds(me * 32, 32)], sh_ref), (ke_hbm, ke_ref), (ve_hbm, ve_ref),
        (ki_hbm, ki_ref), (ko_hbm, ko_ref), (vi_hbm, vi_ref), (vo_hbm, vo_ref), (qw_hbm, qw_ref), (bw_hbm, bw_ref),
        (chosen_hbm, chosen_ref),
    ]
    small = [pltpu.make_async_copy(a, b, in_sem.at[i]) for i, (a, b) in enumerate(small)]
    rows_in = [pltpu.make_async_copy(x_hbm.at[pl.ds(i * ROWS, ROWS)], x_ref.at[i], x_sem.at[i]) for i in range(steps)]
    small[17].start()
    for copy in small[:9]:
        copy.start()
    for copy in rows_in:
        copy.start()
    for copy in small[9:17]:
        copy.start()

    weight = pltpu.make_async_copy(weight_hbm, weight_ref, weight_sem)
    weight.start()

    barrier = pltpu.get_barrier_semaphore()
    for k in range(1, 16):
        pl.semaphore_signal(barrier, inc=1, device_id=((me + k) % 16, tp), device_id_type=MESH)
    for k in range(1, 8):
        pl.semaphore_signal(barrier, inc=1, device_id=(me, (tp + k) % 8), device_id_type=MESH)

    lane = lax.broadcasted_iota(jnp.int32, (1, 128), 1)
    front = lane < 64
    flip = lane % 64 < 32
    sign = jnp.where(flip, -1.0, 1.0)

    small[17].wait()
    block = chosen_ref[0]
    query = lax.broadcasted_iota(jnp.int32, block.shape, 1)
    for s in range(16):
        table_ref[s : s + 1, :] = jnp.sum(jnp.where(block // 32 == s, block % 32, 0), axis=0, keepdims=True)
    usable = block * SEL_BLOCK < query * Q_BLOCK
    rz = (block // 128 + 4 - mz) % 4
    rx = (block // 32 % 4 + 4 - mx) % 4
    for row, r_first, r_second in ((16, rx, rz), (24, rz, rx)):
        place = jnp.where(r_first < 2, r_first, 5 - r_first)
        at = jnp.where(r_second == 0, r_first * 32 + block % 32, 96 + r_second * 32 + place * 8 + query % 16 // 2)
        table_ref[row : row + 8, :] = jnp.where(usable, at, -1)
    find = pltpu.make_async_copy(table_ref, find_ref, find_sem)
    find.start()

    def angles(step):
        cos, sin = [], []
        low_c, low_s = cl_ref[...], sl_ref[...]
        for g in range(ROWS // 64):
            hc = ch_ref[pl.ds(step * (ROWS // 64) + g, 1), :]
            hs = sh_ref[pl.ds(step * (ROWS // 64) + g, 1), :]
            cos.append(low_c * hc - low_s * hs)
            sin.append(low_c * (hs * sign) + low_s * (hc * sign))
        return jnp.concatenate(cos, axis=0), jnp.concatenate(sin, axis=0)

    def turn(v, c, s):
        swapped = jnp.where(flip, pltpu.roll(v, 96, 1), pltpu.roll(v, 32, 1))
        return v * c + swapped * s

    for copy in small[:9]:
        copy.wait()
    gain = gain_ref[...].astype(jnp.float32).reshape(1, width)
    for at, ref in ((0, sk_ref), (64, sv_ref), (128, ck_ref), (192, cv_ref)):
        w_ref[at : at + 64, :] = (ref[...].astype(jnp.float32) * gain).astype(jnp.bfloat16)
    for copy in small[9:11]:
        copy.wait()
    embed = jnp.concatenate([ke_ref[0], ve_ref[0]], axis=1).astype(jnp.float32)
    embed = jnp.concatenate([embed] * (ROWS // CMP_BLOCK), axis=0)

    def keys_and_values(step):
        pltpu.make_async_copy(
            x_hbm.at[pl.ds(pl.multiple_of(step * ROWS, ROWS), ROWS)], x_ref.at[step], x_sem.at[step]
        ).wait()
        x = x_ref[step]
        xf = x.astype(jnp.float32)
        scale = lax.rsqrt(jnp.sum(xf * xf, axis=1, keepdims=True) * (1.0 / width) + NORM_EPS)
        scale_ref[step] = scale
        y = lax.dot_general(x, w_ref[...], NT, preferred_element_type=jnp.float32) * scale
        cos, sin = angles(step)
        kv = turn(y[:, 0:128], jnp.where(front, cos, 1.0), jnp.where(front, sin, 0.0)).astype(jnp.bfloat16)
        kv = kv.reshape(ROWS // 64, 2, 32, 128)
        for kind in range(2):
            own_ref[kind, pl.ds(step * (ROWS // 64), ROWS // 64)] = kv[:, kind]
            ring_ref[kind, pl.ds(step * (ROWS // 64), ROWS // 64)] = kv[:, kind]
        raw = y[:, 128:256].astype(jnp.bfloat16).astype(jnp.float32)
        bi_ref[pl.ds(pl.multiple_of(step * ROWS, ROWS), ROWS), :] = raw + embed

    step_to = {
        "x+": (mz * 4 + (mx + 1) % 4, tp),
        "x-": (mz * 4 + (mx + 3) % 4, tp),
        "z+": (((mz + 1) % 4) * 4 + mx, tp),
        "z-": (((mz + 3) % 4) * 4 + mx, tp),
    }

    def sum_copy(k):
        return pltpu.make_async_remote_copy(
            src_ref=sum_ref, dst_ref=sums_ref.at[me], send_sem=sum_send.at[k - 1], recv_sem=sum_recv.at[k - 1],
            device_id=((me + k) % 16, tp), device_id_type=MESH,
        )

    refs = {"ring": ring_ref, "pack": pack_ref, "pass": pass_ref, "even": even_ref, "odd": odd_ref}

    def span_copy(*name):
        way, source, at, n, target, to = PLAN[name]
        i = NAMES.index(name)
        return pltpu.make_async_remote_copy(
            src_ref=refs[source].at[name[0], pl.ds(at, n)], dst_ref=refs[target].at[name[0], pl.ds(to, n)],
            send_sem=span_send.at[i], recv_sem=span_recv.at[i], device_id=step_to[way], device_id_type=MESH,
        )

    def start(*names):
        for name in names:
            for kind in range(2):
                span_copy(kind, name).start()

    def arrive(*names):
        for name in names:
            for kind in range(2):
                span_copy(kind, name).wait_recv()

    def pack(batch, targets, places, source):
        @pl.loop(0, 8, unroll=2)
        def _(j):
            for kind in range(2):
                for e in targets:
                    d = e + 1
                    to = ((mz + d) % 4) * 4 + mx if kind == 0 else mz * 4 + (mx + d) % 4
                    for place in places:
                        r = ORDER[place]
                        span = mz * 4 + (mx + r) % 4 if kind == 0 else ((mz + r) % 4) * 4 + mx
                        wanted = find_ref[span, to * 16 + 2 * j + batch]
                        pack_ref[kind, 96 * batch + e * 32 + place * 8 + j] = source[kind, r * 32 + wanted]

    pl.loop(0, steps // 2)(keys_and_values)
    pl.semaphore_wait(barrier, 22)
    start("own0+", "own0-")
    pl.loop(steps // 2, steps)(keys_and_values)
    start("own1+", "own1-")
    find.wait()
    for batch in range(2):
        pack(batch, (0, 1, 2), (0,), own_ref)
        start(f"early{batch}+", f"early{batch}-")

    for copy in small[11:17]:
        copy.wait()
    count = bi_ref.shape[0] // CMP_BLOCK
    for t in range(0, CMP_BLOCK, 2):
        a = bi_ref[pl.ds(t, count, stride=CMP_BLOCK), :]
        b = bi_ref[pl.ds(t + 1, count, stride=CMP_BLOCK), :]
        xk_ref[:, t * 64 : t * 64 + 128] = jnp.where(front, a, pltpu.roll(b, 64, 1)).astype(jnp.bfloat16)
        xv_ref[:, t * 64 : t * 64 + 128] = jnp.where(front, pltpu.roll(a, 64, 1), b).astype(jnp.bfloat16)
    summary = []
    for x_in, inner, outer in ((xk_ref, ki_ref, ko_ref), (xv_ref, vi_ref, vo_ref)):
        hidden = lax.dot_general(x_in[...], inner[0], NT, preferred_element_type=jnp.float32)
        hidden = gelu(hidden).astype(jnp.bfloat16)
        summary.append(jnp.dot(hidden, outer[0], preferred_element_type=jnp.float32))
    summary = jnp.concatenate(summary, axis=1).astype(jnp.bfloat16)
    sum_ref[...] = summary
    sums_ref[me] = summary

    w_ref[0:128, :] = (qw_ref[...].astype(jnp.float32).T * gain).astype(jnp.bfloat16)
    r = lax.broadcasted_iota(jnp.int32, (128, 32), 0)
    c = lax.broadcasted_iota(jnp.int32, (128, 32), 1)
    want = jnp.where(r < 2, tp * 2 + r, 16 + tp * 2 + (r - 2))
    pick = jnp.where((r < 4) & (c == want), 1.0, 0.0).astype(jnp.bfloat16)
    gates = jnp.dot(pick, bw_ref[...].reshape(32, width), preferred_element_type=jnp.float32)
    w_ref[128:256, :] = (gates * gain).astype(jnp.bfloat16)

    arrive("own0+", "own0-", "own1+", "own1-")
    start("far+", "far-", "early02+", "early02-", "early12+", "early12-")
    for k in range(1, 16):
        sum_copy(k).start()

    def by_head(v):
        v = v * (HEAD_DIM**-0.5 * math.log2(math.e))
        first = jnp.where(front, v, 0.0)
        second = jnp.where(front, pltpu.roll(v, 64, 1), 0.0)
        return jnp.stack([first, second]).astype(jnp.bfloat16)

    @pl.loop(0, steps)
    def _(step):
        y = lax.dot_general(x_ref[step], w_ref[...], NT, preferred_element_type=jnp.float32) * scale_ref[step]
        at = pl.ds(pl.multiple_of(step * ROWS, ROWS), ROWS)
        q = y[:, 0:128]
        qp_ref[:, at, :] = by_head(q)
        qt_ref[:, at, :] = by_head(turn(q, *angles(step)))
        gates = 1.0 / (1.0 + jnp.exp(-y[:, 128:256]))
        for branch in range(2):
            gate_ref[branch, at, :] = jnp.where(
                front, gates[:, 2 * branch : 2 * branch + 1], gates[:, 2 * branch + 1 : 2 * branch + 2]
            )

    rest = (1, 2, 3)
    arrive("far+", "far-")
    pack(0, (1,), rest, ring_ref)
    start("late02+", "late02-")
    arrive("early02+", "early02-", "early12+", "early12-")
    start("early03+", "early03-", "early13+", "early13-")
    pack(0, (0,), rest, ring_ref)
    start("late0+")
    pack(0, (2,), rest, ring_ref)
    start("late0-")
    pack(1, (0, 1, 2), rest, ring_ref)
    for kind in range(2):
        even_ref[kind, 0:128] = ring_ref[kind]
        odd_ref[kind, 0:128] = ring_ref[kind]
    for k in range(1, 16):
        sum_copy(k).wait_recv()

    base = me * 2048

    def with_totals(keys):
        return jnp.where(front, jnp.ones((), jnp.bfloat16), keys)

    def join(first, second):
        value = jnp.where(front, pltpu.roll(first, 64, 1), second)
        total = jnp.where(front, first, pltpu.roll(second, 64, 1))
        return value / jnp.maximum(total, 0.5)

    def compressed(t):
        at = pl.multiple_of(t * 256, 256)
        rows = base + at + lax.broadcasted_iota(jnp.int32, (256, 1), 0)
        limit = (rows + 1) // CMP_BLOCK
        column = lax.broadcasted_iota(jnp.int32, (256, 1024), 1)
        sums = sums_ref[...].reshape(1024, 128)
        out = []
        for h in range(2):
            s = lax.dot_general(qp_ref[h, pl.ds(at, 256), :], sums, NT, preferred_element_type=jnp.float32)
            s = jnp.where(column < limit, s, NEG)
            p = jnp.exp2(s - jnp.maximum(jnp.max(s, axis=1, keepdims=True), -1e20)).astype(jnp.bfloat16)
            out.append(jnp.dot(p, with_totals(sums), preferred_element_type=jnp.float32))
        mix_ref[pl.ds(at, 256), :] = join(*out) * gate_ref[0, pl.ds(at, 256), :]

    pl.loop(0, 4)(compressed)
    arrive("late02+", "late02-")
    start("late03+", "late03-", "late12+", "late12-", "late1+", "late1-")
    pl.loop(4, 8)(compressed)
    arrive("late12+", "late12-")
    start("late13+", "late13-")

    triangle = lax.broadcasted_iota(jnp.int32, (128, 128), 1) <= lax.broadcasted_iota(jnp.int32, (128, 128), 0)
    ty, core = tp // 2, tp % 2

    def target_of(i):
        pair = i // 2
        dy = jnp.where(pair == 0, 2, jnp.where(pair == 1, 1, jnp.where(pair == 2, 3, 0)))
        flip = jnp.where(pair == 3, 1 - i % 2, i % 2)
        return ((ty + dy) % 4) * 2 + (core + flip) % 2

    def lanes_of(t):
        return pl.ds(pl.multiple_of(t * 128, 128), 128)

    def tp_copy(batch, i, to):
        return pltpu.make_async_remote_copy(
            src_ref=send_ref.at[batch, i], dst_ref=rows_ref.at[pl.ds(batch * 128, 128), lanes_of(tp)],
            send_sem=tp_send.at[batch * 8 + i], recv_sem=tp_recv.at[batch * 8 + i],
            device_id=(me, to), device_id_type=MESH,
        )

    def hop_copy(batch):
        return pltpu.make_async_remote_copy(
            src_ref=send_ref.at[batch, 1], dst_ref=hop_ref.at[batch],
            send_sem=tp_send.at[batch * 8 + 1], recv_sem=tp_recv.at[batch * 8 + 1],
            device_id=(me, (ty + 3) % 4 * 2 + core), device_id_type=MESH,
        )

    def relay_copy(batch):
        return pltpu.make_async_remote_copy(
            src_ref=hop_ref.at[batch],
            dst_ref=rows_ref.at[pl.ds(batch * 128, 128), lanes_of((ty + 1) % 4 * 2 + core)],
            send_sem=tp_send.at[batch * 8 + 7], recv_sem=tp_recv.at[batch * 8 + 7],
            device_id=(me, (ty + 3) % 4 * 2 + 1 - core), device_id_type=MESH,
        )

    def chosen_branch(batch, all_ref):
        @pl.loop(0, 4)
        def _(pair):
            keys, score, at = [], [], []
            for half in range(2):
                j = target_of(2 * pair + half) * 2 + batch
                at.append(pl.ds(pl.multiple_of(j * 128, 128), 128))
                parts = [own_ref[kind, 2 * j + b] for b in range(2) for kind in range(2)]
                bias = []
                for c in range(FAR_PICKS):
                    places = [find_ref[16 + 8 * kind + c, me * 16 + j] for kind in range(2)]
                    parts += [all_ref[kind, jnp.maximum(places[kind], 0)] for kind in range(2)]
                    bias.append(jnp.where(places[0] < 0, NEG, 0.0))
                keys.append(jnp.concatenate(parts, axis=0))
                q = jnp.concatenate([qt_ref[h, at[half], :] for h in range(2)], axis=0)
                s = lax.dot_general(q, keys[half], NT, preferred_element_type=jnp.float32)
                mine = jnp.where(jnp.concatenate([triangle, triangle], axis=0), s[:, :128], NEG)
                far = [
                    s[:, 128 + 128 * c : 256 + 128 * c] + jnp.where(front, bias[2 * c], bias[2 * c + 1])
                    for c in range(FAR_PICKS // 2)
                ]
                score.append(jnp.concatenate([mine, *far], axis=1))
            weights = [jnp.exp2(s - jnp.max(s, axis=1, keepdims=True)).astype(jnp.bfloat16) for s in score]
            out = [
                jnp.dot(w, with_totals(k), preferred_element_type=jnp.float32) for w, k in zip(weights, keys)
            ]
            mixed = [
                (join(o[:128], o[128:]) * gate_ref[1, rows, :] + mix_ref[rows, :]).astype(jnp.bfloat16)
                for o, rows in zip(out, at)
            ]
            for half in range(2):
                send_ref[batch, 2 * pair + half] = mixed[half]

            @pl.when(pair == 0)
            def _():
                tp_copy(batch, 0, target_of(0)).start()
                hop_copy(batch).start()

            @pl.when(pair > 0)
            def _():
                tp_copy(batch, 2 * pair, target_of(2 * pair)).start()

            @pl.when((pair > 0) & (pair < 3))
            def _():
                tp_copy(batch, 2 * pair + 1, target_of(2 * pair + 1)).start()

            @pl.when(pair == 2)
            def _():
                hop_copy(batch).wait_recv()
                relay_copy(batch).start()

            @pl.when(pair == 3)
            def _():
                rows_ref[batch * 128 : batch * 128 + 128, lanes_of(tp)] = mixed[1]

    def rows_arrive(batch, pair):
        if pair == 0:
            tp_copy(batch, 0, target_of(0)).wait_recv()
            relay_copy(batch).wait_recv()
        else:
            for i in range(2 * pair, min(2 * pair + 2, 7)):
                tp_copy(batch, i, target_of(i)).wait_recv()

    for batch, all_ref in ((0, even_ref), (1, odd_ref)):
        for part in ("early", "late"):
            arrive(*(f"{part}{batch}{way}" for way in ("+", "-", "3+", "3-")))
        chosen_branch(batch, all_ref)

    weight.wait()
    for pair in range(4):
        rows_arrive(0, pair)
    out_ref[0:128, :] = jnp.dot(rows_ref[0:128, :], weight_ref[...], preferred_element_type=jnp.float32).astype(
        out_ref.dtype
    )
    for pair, away in ((3, 0), (1, 1), (2, 3), (0, 2)):
        rows_arrive(1, pair)
        at = pl.ds(pl.multiple_of((ty + 4 - away) % 4 * 256, 256), 256)
        part = jnp.dot(rows_ref[128:256, at], weight_ref[at, :], preferred_element_type=jnp.float32)
        if pair == 3:
            total_ref[...] = part
        elif pair:
            total_ref[...] += part
        else:
            out_ref[128:256, :] = (total_ref[...] + part).astype(out_ref.dtype)

    for batch in range(2):
        for i in (0, 2, 3, 4, 5, 6):
            tp_copy(batch, i, target_of(i)).wait_send()
        hop_copy(batch).wait_send()
        relay_copy(batch).wait_send()
    for k in range(1, 16):
        sum_copy(k).wait_send()
    for name in NAMES:
        span_copy(*name).wait_send()


def layer(chosen, tokens, rest, out_weight, seq):
    rows, width = tokens.shape
    args = (tokens, *rest, *rope_tables(seq))
    bf, f32 = jnp.bfloat16, jnp.float32
    spans = seq // rows
    held = [pltpu.VMEM((rows // ROWS, ROWS, width), bf)]
    held += [pltpu.VMEM(a.shape, a.dtype) for a in args[1:-2]]
    held += [pltpu.VMEM((rows // 64, 128), f32)] * 2
    entry = (32, 128)
    dma = pltpu.SemaphoreType.DMA
    return pl.pallas_call(
        layer_kernel,
        in_specs=[pl.BlockSpec(memory_space=pltpu.HBM)] * (len(args) + 2),
        out_specs=pl.BlockSpec(memory_space=pltpu.VMEM),
        out_shape=jax.ShapeDtypeStruct((rows // 8, width), bf),
        scratch_shapes=held + [
            pltpu.VMEM((256, width), bf),
            pltpu.VMEM((rows // ROWS, ROWS, 1), f32),
            pltpu.VMEM((rows, 128), f32),
            pltpu.VMEM((rows // CMP_BLOCK, CMP_BLOCK * 64), bf),
            pltpu.VMEM((rows // CMP_BLOCK, CMP_BLOCK * 64), bf),
            pltpu.VMEM((2, rows, 128), bf),
            pltpu.VMEM((2, rows, 128), bf),
            pltpu.VMEM((2, rows, 128), f32),
            pltpu.VMEM((rows // CMP_BLOCK, 128), bf),
            pltpu.VMEM((2, 32, *entry), bf),
            pltpu.VMEM((2, 128, *entry), bf),
            pltpu.VMEM((2, 192, *entry), bf),
            pltpu.VMEM((2, 64, *entry), bf),
            pltpu.VMEM((2, 224, *entry), bf),
            pltpu.VMEM((2, 224, *entry), bf),
            pltpu.VMEM(chosen.shape, jnp.int32),
            pltpu.VMEM((32, chosen.shape[-1]), jnp.int32),
            pltpu.SMEM((32, chosen.shape[-1]), jnp.int32),
            pltpu.VMEM((spans, rows // CMP_BLOCK, 128), bf),
            pltpu.VMEM((rows, 128), f32),
            pltpu.VMEM((2, 8, 128, 128), bf),
            pltpu.VMEM((rows // 8, 1024), bf),
            pltpu.VMEM((2, 128, 128), bf),
            pltpu.VMEM(out_weight.shape, bf),
            pltpu.VMEM((rows // 16, width), f32),
            dma((18,)), dma((rows // ROWS,)), dma, dma, dma((len(PLAN),)), dma((len(PLAN),)),
            dma((15,)), dma((15,)), dma((16,)), dma((16,)),
        ],
        compiler_params=pltpu.CompilerParams(collective_id=0, has_side_effects=True, vmem_limit_bytes=67043328),
        name="layer",
    )(chosen, *args, out_weight)


def per_device(
    tokens, norm_gain, query_weight, cmp_key_weight, cmp_value_weight, sel_key_weight, sel_value_weight,
    branch_weight, key_embed, key_inner, key_outer, value_embed, value_inner, value_outer, out_weight, chosen,
):
    seq = tokens.shape[0] * lax.axis_size("kv")
    rest = (
        norm_gain, query_weight,
        cmp_key_weight.T, cmp_value_weight.T, sel_key_weight.T, sel_value_weight.T,
        branch_weight.transpose(0, 2, 1),
        key_embed, key_inner.transpose(0, 2, 1), key_outer,
        value_embed, value_inner.transpose(0, 2, 1), value_outer,
    )
    return layer(chosen.transpose(0, 2, 1), tokens, rest, out_weight, seq)


def solution(mesh):
    placed = (
        P("kv", None), P(), P(None, "tp"), P(None, "tp"), P(None, "tp"), P(None, "tp"), P(None, "tp"), P(),
        P("tp", None, None), P("tp", None, None), P("tp", None, None), P("tp", None, None), P("tp", None, None),
        P("tp", None, None), P(), P("tp", None, None),
    )
    return jax.shard_map(
        per_device, mesh=mesh, in_specs=placed, out_specs=P(("kv", "tp"), None), check_vma=False
    )
```

```python
import math

import jax
import jax.numpy as jnp
import numpy as np
from jax import lax
from jax.experimental import pallas as pl
from jax.experimental.pallas import tpu as pltpu
from jax.sharding import PartitionSpec as P

HEAD_DIM = 64
CMP_BLOCK = 32
SEL_BLOCK = 64
Q_BLOCK = 128
FAR_PICKS = 8
ROPE_BASE = 10000.0
NORM_EPS = 1e-06
MESH = pl.DeviceIdType.MESH
NT = (((1,), (1,)), ((), ()))
NEG = -1e30
ROWS = 512


def rope_tables(seq):
    half = HEAD_DIM // 2
    inverse = ROPE_BASE ** (-np.arange(half, dtype=np.float64) / half)
    lane = np.arange(128) % half
    low = np.arange(64, dtype=np.float64)[:, None] * inverse[lane][None, :]
    high = np.arange(seq // 64, dtype=np.float64)[:, None] * 64.0 * inverse[lane][None, :]
    return tuple(np.asarray(f(a), np.float32) for a in (low, high) for f in (np.cos, np.sin))


def gelu(x):
    return 0.5 * x * (1.0 + jnp.tanh(math.sqrt(2.0 / math.pi) * (x + 0.044715 * (x * x * x))))


WAYS = {0: ("x", "z"), 1: ("z", "x")}
ORDER = (0, 1, 3, 2)


def copy_plan():
    plan = {}
    for kind, (first, second) in WAYS.items():
        for part in (0, 1):
            plan[kind, f"own{part}+"] = (first + "+", "ring", 16 * part, 16, "ring", 96 + 16 * part)
            plan[kind, f"own{part}-"] = (first + "-", "ring", 16 * part, 16, "ring", 32 + 16 * part)
        plan[kind, "far+"] = (first + "+", "ring", 96, 16, "ring", 64)
        plan[kind, "far-"] = (first + "-", "ring", 48, 16, "ring", 80)
        for batch, to in enumerate(("even", "odd")):
            out, hop = 96 * batch, 32 * batch
            for name, at, n in ((f"early{batch}", 0, 8), (f"late{batch}", 8, 24)):
                half = n // 2
                plan[kind, name + "+"] = (second + "+", "pack", out + at, n, to, 192 + at)
                plan[kind, name + "-"] = (second + "-", "pack", out + 64 + at, n, to, 128 + at)
                plan[kind, name + "2+"] = (second + "+", "pack", out + 32 + at, half, "pass", hop + at)
                plan[kind, name + "2-"] = (second + "-", "pack", out + 32 + at + half, half, "pass", hop + at + half)
                plan[kind, name + "3+"] = (second + "+", "pass", hop + at, half, to, 160 + at)
                plan[kind, name + "3-"] = (second + "-", "pass", hop + at + half, half, to, 160 + at + half)
    return plan


PLAN = copy_plan()
NAMES = list(PLAN)


def layer_kernel(
    chosen_hbm, x_hbm, gain_hbm, qw_hbm, ck_hbm, cv_hbm, sk_hbm, sv_hbm, bw_hbm,
    ke_hbm, ki_hbm, ko_hbm, ve_hbm, vi_hbm, vo_hbm, cl_hbm, sl_hbm, ch_hbm, sh_hbm, weight_hbm,
    out_hbm,
    x_ref, gain_ref, qw_ref, ck_ref, cv_ref, sk_ref, sv_ref, bw_ref,
    ke_ref, ki_ref, ko_ref, ve_ref, vi_ref, vo_ref, cl_ref, sl_ref, ch_ref, sh_ref,
    w_ref, scale_ref, bi_ref, xk_ref, xv_ref, qp_ref, qt_ref, gate_ref, sum_ref,
    own_ref, ring_ref, pack_ref, pass_ref, even_ref, odd_ref, chosen_ref, table_ref, find_ref,
    sums_ref, mix_ref, send_ref, rows_ref, hop_ref, weight_ref, total_ref, stage_ref,
    in_sem, x_sem, find_sem, weight_sem, leave_sem, span_send, span_recv, sum_send, sum_recv, tp_send, tp_recv,
):
    me = lax.axis_index("kv")
    tp = lax.axis_index("tp")
    mz, mx = me // 4, me % 4
    width = x_ref.shape[-1]
    steps = x_ref.shape[0]

    small = [
        (gain_hbm, gain_ref), (sk_hbm, sk_ref), (sv_hbm, sv_ref), (ck_hbm, ck_ref), (cv_hbm, cv_ref),
        (cl_hbm, cl_ref), (sl_hbm, sl_ref), (ch_hbm.at[pl.ds(me * 32, 32)], ch_ref),
        (sh_hbm.at[pl.ds(me * 32, 32)], sh_ref), (ke_hbm, ke_ref), (ve_hbm, ve_ref),
        (ki_hbm, ki_ref), (ko_hbm, ko_ref), (vi_hbm, vi_ref), (vo_hbm, vo_ref), (qw_hbm, qw_ref), (bw_hbm, bw_ref),
        (chosen_hbm, chosen_ref),
    ]
    small = [pltpu.make_async_copy(a, b, in_sem.at[i]) for i, (a, b) in enumerate(small)]
    rows_in = [pltpu.make_async_copy(x_hbm.at[pl.ds(i * ROWS, ROWS)], x_ref.at[i], x_sem.at[i]) for i in range(steps)]
    small[17].start()
    for copy in small[:9]:
        copy.start()
    for copy in rows_in:
        copy.start()
    for copy in small[9:17]:
        copy.start()

    weight = pltpu.make_async_copy(weight_hbm, weight_ref, weight_sem)
    weight.start()

    barrier = pltpu.get_barrier_semaphore()
    for k in range(1, 16):
        pl.semaphore_signal(barrier, inc=1, device_id=((me + k) % 16, tp), device_id_type=MESH)
    for k in range(1, 8):
        pl.semaphore_signal(barrier, inc=1, device_id=(me, (tp + k) % 8), device_id_type=MESH)

    lane = lax.broadcasted_iota(jnp.int32, (1, 128), 1)
    front = lane < 64
    flip = lane % 64 < 32
    sign = jnp.where(flip, -1.0, 1.0)

    small[17].wait()
    block = chosen_ref[0]
    query = lax.broadcasted_iota(jnp.int32, block.shape, 1)
    for s in range(16):
        table_ref[s : s + 1, :] = jnp.sum(jnp.where(block // 32 == s, block % 32, 0), axis=0, keepdims=True)
    usable = block * SEL_BLOCK < query * Q_BLOCK
    rz = (block // 128 + 4 - mz) % 4
    rx = (block // 32 % 4 + 4 - mx) % 4
    for row, r_first, r_second in ((16, rx, rz), (24, rz, rx)):
        place = jnp.where(r_first < 2, r_first, 5 - r_first)
        at = jnp.where(r_second == 0, r_first * 32 + block % 32, 96 + r_second * 32 + place * 8 + query % 16 // 2)
        table_ref[row : row + 8, :] = jnp.where(usable, at, -1)
    find = pltpu.make_async_copy(table_ref, find_ref, find_sem)
    find.start()

    def angles(step):
        cos, sin = [], []
        low_c, low_s = cl_ref[...], sl_ref[...]
        for g in range(ROWS // 64):
            hc = ch_ref[pl.ds(step * (ROWS // 64) + g, 1), :]
            hs = sh_ref[pl.ds(step * (ROWS // 64) + g, 1), :]
            cos.append(low_c * hc - low_s * hs)
            sin.append(low_c * (hs * sign) + low_s * (hc * sign))
        return jnp.concatenate(cos, axis=0), jnp.concatenate(sin, axis=0)

    def turn(v, c, s):
        swapped = jnp.where(flip, pltpu.roll(v, 96, 1), pltpu.roll(v, 32, 1))
        return v * c + swapped * s

    for copy in small[:9]:
        copy.wait()
    gain = gain_ref[...].astype(jnp.float32).reshape(1, width)
    for at, ref in ((0, sk_ref), (64, sv_ref), (128, ck_ref), (192, cv_ref)):
        w_ref[at : at + 64, :] = (ref[...].astype(jnp.float32) * gain).astype(jnp.bfloat16)
    for copy in small[9:11]:
        copy.wait()
    embed = jnp.concatenate([ke_ref[0], ve_ref[0]], axis=1).astype(jnp.float32)
    embed = jnp.concatenate([embed] * (ROWS // CMP_BLOCK), axis=0)

    def keys_and_values(step):
        pltpu.make_async_copy(
            x_hbm.at[pl.ds(pl.multiple_of(step * ROWS, ROWS), ROWS)], x_ref.at[step], x_sem.at[step]
        ).wait()
        x = x_ref[step]
        xf = x.astype(jnp.float32)
        scale = lax.rsqrt(jnp.sum(xf * xf, axis=1, keepdims=True) * (1.0 / width) + NORM_EPS)
        scale_ref[step] = scale
        y = lax.dot_general(x, w_ref[...], NT, preferred_element_type=jnp.float32) * scale
        cos, sin = angles(step)
        kv = turn(y[:, 0:128], jnp.where(front, cos, 1.0), jnp.where(front, sin, 0.0)).astype(jnp.bfloat16)
        kv = kv.reshape(ROWS // 64, 2, 32, 128)
        for kind in range(2):
            own_ref[kind, pl.ds(step * (ROWS // 64), ROWS // 64)] = kv[:, kind]
            ring_ref[kind, pl.ds(step * (ROWS // 64), ROWS // 64)] = kv[:, kind]
        raw = y[:, 128:256].astype(jnp.bfloat16).astype(jnp.float32)
        bi_ref[pl.ds(pl.multiple_of(step * ROWS, ROWS), ROWS), :] = raw + embed

    step_to = {
        "x+": (mz * 4 + (mx + 1) % 4, tp),
        "x-": (mz * 4 + (mx + 3) % 4, tp),
        "z+": (((mz + 1) % 4) * 4 + mx, tp),
        "z-": (((mz + 3) % 4) * 4 + mx, tp),
    }

    def sum_copy(k):
        return pltpu.make_async_remote_copy(
            src_ref=sum_ref, dst_ref=sums_ref.at[me], send_sem=sum_send.at[k - 1], recv_sem=sum_recv.at[k - 1],
            device_id=((me + k) % 16, tp), device_id_type=MESH,
        )

    refs = {"ring": ring_ref, "pack": pack_ref, "pass": pass_ref, "even": even_ref, "odd": odd_ref}

    def span_copy(*name):
        way, source, at, n, target, to = PLAN[name]
        i = NAMES.index(name)
        return pltpu.make_async_remote_copy(
            src_ref=refs[source].at[name[0], pl.ds(at, n)], dst_ref=refs[target].at[name[0], pl.ds(to, n)],
            send_sem=span_send.at[i], recv_sem=span_recv.at[i], device_id=step_to[way], device_id_type=MESH,
        )

    def start(*names):
        for name in names:
            for kind in range(2):
                span_copy(kind, name).start()

    def arrive(*names):
        for name in names:
            for kind in range(2):
                span_copy(kind, name).wait_recv()

    def pack(batch, targets, places, source):
        @pl.loop(0, 8, unroll=2)
        def _(j):
            for kind in range(2):
                for e in targets:
                    d = e + 1
                    to = ((mz + d) % 4) * 4 + mx if kind == 0 else mz * 4 + (mx + d) % 4
                    for place in places:
                        r = ORDER[place]
                        span = mz * 4 + (mx + r) % 4 if kind == 0 else ((mz + r) % 4) * 4 + mx
                        wanted = find_ref[span, to * 16 + 2 * j + batch]
                        pack_ref[kind, 96 * batch + e * 32 + place * 8 + j] = source[kind, r * 32 + wanted]

    pl.loop(0, steps // 2)(keys_and_values)
    pl.semaphore_wait(barrier, 22)
    start("own0+", "own0-")
    pl.loop(steps // 2, steps)(keys_and_values)
    start("own1+", "own1-")
    find.wait()
    for batch in range(2):
        pack(batch, (0, 1, 2), (0,), own_ref)
        start(f"early{batch}+", f"early{batch}-")

    for copy in small[11:17]:
        copy.wait()
    count = bi_ref.shape[0] // CMP_BLOCK
    for t in range(0, CMP_BLOCK, 2):
        a = bi_ref[pl.ds(t, count, stride=CMP_BLOCK), :]
        b = bi_ref[pl.ds(t + 1, count, stride=CMP_BLOCK), :]
        xk_ref[:, t * 64 : t * 64 + 128] = jnp.where(front, a, pltpu.roll(b, 64, 1)).astype(jnp.bfloat16)
        xv_ref[:, t * 64 : t * 64 + 128] = jnp.where(front, pltpu.roll(a, 64, 1), b).astype(jnp.bfloat16)
    summary = []
    for x_in, inner, outer in ((xk_ref, ki_ref, ko_ref), (xv_ref, vi_ref, vo_ref)):
        hidden = lax.dot_general(x_in[...], inner[0], NT, preferred_element_type=jnp.float32)
        hidden = gelu(hidden).astype(jnp.bfloat16)
        summary.append(jnp.dot(hidden, outer[0], preferred_element_type=jnp.float32))
    summary = jnp.concatenate(summary, axis=1).astype(jnp.bfloat16)
    sum_ref[...] = summary
    sums_ref[me] = summary

    w_ref[0:128, :] = (qw_ref[...].astype(jnp.float32).T * gain).astype(jnp.bfloat16)
    r = lax.broadcasted_iota(jnp.int32, (128, 32), 0)
    c = lax.broadcasted_iota(jnp.int32, (128, 32), 1)
    want = jnp.where(r < 2, tp * 2 + r, 16 + tp * 2 + (r - 2))
    pick = jnp.where((r < 4) & (c == want), 1.0, 0.0).astype(jnp.bfloat16)
    gates = jnp.dot(pick, bw_ref[...].reshape(32, width), preferred_element_type=jnp.float32)
    w_ref[128:256, :] = (gates * gain).astype(jnp.bfloat16)

    arrive("own0+", "own0-", "own1+", "own1-")
    start("far+", "far-", "early02+", "early02-", "early12+", "early12-")
    for k in range(1, 16):
        sum_copy(k).start()

    def by_head(v):
        v = v * (HEAD_DIM**-0.5 * math.log2(math.e))
        first = jnp.where(front, v, 0.0)
        second = jnp.where(front, pltpu.roll(v, 64, 1), 0.0)
        return jnp.stack([first, second]).astype(jnp.bfloat16)

    @pl.loop(0, steps)
    def _(step):
        y = lax.dot_general(x_ref[step], w_ref[...], NT, preferred_element_type=jnp.float32) * scale_ref[step]
        at = pl.ds(pl.multiple_of(step * ROWS, ROWS), ROWS)
        q = y[:, 0:128]
        qp_ref[:, at, :] = by_head(q)
        qt_ref[:, at, :] = by_head(turn(q, *angles(step)))
        gates = 1.0 / (1.0 + jnp.exp(-y[:, 128:256]))
        for branch in range(2):
            gate_ref[branch, at, :] = jnp.where(
                front, gates[:, 2 * branch : 2 * branch + 1], gates[:, 2 * branch + 1 : 2 * branch + 2]
            )

    rest = (1, 2, 3)
    arrive("far+", "far-")
    pack(0, (1,), rest, ring_ref)
    start("late02+", "late02-")
    arrive("early02+", "early02-", "early12+", "early12-")
    start("early03+", "early03-", "early13+", "early13-")
    pack(0, (0,), rest, ring_ref)
    start("late0+")
    pack(0, (2,), rest, ring_ref)
    start("late0-")
    pack(1, (0, 1, 2), rest, ring_ref)
    for kind in range(2):
        even_ref[kind, 0:128] = ring_ref[kind]
        odd_ref[kind, 0:128] = ring_ref[kind]
    for k in range(1, 16):
        sum_copy(k).wait_recv()

    base = me * 2048

    def with_totals(keys):
        return jnp.where(front, jnp.ones((), jnp.bfloat16), keys)

    def join(first, second):
        value = jnp.where(front, pltpu.roll(first, 64, 1), second)
        total = jnp.where(front, first, pltpu.roll(second, 64, 1))
        return value / jnp.maximum(total, 0.5)

    def compressed(t):
        at = pl.multiple_of(t * 256, 256)
        rows = base + at + lax.broadcasted_iota(jnp.int32, (256, 1), 0)
        limit = (rows + 1) // CMP_BLOCK
        column = lax.broadcasted_iota(jnp.int32, (256, 1024), 1)
        sums = sums_ref[...].reshape(1024, 128)
        out = []
        for h in range(2):
            s = lax.dot_general(qp_ref[h, pl.ds(at, 256), :], sums, NT, preferred_element_type=jnp.float32)
            s = jnp.where(column < limit, s, NEG)
            p = jnp.exp2(s - jnp.maximum(jnp.max(s, axis=1, keepdims=True), -1e20)).astype(jnp.bfloat16)
            out.append(jnp.dot(p, with_totals(sums), preferred_element_type=jnp.float32))
        mix_ref[pl.ds(at, 256), :] = join(*out) * gate_ref[0, pl.ds(at, 256), :]

    pl.loop(0, 3)(compressed)
    arrive("late02+", "late02-")
    start("late03+", "late03-", "late12+", "late12-", "late1+", "late1-")
    pl.loop(3, 8)(compressed)
    arrive("late12+", "late12-")
    start("late13+", "late13-")

    triangle = lax.broadcasted_iota(jnp.int32, (128, 128), 1) <= lax.broadcasted_iota(jnp.int32, (128, 128), 0)
    ty, core = tp // 2, tp % 2

    def target_of(i):
        pair = i // 2
        dy = jnp.where(pair == 0, 2, jnp.where(pair == 1, 1, jnp.where(pair == 2, 3, 0)))
        flip = jnp.where(pair == 3, 1 - i % 2, i % 2)
        return ((ty + dy) % 4) * 2 + (core + flip) % 2

    def lanes_of(t):
        return pl.ds(pl.multiple_of(t * 128, 128), 128)

    def tp_copy(batch, i, to):
        return pltpu.make_async_remote_copy(
            src_ref=send_ref.at[batch, i], dst_ref=rows_ref.at[pl.ds(batch * 128, 128), lanes_of(tp)],
            send_sem=tp_send.at[batch * 8 + i], recv_sem=tp_recv.at[batch * 8 + i],
            device_id=(me, to), device_id_type=MESH,
        )

    def hop_copy(batch):
        return pltpu.make_async_remote_copy(
            src_ref=send_ref.at[batch, 1], dst_ref=hop_ref.at[batch],
            send_sem=tp_send.at[batch * 8 + 1], recv_sem=tp_recv.at[batch * 8 + 1],
            device_id=(me, (ty + 3) % 4 * 2 + core), device_id_type=MESH,
        )

    def relay_copy(batch):
        return pltpu.make_async_remote_copy(
            src_ref=hop_ref.at[batch],
            dst_ref=rows_ref.at[pl.ds(batch * 128, 128), lanes_of((ty + 1) % 4 * 2 + core)],
            send_sem=tp_send.at[batch * 8 + 7], recv_sem=tp_recv.at[batch * 8 + 7],
            device_id=(me, (ty + 3) % 4 * 2 + 1 - core), device_id_type=MESH,
        )

    def chosen_branch(batch, all_ref):
        @pl.loop(0, 4)
        def _(pair):
            keys, score, at = [], [], []
            for half in range(2):
                j = target_of(2 * pair + half) * 2 + batch
                at.append(pl.ds(pl.multiple_of(j * 128, 128), 128))
                parts = [own_ref[kind, 2 * j + b] for b in range(2) for kind in range(2)]
                bias = []
                for c in range(FAR_PICKS):
                    places = [find_ref[16 + 8 * kind + c, me * 16 + j] for kind in range(2)]
                    parts += [all_ref[kind, jnp.maximum(places[kind], 0)] for kind in range(2)]
                    bias.append(jnp.where(places[0] < 0, NEG, 0.0))
                keys.append(jnp.concatenate(parts, axis=0))
                q = jnp.concatenate([qt_ref[h, at[half], :] for h in range(2)], axis=0)
                s = lax.dot_general(q, keys[half], NT, preferred_element_type=jnp.float32)
                mine = jnp.where(jnp.concatenate([triangle, triangle], axis=0), s[:, :128], NEG)
                far = [
                    s[:, 128 + 128 * c : 256 + 128 * c] + jnp.where(front, bias[2 * c], bias[2 * c + 1])
                    for c in range(FAR_PICKS // 2)
                ]
                score.append(jnp.concatenate([mine, *far], axis=1))
            weights = [jnp.exp2(s - jnp.max(s, axis=1, keepdims=True)).astype(jnp.bfloat16) for s in score]
            out = [
                jnp.dot(w, with_totals(k), preferred_element_type=jnp.float32) for w, k in zip(weights, keys)
            ]
            mixed = [
                (join(o[:128], o[128:]) * gate_ref[1, rows, :] + mix_ref[rows, :]).astype(jnp.bfloat16)
                for o, rows in zip(out, at)
            ]
            for half in range(2):
                send_ref[batch, 2 * pair + half] = mixed[half]

            @pl.when(pair == 0)
            def _():
                tp_copy(batch, 0, target_of(0)).start()
                hop_copy(batch).start()

            @pl.when(pair > 0)
            def _():
                tp_copy(batch, 2 * pair, target_of(2 * pair)).start()

            @pl.when((pair > 0) & (pair < 3))
            def _():
                tp_copy(batch, 2 * pair + 1, target_of(2 * pair + 1)).start()

            @pl.when(pair == 3)
            def _():
                hop_copy(batch).wait_recv()
                relay_copy(batch).start()

            @pl.when(pair == 3)
            def _():
                rows_ref[batch * 128 : batch * 128 + 128, lanes_of(tp)] = mixed[1]

    def rows_arrive(batch, pair):
        if pair == 0:
            tp_copy(batch, 0, target_of(0)).wait_recv()
            relay_copy(batch).wait_recv()
        else:
            for i in range(2 * pair, min(2 * pair + 2, 7)):
                tp_copy(batch, i, target_of(i)).wait_recv()

    for batch, all_ref in ((0, even_ref), (1, odd_ref)):
        for part in ("early", "late"):
            arrive(*(f"{part}{batch}{way}" for way in ("+", "-", "3+", "3-")))
        chosen_branch(batch, all_ref)

    weight.wait()
    for pair in range(4):
        rows_arrive(0, pair)
    stage_ref[0] = jnp.dot(rows_ref[0:128, :], weight_ref[...], preferred_element_type=jnp.float32).astype(
        stage_ref.dtype
    )
    leave = [pltpu.make_async_copy(stage_ref.at[i], out_hbm.at[i], leave_sem.at[i]) for i in range(2)]
    leave[0].start()
    for pair, away in ((3, 0), (1, 1), (2, 3), (0, 2)):
        rows_arrive(1, pair)
        at = pl.ds(pl.multiple_of((ty + 4 - away) % 4 * 256, 256), 256)
        part = jnp.dot(rows_ref[128:256, at], weight_ref[at, :], preferred_element_type=jnp.float32)
        if pair == 3:
            total_ref[...] = part
        elif pair:
            total_ref[...] += part
        else:
            stage_ref[1] = (total_ref[...] + part).astype(stage_ref.dtype)
    leave[1].start()

    for batch in range(2):
        for i in (0, 2, 3, 4, 5, 6):
            tp_copy(batch, i, target_of(i)).wait_send()
        hop_copy(batch).wait_send()
        relay_copy(batch).wait_send()
    for k in range(1, 16):
        sum_copy(k).wait_send()
    for copy in leave:
        copy.wait()
    for name in NAMES:
        span_copy(*name).wait_send()


def layer(chosen, tokens, rest, out_weight, seq):
    rows, width = tokens.shape
    args = (tokens, *rest, *rope_tables(seq))
    bf, f32 = jnp.bfloat16, jnp.float32
    spans = seq // rows
    held = [pltpu.VMEM((rows // ROWS, ROWS, width), bf)]
    held += [pltpu.VMEM(a.shape, a.dtype) for a in args[1:-2]]
    held += [pltpu.VMEM((rows // 64, 128), f32)] * 2
    entry = (32, 128)
    dma = pltpu.SemaphoreType.DMA
    return pl.pallas_call(
        layer_kernel,
        in_specs=[pl.BlockSpec(memory_space=pltpu.HBM)] * (len(args) + 2),
        out_specs=pl.BlockSpec(memory_space=pltpu.HBM),
        out_shape=jax.ShapeDtypeStruct((2, rows // 16, width), bf),
        scratch_shapes=held + [
            pltpu.VMEM((256, width), bf),
            pltpu.VMEM((rows // ROWS, ROWS, 1), f32),
            pltpu.VMEM((rows, 128), f32),
            pltpu.VMEM((rows // CMP_BLOCK, CMP_BLOCK * 64), bf),
            pltpu.VMEM((rows // CMP_BLOCK, CMP_BLOCK * 64), bf),
            pltpu.VMEM((2, rows, 128), bf),
            pltpu.VMEM((2, rows, 128), bf),
            pltpu.VMEM((2, rows, 128), f32),
            pltpu.VMEM((rows // CMP_BLOCK, 128), bf),
            pltpu.VMEM((2, 32, *entry), bf),
            pltpu.VMEM((2, 128, *entry), bf),
            pltpu.VMEM((2, 192, *entry), bf),
            pltpu.VMEM((2, 64, *entry), bf),
            pltpu.VMEM((2, 224, *entry), bf),
            pltpu.VMEM((2, 224, *entry), bf),
            pltpu.VMEM(chosen.shape, jnp.int32),
            pltpu.VMEM((32, chosen.shape[-1]), jnp.int32),
            pltpu.SMEM((32, chosen.shape[-1]), jnp.int32),
            pltpu.VMEM((spans, rows // CMP_BLOCK, 128), bf),
            pltpu.VMEM((rows, 128), f32),
            pltpu.VMEM((2, 8, 128, 128), bf),
            pltpu.VMEM((rows // 8, 1024), bf),
            pltpu.VMEM((2, 128, 128), bf),
            pltpu.VMEM(out_weight.shape, bf),
            pltpu.VMEM((rows // 16, width), f32),
            pltpu.VMEM((2, rows // 16, width), bf),
            dma((18,)), dma((rows // ROWS,)), dma, dma, dma((2,)), dma((len(PLAN),)), dma((len(PLAN),)),
            dma((15,)), dma((15,)), dma((16,)), dma((16,)),
        ],
        compiler_params=pltpu.CompilerParams(collective_id=0, has_side_effects=True, vmem_limit_bytes=67043328),
        name="layer",
    )(chosen, *args, out_weight)


def finish_kernel(in_ref, out_ref, held_ref, in_sem, out_sem):
    n = held_ref.shape[0]
    come = [pltpu.make_async_copy(in_ref.at[i], held_ref.at[i], in_sem.at[i]) for i in range(n)]
    go = [pltpu.make_async_copy(held_ref.at[i], out_ref.at[i], out_sem.at[i]) for i in range(n)]
    for copy in come:
        copy.start()
    for a, b in zip(come, go):
        a.wait()
        b.start()
    for copy in go:
        copy.wait()


def finish(rows):
    shape = (4, rows.shape[1] // 2, rows.shape[2])
    hbm = pl.BlockSpec(memory_space=pltpu.HBM)
    return pl.pallas_call(
        finish_kernel,
        in_specs=[hbm],
        out_specs=hbm,
        out_shape=jax.ShapeDtypeStruct(shape, rows.dtype),
        scratch_shapes=[pltpu.VMEM(shape, rows.dtype), pltpu.SemaphoreType.DMA((4,)), pltpu.SemaphoreType.DMA((4,))],
        name="finish",
    )(rows.reshape(shape)).reshape(-1, rows.shape[2])


def per_device(
    tokens, norm_gain, query_weight, cmp_key_weight, cmp_value_weight, sel_key_weight, sel_value_weight,
    branch_weight, key_embed, key_inner, key_outer, value_embed, value_inner, value_outer, out_weight, chosen,
):
    seq = tokens.shape[0] * lax.axis_size("kv")
    rest = (
        norm_gain, query_weight,
        cmp_key_weight.T, cmp_value_weight.T, sel_key_weight.T, sel_value_weight.T,
        branch_weight.transpose(0, 2, 1),
        key_embed, key_inner.transpose(0, 2, 1), key_outer,
        value_embed, value_inner.transpose(0, 2, 1), value_outer,
    )
    return finish(layer(chosen.transpose(0, 2, 1), tokens, rest, out_weight, seq))


def solution(mesh):
    placed = (
        P("kv", None), P(), P(None, "tp"), P(None, "tp"), P(None, "tp"), P(None, "tp"), P(None, "tp"), P(),
        P("tp", None, None), P("tp", None, None), P("tp", None, None), P("tp", None, None), P("tp", None, None),
        P("tp", None, None), P(), P("tp", None, None),
    )
    return jax.shard_map(
        per_device, mesh=mesh, in_specs=placed, out_specs=P(("kv", "tp"), None), check_vma=False
    )
```

```python
import math

import jax
import jax.numpy as jnp
import numpy as np
from jax import lax
from jax.experimental import pallas as pl
from jax.experimental.pallas import tpu as pltpu
from jax.sharding import PartitionSpec as P

HEAD_DIM = 64
CMP_BLOCK = 32
SEL_BLOCK = 64
Q_BLOCK = 128
FAR_PICKS = 8
ROPE_BASE = 10000.0
NORM_EPS = 1e-06
MESH = pl.DeviceIdType.MESH
NT = (((1,), (1,)), ((), ()))
NEG = -1e30
ROWS = 512


def rope_tables(seq):
    half = HEAD_DIM // 2
    inverse = ROPE_BASE ** (-np.arange(half, dtype=np.float64) / half)
    lane = np.arange(128) % half
    low = np.arange(64, dtype=np.float64)[:, None] * inverse[lane][None, :]
    high = np.arange(seq // 64, dtype=np.float64)[:, None] * 64.0 * inverse[lane][None, :]
    return tuple(np.asarray(f(a), np.float32) for a in (low, high) for f in (np.cos, np.sin))


def gelu(x):
    return 0.5 * x * (1.0 + jnp.tanh(math.sqrt(2.0 / math.pi) * (x + 0.044715 * (x * x * x))))


WAYS = {0: ("x", "z"), 1: ("z", "x")}
ORDER = (0, 1, 3, 2)


def copy_plan():
    plan = {}
    for kind, (first, second) in WAYS.items():
        for part in (0, 1):
            plan[kind, f"own{part}+"] = (first + "+", "ring", 16 * part, 16, "ring", 96 + 16 * part)
            plan[kind, f"own{part}-"] = (first + "-", "ring", 16 * part, 16, "ring", 32 + 16 * part)
        plan[kind, "far+"] = (first + "+", "ring", 96, 16, "ring", 64)
        plan[kind, "far-"] = (first + "-", "ring", 48, 16, "ring", 80)
        for batch, to in enumerate(("even", "odd")):
            out, hop = 96 * batch, 32 * batch
            for name, at, n in ((f"early{batch}", 0, 8), (f"late{batch}", 8, 24)):
                half = n // 2
                plan[kind, name + "+"] = (second + "+", "pack", out + at, n, to, 192 + at)
                plan[kind, name + "-"] = (second + "-", "pack", out + 64 + at, n, to, 128 + at)
                plan[kind, name + "2+"] = (second + "+", "pack", out + 32 + at, half, "pass", hop + at)
                plan[kind, name + "2-"] = (second + "-", "pack", out + 32 + at + half, half, "pass", hop + at + half)
                plan[kind, name + "3+"] = (second + "+", "pass", hop + at, half, to, 160 + at)
                plan[kind, name + "3-"] = (second + "-", "pass", hop + at + half, half, to, 160 + at + half)
    return plan


PLAN = copy_plan()
NAMES = list(PLAN)


def layer_kernel(
    chosen_hbm, x_hbm, gain_hbm, qw_hbm, ck_hbm, cv_hbm, sk_hbm, sv_hbm, bw_hbm,
    ke_hbm, ki_hbm, ko_hbm, ve_hbm, vi_hbm, vo_hbm, cl_hbm, sl_hbm, ch_hbm, sh_hbm, weight_hbm,
    out_hbm,
    x_ref, gain_ref, qw_ref, ck_ref, cv_ref, sk_ref, sv_ref, bw_ref,
    ke_ref, ki_ref, ko_ref, ve_ref, vi_ref, vo_ref, cl_ref, sl_ref, ch_ref, sh_ref,
    w_ref, scale_ref, bi_ref, xk_ref, xv_ref, qp_ref, qt_ref, gate_ref, sum_ref,
    own_ref, ring_ref, pack_ref, pass_ref, even_ref, odd_ref, chosen_ref, table_ref, find_ref,
    sums_ref, mix_ref, send_ref, rows_ref, hop_ref, weight_ref, total_ref, stage_ref,
    in_sem, x_sem, find_sem, weight_sem, leave_sem, span_send, span_recv, sum_send, sum_recv, tp_send, tp_recv,
):
    me = lax.axis_index("kv")
    tp = lax.axis_index("tp")
    mz, mx = me // 4, me % 4
    width = x_ref.shape[-1]
    steps = x_ref.shape[0]

    small = [
        (gain_hbm, gain_ref), (sk_hbm, sk_ref), (sv_hbm, sv_ref), (ck_hbm, ck_ref), (cv_hbm, cv_ref),
        (cl_hbm, cl_ref), (sl_hbm, sl_ref), (ch_hbm.at[pl.ds(me * 32, 32)], ch_ref),
        (sh_hbm.at[pl.ds(me * 32, 32)], sh_ref), (ke_hbm, ke_ref), (ve_hbm, ve_ref),
        (ki_hbm, ki_ref), (ko_hbm, ko_ref), (vi_hbm, vi_ref), (vo_hbm, vo_ref), (qw_hbm, qw_ref), (bw_hbm, bw_ref),
        (chosen_hbm, chosen_ref),
    ]
    small = [pltpu.make_async_copy(a, b, in_sem.at[i]) for i, (a, b) in enumerate(small)]
    rows_in = [pltpu.make_async_copy(x_hbm.at[pl.ds(i * ROWS, ROWS)], x_ref.at[i], x_sem.at[i]) for i in range(steps)]
    small[17].start()
    for copy in small[:9]:
        copy.start()
    for copy in rows_in:
        copy.start()
    for copy in small[9:17]:
        copy.start()

    weight = pltpu.make_async_copy(weight_hbm, weight_ref, weight_sem)
    weight.start()

    barrier = pltpu.get_barrier_semaphore()
    for k in range(1, 16):
        pl.semaphore_signal(barrier, inc=1, device_id=((me + k) % 16, tp), device_id_type=MESH)
    for k in range(1, 8):
        pl.semaphore_signal(barrier, inc=1, device_id=(me, (tp + k) % 8), device_id_type=MESH)

    lane = lax.broadcasted_iota(jnp.int32, (1, 128), 1)
    front = lane < 64
    flip = lane % 64 < 32
    sign = jnp.where(flip, -1.0, 1.0)

    small[17].wait()
    block = chosen_ref[0]
    query = lax.broadcasted_iota(jnp.int32, block.shape, 1)
    for s in range(16):
        table_ref[s : s + 1, :] = jnp.sum(jnp.where(block // 32 == s, block % 32, 0), axis=0, keepdims=True)
    usable = block * SEL_BLOCK < query * Q_BLOCK
    rz = (block // 128 + 4 - mz) % 4
    rx = (block // 32 % 4 + 4 - mx) % 4
    for row, r_first, r_second in ((16, rx, rz), (24, rz, rx)):
        place = jnp.where(r_first < 2, r_first, 5 - r_first)
        at = jnp.where(r_second == 0, r_first * 32 + block % 32, 96 + r_second * 32 + place * 8 + query % 16 // 2)
        table_ref[row : row + 8, :] = jnp.where(usable, at, -1)
    find = pltpu.make_async_copy(table_ref, find_ref, find_sem)
    find.start()

    def angles(step):
        cos, sin = [], []
        low_c, low_s = cl_ref[...], sl_ref[...]
        for g in range(ROWS // 64):
            hc = ch_ref[pl.ds(step * (ROWS // 64) + g, 1), :]
            hs = sh_ref[pl.ds(step * (ROWS // 64) + g, 1), :]
            cos.append(low_c * hc - low_s * hs)
            sin.append(low_c * (hs * sign) + low_s * (hc * sign))
        return jnp.concatenate(cos, axis=0), jnp.concatenate(sin, axis=0)

    def turn(v, c, s):
        swapped = jnp.where(flip, pltpu.roll(v, 96, 1), pltpu.roll(v, 32, 1))
        return v * c + swapped * s

    for copy in small[:9]:
        copy.wait()
    gain = gain_ref[...].astype(jnp.float32).reshape(1, width)
    for at, ref in ((0, sk_ref), (64, sv_ref), (128, ck_ref), (192, cv_ref)):
        w_ref[at : at + 64, :] = (ref[...].astype(jnp.float32) * gain).astype(jnp.bfloat16)
    for copy in small[9:11]:
        copy.wait()
    embed = jnp.concatenate([ke_ref[0], ve_ref[0]], axis=1).astype(jnp.float32)
    embed = jnp.concatenate([embed] * (ROWS // CMP_BLOCK), axis=0)

    def keys_and_values(step):
        pltpu.make_async_copy(
            x_hbm.at[pl.ds(pl.multiple_of(step * ROWS, ROWS), ROWS)], x_ref.at[step], x_sem.at[step]
        ).wait()
        x = x_ref[step]
        xf = x.astype(jnp.float32)
        scale = lax.rsqrt(jnp.sum(xf * xf, axis=1, keepdims=True) * (1.0 / width) + NORM_EPS)
        scale_ref[step] = scale
        y = lax.dot_general(x, w_ref[...], NT, preferred_element_type=jnp.float32) * scale
        cos, sin = angles(step)
        kv = turn(y[:, 0:128], jnp.where(front, cos, 1.0), jnp.where(front, sin, 0.0)).astype(jnp.bfloat16)
        kv = kv.reshape(ROWS // 64, 2, 32, 128)
        for kind in range(2):
            own_ref[kind, pl.ds(step * (ROWS // 64), ROWS // 64)] = kv[:, kind]
            ring_ref[kind, pl.ds(step * (ROWS // 64), ROWS // 64)] = kv[:, kind]
        raw = y[:, 128:256].astype(jnp.bfloat16).astype(jnp.float32)
        bi_ref[pl.ds(pl.multiple_of(step * ROWS, ROWS), ROWS), :] = raw + embed

    step_to = {
        "x+": (mz * 4 + (mx + 1) % 4, tp),
        "x-": (mz * 4 + (mx + 3) % 4, tp),
        "z+": (((mz + 1) % 4) * 4 + mx, tp),
        "z-": (((mz + 3) % 4) * 4 + mx, tp),
    }

    def sum_copy(k):
        return pltpu.make_async_remote_copy(
            src_ref=sum_ref, dst_ref=sums_ref.at[me], send_sem=sum_send.at[k - 1], recv_sem=sum_recv.at[k - 1],
            device_id=((me + k) % 16, tp), device_id_type=MESH,
        )

    refs = {"ring": ring_ref, "pack": pack_ref, "pass": pass_ref, "even": even_ref, "odd": odd_ref}

    def span_copy(*name):
        way, source, at, n, target, to = PLAN[name]
        i = NAMES.index(name)
        return pltpu.make_async_remote_copy(
            src_ref=refs[source].at[name[0], pl.ds(at, n)], dst_ref=refs[target].at[name[0], pl.ds(to, n)],
            send_sem=span_send.at[i], recv_sem=span_recv.at[i], device_id=step_to[way], device_id_type=MESH,
        )

    def start(*names):
        for name in names:
            for kind in range(2):
                span_copy(kind, name).start()

    def arrive(*names):
        for name in names:
            for kind in range(2):
                span_copy(kind, name).wait_recv()

    def pack(batch, targets, places, source):
        @pl.loop(0, 8, unroll=2)
        def _(j):
            for kind in range(2):
                for e in targets:
                    d = e + 1
                    to = ((mz + d) % 4) * 4 + mx if kind == 0 else mz * 4 + (mx + d) % 4
                    for place in places:
                        r = ORDER[place]
                        span = mz * 4 + (mx + r) % 4 if kind == 0 else ((mz + r) % 4) * 4 + mx
                        wanted = find_ref[span, to * 16 + 2 * j + batch]
                        pack_ref[kind, 96 * batch + e * 32 + place * 8 + j] = source[kind, r * 32 + wanted]

    pl.loop(0, steps // 2)(keys_and_values)
    pl.semaphore_wait(barrier, 22)
    start("own0+", "own0-")
    pl.loop(steps // 2, steps)(keys_and_values)
    start("own1+", "own1-")
    find.wait()
    for batch in range(2):
        pack(batch, (0, 1, 2), (0,), own_ref)
        start(f"early{batch}+", f"early{batch}-")

    for copy in small[11:17]:
        copy.wait()
    count = bi_ref.shape[0] // CMP_BLOCK
    for t in range(0, CMP_BLOCK, 2):
        a = bi_ref[pl.ds(t, count, stride=CMP_BLOCK), :]
        b = bi_ref[pl.ds(t + 1, count, stride=CMP_BLOCK), :]
        xk_ref[:, t * 64 : t * 64 + 128] = jnp.where(front, a, pltpu.roll(b, 64, 1)).astype(jnp.bfloat16)
        xv_ref[:, t * 64 : t * 64 + 128] = jnp.where(front, pltpu.roll(a, 64, 1), b).astype(jnp.bfloat16)
    summary = []
    for x_in, inner, outer in ((xk_ref, ki_ref, ko_ref), (xv_ref, vi_ref, vo_ref)):
        hidden = lax.dot_general(x_in[...], inner[0], NT, preferred_element_type=jnp.float32)
        hidden = gelu(hidden).astype(jnp.bfloat16)
        summary.append(jnp.dot(hidden, outer[0], preferred_element_type=jnp.float32))
    summary = jnp.concatenate(summary, axis=1).astype(jnp.bfloat16)
    sum_ref[...] = summary
    sums_ref[me] = summary

    w_ref[0:128, :] = (qw_ref[...].astype(jnp.float32).T * gain).astype(jnp.bfloat16)
    r = lax.broadcasted_iota(jnp.int32, (128, 32), 0)
    c = lax.broadcasted_iota(jnp.int32, (128, 32), 1)
    want = jnp.where(r < 2, tp * 2 + r, 16 + tp * 2 + (r - 2))
    pick = jnp.where((r < 4) & (c == want), 1.0, 0.0).astype(jnp.bfloat16)
    gates = jnp.dot(pick, bw_ref[...].reshape(32, width), preferred_element_type=jnp.float32)
    w_ref[128:256, :] = (gates * gain).astype(jnp.bfloat16)

    arrive("own0+", "own0-", "own1+", "own1-")
    start("far+", "far-", "early02+", "early02-", "early12+", "early12-")
    for k in range(1, 16):
        sum_copy(k).start()

    def by_head(v):
        v = v * (HEAD_DIM**-0.5 * math.log2(math.e))
        first = jnp.where(front, v, 0.0)
        second = jnp.where(front, pltpu.roll(v, 64, 1), 0.0)
        return jnp.stack([first, second]).astype(jnp.bfloat16)

    @pl.loop(0, steps)
    def _(step):
        y = lax.dot_general(x_ref[step], w_ref[...], NT, preferred_element_type=jnp.float32) * scale_ref[step]
        at = pl.ds(pl.multiple_of(step * ROWS, ROWS), ROWS)
        q = y[:, 0:128]
        qp_ref[:, at, :] = by_head(q)
        qt_ref[:, at, :] = by_head(turn(q, *angles(step)))
        gates = 1.0 / (1.0 + jnp.exp(-y[:, 128:256]))
        for branch in range(2):
            gate_ref[branch, at, :] = jnp.where(
                front, gates[:, 2 * branch : 2 * branch + 1], gates[:, 2 * branch + 1 : 2 * branch + 2]
            )

    rest = (1, 2, 3)
    arrive("far+", "far-")
    pack(0, (1,), rest, ring_ref)
    start("late02+", "late02-")
    arrive("early02+", "early02-", "early12+", "early12-")
    start("early03+", "early03-", "early13+", "early13-")
    pack(0, (0,), rest, ring_ref)
    start("late0+")
    pack(0, (2,), rest, ring_ref)
    start("late0-")
    pack(1, (0, 1, 2), rest, ring_ref)
    for kind in range(2):
        even_ref[kind, 0:128] = ring_ref[kind]
        odd_ref[kind, 0:128] = ring_ref[kind]
    for k in range(1, 16):
        sum_copy(k).wait_recv()

    base = me * 2048

    def with_totals(keys):
        return jnp.where(front, jnp.ones((), jnp.bfloat16), keys)

    def join(first, second):
        value = jnp.where(front, pltpu.roll(first, 64, 1), second)
        total = jnp.where(front, first, pltpu.roll(second, 64, 1))
        return value / jnp.maximum(total, 0.5)

    def compressed(t):
        at = pl.multiple_of(t * 256, 256)
        rows = base + at + lax.broadcasted_iota(jnp.int32, (256, 1), 0)
        limit = (rows + 1) // CMP_BLOCK
        column = lax.broadcasted_iota(jnp.int32, (256, 1024), 1)
        sums = sums_ref[...].reshape(1024, 128)
        out = []
        for h in range(2):
            s = lax.dot_general(qp_ref[h, pl.ds(at, 256), :], sums, NT, preferred_element_type=jnp.float32)
            s = jnp.where(column < limit, s, NEG)
            p = jnp.exp2(s - jnp.maximum(jnp.max(s, axis=1, keepdims=True), -1e20)).astype(jnp.bfloat16)
            out.append(jnp.dot(p, with_totals(sums), preferred_element_type=jnp.float32))
        mix_ref[pl.ds(at, 256), :] = join(*out) * gate_ref[0, pl.ds(at, 256), :]

    pl.loop(0, 3)(compressed)
    arrive("late02+", "late02-")
    start("late03+", "late03-", "late12+", "late12-", "late1+", "late1-")
    pl.loop(3, 8)(compressed)
    arrive("late12+", "late12-")
    start("late13+", "late13-")

    triangle = lax.broadcasted_iota(jnp.int32, (128, 128), 1) <= lax.broadcasted_iota(jnp.int32, (128, 128), 0)
    ty, core = tp // 2, tp % 2

    def target_of(i):
        pair = i // 2
        dy = jnp.where(pair == 0, 2, jnp.where(pair == 1, 1, jnp.where(pair == 2, 3, 0)))
        flip = jnp.where(pair == 3, 1 - i % 2, i % 2)
        return ((ty + dy) % 4) * 2 + (core + flip) % 2

    def lanes_of(t):
        return pl.ds(pl.multiple_of(t * 128, 128), 128)

    def tp_copy(batch, i, to):
        return pltpu.make_async_remote_copy(
            src_ref=send_ref.at[batch, i], dst_ref=rows_ref.at[pl.ds(batch * 128, 128), lanes_of(tp)],
            send_sem=tp_send.at[batch * 8 + i], recv_sem=tp_recv.at[batch * 8 + i],
            device_id=(me, to), device_id_type=MESH,
        )

    def hop_copy(batch):
        return pltpu.make_async_remote_copy(
            src_ref=send_ref.at[batch, 1], dst_ref=hop_ref.at[batch],
            send_sem=tp_send.at[batch * 8 + 1], recv_sem=tp_recv.at[batch * 8 + 1],
            device_id=(me, (ty + 3) % 4 * 2 + core), device_id_type=MESH,
        )

    def relay_copy(batch):
        return pltpu.make_async_remote_copy(
            src_ref=hop_ref.at[batch],
            dst_ref=rows_ref.at[pl.ds(batch * 128, 128), lanes_of((ty + 1) % 4 * 2 + core)],
            send_sem=tp_send.at[batch * 8 + 7], recv_sem=tp_recv.at[batch * 8 + 7],
            device_id=(me, (ty + 3) % 4 * 2 + 1 - core), device_id_type=MESH,
        )

    def chosen_branch(batch, all_ref):
        @pl.loop(0, 4)
        def _(pair):
            keys, score, at = [], [], []
            for half in range(2):
                j = target_of(2 * pair + half) * 2 + batch
                at.append(pl.ds(pl.multiple_of(j * 128, 128), 128))
                parts = [own_ref[kind, 2 * j + b] for b in range(2) for kind in range(2)]
                bias = []
                for c in range(FAR_PICKS):
                    places = [find_ref[16 + 8 * kind + c, me * 16 + j] for kind in range(2)]
                    parts += [all_ref[kind, jnp.maximum(places[kind], 0)] for kind in range(2)]
                    bias.append(jnp.where(places[0] < 0, NEG, 0.0))
                keys.append(jnp.concatenate(parts, axis=0))
                q = jnp.concatenate([qt_ref[h, at[half], :] for h in range(2)], axis=0)
                s = lax.dot_general(q, keys[half], NT, preferred_element_type=jnp.float32)
                mine = jnp.where(jnp.concatenate([triangle, triangle], axis=0), s[:, :128], NEG)
                far = [
                    s[:, 128 + 128 * c : 256 + 128 * c] + jnp.where(front, bias[2 * c], bias[2 * c + 1])
                    for c in range(FAR_PICKS // 2)
                ]
                score.append(jnp.concatenate([mine, *far], axis=1))
            weights = [jnp.exp2(s - jnp.max(s, axis=1, keepdims=True)).astype(jnp.bfloat16) for s in score]
            out = [
                jnp.dot(w, with_totals(k), preferred_element_type=jnp.float32) for w, k in zip(weights, keys)
            ]
            mixed = [
                (join(o[:128], o[128:]) * gate_ref[1, rows, :] + mix_ref[rows, :]).astype(jnp.bfloat16)
                for o, rows in zip(out, at)
            ]
            for half in range(2):
                send_ref[batch, 2 * pair + half] = mixed[half]

            @pl.when(pair == 0)
            def _():
                tp_copy(batch, 0, target_of(0)).start()
                (hop_copy(batch) if batch == 0 else tp_copy(batch, 1, target_of(1))).start()

            @pl.when(pair > 0)
            def _():
                tp_copy(batch, 2 * pair, target_of(2 * pair)).start()

            @pl.when((pair > 0) & (pair < 3))
            def _():
                tp_copy(batch, 2 * pair + 1, target_of(2 * pair + 1)).start()

            @pl.when(pair == 3)
            def _():
                if batch == 0:
                    hop_copy(batch).wait_recv()
                    relay_copy(batch).start()

            @pl.when(pair == 3)
            def _():
                rows_ref[batch * 128 : batch * 128 + 128, lanes_of(tp)] = mixed[1]

    def rows_arrive(batch, pair):
        if pair == 0:
            tp_copy(batch, 0, target_of(0)).wait_recv()
            (relay_copy(batch) if batch == 0 else tp_copy(batch, 1, target_of(1))).wait_recv()
        else:
            for i in range(2 * pair, min(2 * pair + 2, 7)):
                tp_copy(batch, i, target_of(i)).wait_recv()

    for batch, all_ref in ((0, even_ref), (1, odd_ref)):
        for part in ("early", "late"):
            arrive(*(f"{part}{batch}{way}" for way in ("+", "-", "3+", "3-")))
        chosen_branch(batch, all_ref)

    weight.wait()
    for pair in range(4):
        rows_arrive(0, pair)
    stage_ref[0] = jnp.dot(rows_ref[0:128, :], weight_ref[...], preferred_element_type=jnp.float32).astype(
        stage_ref.dtype
    )
    leave = [pltpu.make_async_copy(stage_ref.at[i], out_hbm.at[i], leave_sem.at[i]) for i in range(2)]
    leave[0].start()
    for pair, away in ((3, 0), (1, 1), (2, 3), (0, 2)):
        rows_arrive(1, pair)
        at = pl.ds(pl.multiple_of((ty + 4 - away) % 4 * 256, 256), 256)
        part = jnp.dot(rows_ref[128:256, at], weight_ref[at, :], preferred_element_type=jnp.float32)
        if pair == 3:
            total_ref[...] = part
        elif pair:
            total_ref[...] += part
        else:
            stage_ref[1] = (total_ref[...] + part).astype(stage_ref.dtype)
    leave[1].start()

    for batch in range(2):
        for i in (0, 2, 3, 4, 5, 6):
            tp_copy(batch, i, target_of(i)).wait_send()
        if batch == 0:
            hop_copy(batch).wait_send()
            relay_copy(batch).wait_send()
        else:
            tp_copy(batch, 1, target_of(1)).wait_send()
    for k in range(1, 16):
        sum_copy(k).wait_send()
    for copy in leave:
        copy.wait()
    for name in NAMES:
        span_copy(*name).wait_send()


def layer(chosen, tokens, rest, out_weight, seq):
    rows, width = tokens.shape
    args = (tokens, *rest, *rope_tables(seq))
    bf, f32 = jnp.bfloat16, jnp.float32
    spans = seq // rows
    held = [pltpu.VMEM((rows // ROWS, ROWS, width), bf)]
    held += [pltpu.VMEM(a.shape, a.dtype) for a in args[1:-2]]
    held += [pltpu.VMEM((rows // 64, 128), f32)] * 2
    entry = (32, 128)
    dma = pltpu.SemaphoreType.DMA
    return pl.pallas_call(
        layer_kernel,
        in_specs=[pl.BlockSpec(memory_space=pltpu.HBM)] * (len(args) + 2),
        out_specs=pl.BlockSpec(memory_space=pltpu.HBM),
        out_shape=jax.ShapeDtypeStruct((2, rows // 16, width), bf),
        scratch_shapes=held + [
            pltpu.VMEM((256, width), bf),
            pltpu.VMEM((rows // ROWS, ROWS, 1), f32),
            pltpu.VMEM((rows, 128), f32),
            pltpu.VMEM((rows // CMP_BLOCK, CMP_BLOCK * 64), bf),
            pltpu.VMEM((rows // CMP_BLOCK, CMP_BLOCK * 64), bf),
            pltpu.VMEM((2, rows, 128), bf),
            pltpu.VMEM((2, rows, 128), bf),
            pltpu.VMEM((2, rows, 128), f32),
            pltpu.VMEM((rows // CMP_BLOCK, 128), bf),
            pltpu.VMEM((2, 32, *entry), bf),
            pltpu.VMEM((2, 128, *entry), bf),
            pltpu.VMEM((2, 192, *entry), bf),
            pltpu.VMEM((2, 64, *entry), bf),
            pltpu.VMEM((2, 224, *entry), bf),
            pltpu.VMEM((2, 224, *entry), bf),
            pltpu.VMEM(chosen.shape, jnp.int32),
            pltpu.VMEM((32, chosen.shape[-1]), jnp.int32),
            pltpu.SMEM((32, chosen.shape[-1]), jnp.int32),
            pltpu.VMEM((spans, rows // CMP_BLOCK, 128), bf),
            pltpu.VMEM((rows, 128), f32),
            pltpu.VMEM((2, 8, 128, 128), bf),
            pltpu.VMEM((rows // 8, 1024), bf),
            pltpu.VMEM((2, 128, 128), bf),
            pltpu.VMEM(out_weight.shape, bf),
            pltpu.VMEM((rows // 16, width), f32),
            pltpu.VMEM((2, rows // 16, width), bf),
            dma((18,)), dma((rows // ROWS,)), dma, dma, dma((2,)), dma((len(PLAN),)), dma((len(PLAN),)),
            dma((15,)), dma((15,)), dma((16,)), dma((16,)),
        ],
        compiler_params=pltpu.CompilerParams(collective_id=0, has_side_effects=True, vmem_limit_bytes=67043328),
        name="layer",
    )(chosen, *args, out_weight)


def finish_kernel(in_ref, out_ref, held_ref, in_sem, out_sem):
    n = held_ref.shape[0]
    come = [pltpu.make_async_copy(in_ref.at[i], held_ref.at[i], in_sem.at[i]) for i in range(n)]
    go = [pltpu.make_async_copy(held_ref.at[i], out_ref.at[i], out_sem.at[i]) for i in range(n)]
    for copy in come:
        copy.start()
    for a, b in zip(come, go):
        a.wait()
        b.start()
    for copy in go:
        copy.wait()


def finish(rows):
    shape = (4, rows.shape[1] // 2, rows.shape[2])
    hbm = pl.BlockSpec(memory_space=pltpu.HBM)
    return pl.pallas_call(
        finish_kernel,
        in_specs=[hbm],
        out_specs=hbm,
        out_shape=jax.ShapeDtypeStruct(shape, rows.dtype),
        scratch_shapes=[pltpu.VMEM(shape, rows.dtype), pltpu.SemaphoreType.DMA((4,)), pltpu.SemaphoreType.DMA((4,))],
        name="finish",
    )(rows.reshape(shape)).reshape(-1, rows.shape[2])


def per_device(
    tokens, norm_gain, query_weight, cmp_key_weight, cmp_value_weight, sel_key_weight, sel_value_weight,
    branch_weight, key_embed, key_inner, key_outer, value_embed, value_inner, value_outer, out_weight, chosen,
):
    seq = tokens.shape[0] * lax.axis_size("kv")
    rest = (
        norm_gain, query_weight,
        cmp_key_weight.T, cmp_value_weight.T, sel_key_weight.T, sel_value_weight.T,
        branch_weight.transpose(0, 2, 1),
        key_embed, key_inner.transpose(0, 2, 1), key_outer,
        value_embed, value_inner.transpose(0, 2, 1), value_outer,
    )
    return finish(layer(chosen.transpose(0, 2, 1), tokens, rest, out_weight, seq))


def solution(mesh):
    placed = (
        P("kv", None), P(), P(None, "tp"), P(None, "tp"), P(None, "tp"), P(None, "tp"), P(None, "tp"), P(),
        P("tp", None, None), P("tp", None, None), P("tp", None, None), P("tp", None, None), P("tp", None, None),
        P("tp", None, None), P(), P("tp", None, None),
    )
    return jax.shard_map(
        per_device, mesh=mesh, in_specs=placed, out_specs=P(("kv", "tp"), None), check_vma=False
    )
```
